256 devices in a mesh: ep: 32 (over z, x), tp: 8 (over y, core).
Axes of the slice: x: 4, y: 4, z: 8, core: 2. Of those that a mesh axis runs over, the one named last changes fastest.
Arguments:
- hidden_in: bfloat16 [1024, 2048], P('ep', 'tp'), may hold values from -6 to 6
- state_in: float32 [1024, 8, 128, 128], P('ep', 'tp'), may hold values from -0.6 to 0.6
- attn_gain: float32 [2048], replicated, may hold values from 0.1 to 1.9
- w_query: bfloat16 [2048, 1024], P(None, 'tp'), may hold values from -0.125 to 0.125
- w_key: bfloat16 [2048, 1024], P(None, 'tp'), may hold values from -0.125 to 0.125
- w_value: bfloat16 [2048, 1024], P(None, 'tp'), may hold values from -0.125 to 0.125
- w_gate: bfloat16 [2048, 1024], P(None, 'tp'), may hold values from -0.125 to 0.125
- w_beta: bfloat16 [2048, 8], replicated, may hold values from -0.125 to 0.125
- w_decay: bfloat16 [2048, 8], replicated, may hold values from -0.125 to 0.125
- decay_scale: float32 [8], replicated, may hold values from 0.05 to 3
- head_gain: float32 [128], replicated, may hold values from 0.1 to 1.9
- w_output: bfloat16 [1024, 2048], P(None, 'tp'), may hold values from -0.1875 to 0.1875
- ffn_gain: float32 [2048], replicated, may hold values from 0.1 to 1.9
- expert_ids: int32 [1024, 2], P('ep'), may hold values from 0 to 31, all different within a row; in each aligned block of 32 rows (0 to 31, 32 to 63, ...) at most 4 rows name the same one
- route_weight: float32 [1024, 2], P('ep'), may hold values from 0.2 to 1
- expert_gate: bfloat16 [32, 2048, 3072], P('ep', None, 'tp'), may hold values from -0.125 to 0.125
- expert_up: bfloat16 [32, 2048, 3072], P('ep', None, 'tp'), may hold values from -0.125 to 0.125
- expert_down: bfloat16 [32, 3072, 2048], P('ep', 'tp'), may hold values from -0.109375 to 0.109375
- dense_gate: bfloat16 [2048, 4096], P(None, 'ep'), may hold values from -0.125 to 0.125
- dense_up: bfloat16 [2048, 4096], P(None, 'ep'), may hold values from -0.125 to 0.125
- dense_down: bfloat16 [4096, 2048], P('ep'), may hold values from -0.09375 to 0.09375
- dense_mix: float32 [2048], P('tp'), may hold values from -6 to 6
Outputs:
- result: bfloat16 [1024, 2048], P('ep', 'tp')
- new_state: float32 [1024, 8, 128, 128], P('ep', 'tp')
The draws below stay inside these ranges and needn't reach their ends.
Inputs may be any that keep to these rules, and one draw needn't show every extreme that they name: `expert_ids`: each row names 2 different experts. Within the rows of one index of ep (aligned blocks of 32 sequences) no expert is named more than 4 times, a bound that some block reaches.
All inputs are finite; a program needn't handle non-finite values.
Results may differ from the reference program's by a relative error of at most 0.015.
Values may be sent and summed in bfloat16 or wider, within the bound.
A program may use at most 64 MiB of HBM per device.

```python
import math
import jax
import jax.numpy as jnp
import numpy as np
from jax import lax

D = 2048
H = 8
DK = 128
DV = 128
FE = 3072
FFD = 4096
TOP = 2
SEQ_DEV = 32
EXPERTS = 32
CAP = 4
SEQS = 1024
N_EP = 32
N_TP = 8


def steps_of(key, dims, shards, least, largest):
    def one(position, shards_of):
        heights = jax.random.uniform(jax.random.fold_in(jax.random.fold_in(key, 6), position), (shards_of,), jnp.float32, least / len(shards), largest / len(shards))
        return jnp.repeat(jnp.exp(heights), dims[position] // shards_of).reshape((-1,) + (1,) * (len(dims) - position - 1))

    level = one(*shards[0])
    for cut in shards[1:]:
        level = level * one(*cut)
    return level


def deal_out(key, own, number, rows, count, top, reach, skew):
    sequence = jax.random.permutation(key, count)
    packed, ordinary = portions_of(count, rows * top, reach, skew, True), portions_of(count, rows * top, reach, skew, False)
    places = jnp.arange(count)

    def named(lengths, offset_by):
        used = int((lengths > 0).sum())
        fixed = max(1, used // 4)
        shifted = fixed + (places - fixed + offset_by * (used - fixed)) % max(1, count - fixed)
        return jnp.zeros((count,), jnp.int32).at[sequence[jnp.where(places < fixed, places, shifted)]].set(jnp.asarray(lengths, jnp.int32))

    lengths = jnp.where(number % 4 == 0, named(packed, number // 4), named(ordinary, number - number // 4 - 1))
    mixed = jax.random.permutation(jax.random.fold_in(own, 3), count)
    donor, receiver = mixed[0:count // 2 * 2:2], mixed[1:count // 2 * 2:2]
    slack = jnp.minimum(lengths[donor] - 1, reach - lengths[receiver]) // 2
    slack = jnp.where((donor == sequence[0]) | (receiver == sequence[0]) | (lengths[receiver] == 0), 0, jnp.maximum(slack, 0))
    shifted = jax.random.randint(jax.random.fold_in(own, 4), (count // 2,), 0, 1 << 20) % (slack + 1)
    lengths = lengths.at[donor].add(-shifted).at[receiver].add(shifted)
    members = jnp.searchsorted(jnp.cumsum(lengths), jnp.arange(rows * top), side="right").astype(jnp.int32)
    listing = members.reshape(top, rows).T
    listing = listing[jax.random.permutation(jax.random.fold_in(own, 1), rows)]
    offset_by = jax.random.randint(jax.random.fold_in(own, 2), (rows, 1), 0, top)
    return jnp.take_along_axis(listing, (jnp.arange(top)[None, :] + offset_by) % top, axis=1)


def portions_of(number_of, total, reach, skew, full):
    portions = [(1 << 20) // math.isqrt(grade ** skew) + 1 for grade in range(1, number_of + 1)]
    largest = reach if full else min(reach, max(-(-total // number_of), total * portions[0] // sum(portions)))
    least = 1 if total - largest >= number_of - 1 else 0
    holding, rest = [largest] + [least] * (number_of - 1), total - largest - least * (number_of - 1)
    while rest > 0:
        candidates = [i for i in range(1, number_of) if holding[i] < largest] or [i for i in range(1, number_of) if holding[i] < reach]
        pool, left = sum([portions[i] for i in candidates]), rest
        for i in candidates:
            extra = min(reach - holding[i], max(1, left * portions[i] // pool), rest)
            holding[i] = holding[i] + extra
            rest = rest - extra
    return np.array(holding)


def bell_draw(key, extent, spread, reach, cuts=(), kind=jnp.bfloat16):
    entries = jax.random.normal(key, extent, jnp.float32) * spread
    if len(cuts) > 0:
        entries = steps_of(key, extent, cuts, -0.22, 0.18) * entries
    return jnp.clip(entries, min=-reach, max=reach).astype(kind)


def setup_inputs(seed: int = 0) -> dict:
    arg_keys = jax.random.split(jax.random.key(seed), 23)
    hidden_in = bell_draw(arg_keys[0], (SEQS, D), 1.0, 6.0, ((0, 32), (1, 8)))
    state_in = bell_draw(arg_keys[1], (SEQS, H, DK, DV), 0.09, 0.6, ((0, 32), (1, 8)), jnp.float32)
    attn_gain = jnp.clip(1.0 + 0.18 * jax.random.normal(arg_keys[2], (D,), jnp.float32), 0.1, 1.9)
    w_query = bell_draw(arg_keys[3], (D, H * DK), D ** -0.5, 0.125, ((1, 8),))
    w_key = bell_draw(arg_keys[4], (D, H * DK), D ** -0.5, 0.125, ((1, 8),))
    w_value = bell_draw(arg_keys[5], (D, H * DV), D ** -0.5, 0.125, ((1, 8),))
    w_gate = bell_draw(arg_keys[6], (D, H * DV), D ** -0.5, 0.125, ((1, 8),))
    w_beta = bell_draw(arg_keys[7], (D, H), D ** -0.5, 0.125)
    w_decay = bell_draw(arg_keys[8], (D, H), D ** -0.5, 0.125)
    decay_scale = jnp.clip(jnp.exp(jax.random.uniform(arg_keys[9], (H,), jnp.float32, math.log(0.05), math.log(3.0))), 0.05, 3.0)
    head_gain = jnp.clip(1.0 + 0.18 * jax.random.normal(arg_keys[10], (DV,), jnp.float32), 0.1, 1.9)
    w_output = bell_draw(arg_keys[11], (H * DV, D), (H * DV) ** -0.5, 0.1875, ((1, 8),))
    ffn_gain = jnp.clip(1.0 + 0.18 * jax.random.normal(arg_keys[12], (D,), jnp.float32), 0.1, 1.9)
    expert_ids_keys = jax.random.split(jax.random.fold_in(arg_keys[13], 1), SEQS // SEQ_DEV)
    expert_ids_turns = jax.random.permutation(jax.random.fold_in(arg_keys[13], 3), SEQS // SEQ_DEV)
    expert_ids = jax.vmap(lambda own, number: deal_out(jax.random.fold_in(arg_keys[13], 2), own, number, SEQ_DEV, EXPERTS, TOP, CAP, 2))(expert_ids_keys, expert_ids_turns).reshape((SEQS, TOP))
    route_weight = jnp.clip(jnp.exp(math.log(1.0) - 1.609438 * jax.random.uniform(arg_keys[14], (SEQS, TOP), jnp.float32) ** steps_of(arg_keys[14], (SEQS, TOP), ((0, 32),), -0.2, 0.2)), 0.2, 1.0)
    expert_gate = bell_draw(arg_keys[15], (EXPERTS, D, FE), D ** -0.5, 0.125, ((0, 32), (2, 8)))
    expert_up = bell_draw(arg_keys[16], (EXPERTS, D, FE), D ** -0.5, 0.125, ((0, 32), (2, 8)))
    expert_down = bell_draw(arg_keys[17], (EXPERTS, FE, D), FE ** -0.5, 0.109375, ((0, 32), (1, 8)))
    dense_gate = bell_draw(arg_keys[18], (D, FFD), D ** -0.5, 0.125, ((1, 32),))
    dense_up = bell_draw(arg_keys[19], (D, FFD), D ** -0.5, 0.125, ((1, 32),))
    dense_down = bell_draw(arg_keys[20], (FFD, D), FFD ** -0.5, 0.09375, ((0, 32),))
    dense_mix = bell_draw(arg_keys[21], (D,), 1.5, 6.0, ((0, 8),), jnp.float32)
    return dict(hidden_in=hidden_in, state_in=state_in, attn_gain=attn_gain, w_query=w_query, w_key=w_key, w_value=w_value, w_gate=w_gate, w_beta=w_beta, w_decay=w_decay, decay_scale=decay_scale, head_gain=head_gain, w_output=w_output, ffn_gain=ffn_gain, expert_ids=expert_ids, route_weight=route_weight, expert_gate=expert_gate, expert_up=expert_up, expert_down=expert_down, dense_gate=dense_gate, dense_up=dense_up, dense_down=dense_down, dense_mix=dense_mix)


EPS = 1e-06

def root_norm(values, scale_vec):
    wide = values.astype(jnp.float32)
    return wide * lax.rsqrt(lax.optimization_barrier(jnp.mean(wide * wide, axis=-1, keepdims=True)) + EPS) * scale_vec.astype(jnp.float32)

def unit_norm(values):
    return values * lax.rsqrt(lax.optimization_barrier(jnp.sum(values * values, axis=-1, keepdims=True)) + EPS)

def slot_table(expert_ids, count):
    flat = expert_ids.reshape(-1)
    onehot = (flat[:, None] == jnp.arange(count, dtype=jnp.int32)[None, :]).astype(jnp.int32)
    before = jnp.cumsum(onehot, axis=0) - onehot
    return lax.optimization_barrier(jnp.sum(before * onehot, axis=1)).reshape(expert_ids.shape)

def delta_update(old_state, key_rows, value_rows, beta_rate, decay_rate):
    recalled = jnp.einsum('shk,shkv->shv', key_rows, old_state, precision=lax.Precision.HIGHEST)
    erased = old_state - beta_rate[..., None, None] * key_rows[..., :, None] * recalled[..., None, :]
    written = beta_rate[..., None, None] * key_rows[..., :, None] * value_rows[..., None, :]
    return decay_rate[..., None, None] * erased + written

def head_output(new_state, queries, gate_rows, head_gain):
    read = jnp.einsum('shk,shkv->shv', queries, new_state, precision=lax.Precision.HIGHEST)
    return (root_norm(read, head_gain) * jax.nn.silu(gate_rows)).astype(jnp.bfloat16)

def reference(hidden_in, state_in, attn_gain, w_query, w_key, w_value, w_gate, w_beta, w_decay, decay_scale, head_gain, w_output, ffn_gain, expert_ids, route_weight, expert_gate, expert_up, expert_down, dense_gate, dense_up, dense_down, dense_mix):
    seqs = hidden_in.shape[0]
    normed = root_norm(hidden_in, attn_gain).astype(jnp.bfloat16)
    queries = unit_norm(jnp.dot(normed, w_query, preferred_element_type=jnp.float32).reshape(seqs, H, DK)) * DK ** (-0.5)
    key_rows = unit_norm(jnp.dot(normed, w_key, preferred_element_type=jnp.float32).reshape(seqs, H, DK))
    value_rows = jnp.dot(normed, w_value, preferred_element_type=jnp.float32).reshape(seqs, H, DV)
    gate_rows = jnp.dot(normed, w_gate, preferred_element_type=jnp.float32).reshape(seqs, H, DV)
    beta_rate = jax.nn.sigmoid(jnp.dot(normed, w_beta, preferred_element_type=jnp.float32))
    decay_logit = jnp.dot(normed, w_decay, preferred_element_type=jnp.float32)
    decay_rate = jnp.exp(-decay_scale[None, :] * jax.nn.softplus(decay_logit))
    new_state = delta_update(state_in, key_rows, value_rows, beta_rate, decay_rate)
    heads_out = head_output(new_state, queries, gate_rows, head_gain).reshape(seqs, H * DV)
    mixed = (hidden_in.astype(jnp.float32) + jnp.dot(heads_out, w_output, preferred_element_type=jnp.float32)).astype(jnp.bfloat16)
    normed2 = root_norm(mixed, ffn_gain).astype(jnp.bfloat16)
    groups = expert_ids.reshape(N_EP, SEQ_DEV, TOP)
    slots = jax.vmap(lambda group_ids: slot_table(group_ids, EXPERTS))(groups).reshape(seqs, TOP)
    group_index = (jnp.arange(seqs, dtype=jnp.int32) // SEQ_DEV)[:, None]
    place = (group_index * CAP + slots).astype(jnp.int32)
    spread_rows = jnp.broadcast_to(normed2[:, None, :], (seqs, TOP, D))
    buffer = jnp.zeros((EXPERTS, N_EP * CAP, D), jnp.bfloat16).at[expert_ids, place].set(spread_rows)

    def one_expert(operands):
        rows, gate_weight, up_weight, down_weight = operands
        gate_val = jnp.dot(rows, gate_weight, preferred_element_type=jnp.float32)
        up_val = jnp.dot(rows, up_weight, preferred_element_type=jnp.float32)
        inner = (jax.nn.silu(gate_val) * up_val).astype(jnp.bfloat16)
        width = inner.shape[1] // N_TP
        total = jnp.zeros((rows.shape[0], D), jnp.float32)
        for section in range(N_TP):
            term = jnp.dot(inner[:, section * width:(section + 1) * width], down_weight[section * width:(section + 1) * width, :], preferred_element_type=jnp.float32)
            total = total + lax.optimization_barrier(term.astype(jnp.bfloat16)).astype(jnp.float32)
        return total.astype(jnp.bfloat16)
    expert_out = lax.map(one_expert, (buffer, expert_gate, expert_up, expert_down))
    picked = expert_out[expert_ids, place].astype(jnp.float32)
    moe_sum = lax.optimization_barrier(jnp.sum(route_weight[..., None] * picked, axis=1))
    dense_gate_val = jnp.dot(normed2, dense_gate, preferred_element_type=jnp.float32)
    dense_up_val = jnp.dot(normed2, dense_up, preferred_element_type=jnp.float32)
    dense_hidden = (jax.nn.silu(dense_gate_val) * dense_up_val).astype(jnp.bfloat16)
    dense_out = jnp.dot(dense_hidden, dense_down, preferred_element_type=jnp.float32)
    result = (mixed.astype(jnp.float32) + moe_sum + jax.nn.sigmoid(dense_mix)[None, :] * dense_out).astype(jnp.bfloat16)
    return (result, new_state)
```

```python
import functools

import jax
import jax.numpy as jnp
from jax import lax
from jax.experimental import pallas as pl
from jax.experimental.pallas import tpu as pltpu
from jax.sharding import PartitionSpec as P

EPS = 1e-06
MESH = pl.DeviceIdType.MESH
F32, BF16, I32 = jnp.float32, jnp.bfloat16, jnp.int32

NX, NZ, NTP, NEP = 4, 8, 8, 32
SEQ, D, WIDTH, DK, CAP = 32, 2048, 256, 128, 4
ROWS = NEP * CAP
FE, FD = 384, 128
PITCH = 72
CHUNKS = 4


def silu(v):
    return v * jax.nn.sigmoid(v)


def dot(a, b):
    return jnp.dot(a, b, preferred_element_type=F32)


def iota(shape, dim):
    return lax.broadcasted_iota(I32, shape, dim)


def kernel(
    hidden, state, attn_gain, wq, wk, wv, wg, w_beta, w_decay, decay_scale, head_gain, w_out, ffn_gain, ids, route,
    eg, eu, ed, dg, du, dd, mix,
    result, new_state,
    hid_all, v_state, v_again, v_wq, v_wk, v_wv, v_wg, v_wb, v_wd, v_dscale, v_hgain, v_wo, v_fgain, v_ids, v_route,
    v_eg, v_eu, v_ed, v_dg, v_du, v_dd, v_mix,
    xn_a, heads_all, mixed_s, send_mat, take_mat,
    disp, xa, stage, xn_e, inner_s, pb, pr, qs, yr, ret, rb,
    own_tok, dx, xn_d, px, xr, zs, zr, fs, fr,
    l_sem, out_sem,
    a_send, a_recv, h_send, h_recv, t_send, t_recv, d_send, d_recv, z_send, z_recv, x_send, x_recv,
    y_send, y_recv, c_send, c_recv, p_send, p_recv, q_send, q_recv, b_send, b_recv,
    u_send, u_recv, w_send, w_recv, f_send, f_recv,
):
    ep = lax.axis_index("ep")
    t = lax.axis_index("tp")
    z, x = lax.div(ep, NX), lax.rem(ep, NX)
    y, c = lax.div(t, 2), lax.rem(t, 2)

    def tp_peer(d):
        return ep, lax.rem(t + d, NTP)

    def ep_peer(d):
        return lax.rem(ep + d, NEP), t

    def z_peer(d):
        return lax.rem(z + d, NZ) * NX + x, t

    def x_peer(d):
        return z * NX + lax.rem(x + d, NX), t

    def y_peer(d):
        return ep, lax.rem(y + d, 4) * 2 + c

    partner = (ep, y * 2 + 1 - c)

    def remote(src, dst, send, recv, peer):
        return pltpu.make_async_remote_copy(
            src_ref=src, dst_ref=dst, send_sem=send, recv_sem=recv, device_id=peer, device_id_type=MESH
        )

    def take(view, sem):
        pltpu.make_async_copy(view, view, sem).wait()

    loads = {}
    pairs = (
        ("hid", hidden, hid_all.at[t]), ("ids", ids, v_ids), ("route", route, v_route), ("again", attn_gain, v_again),
        ("wq", wq, v_wq), ("wk", wk, v_wk), ("wv", wv, v_wv), ("wg", wg, v_wg), ("wb", w_beta, v_wb),
        ("wd", w_decay, v_wd), ("dscale", decay_scale, v_dscale), ("hgain", head_gain, v_hgain),
        ("state", state, v_state), ("wo", w_out, v_wo), ("fgain", ffn_gain, v_fgain), ("mix", mix, v_mix),
        ("dg", dg, v_dg), ("du", du, v_du), ("dd", dd, v_dd), ("eg", eg, v_eg), ("eu", eu, v_eu), ("ed", ed, v_ed),
    )
    for number, (name, src, dst) in enumerate(pairs):
        loads[name] = pltpu.make_async_copy(src, dst, l_sem.at[number])
        loads[name].start()

    barrier = pltpu.get_barrier_semaphore()
    for d in range(1, NTP):
        pl.semaphore_signal(barrier, inc=1, device_id=tp_peer(d), device_id_type=MESH)

    def greet(d, carry):
        pl.semaphore_signal(barrier, inc=1, device_id=ep_peer(d), device_id_type=MESH)
        return carry

    lax.fori_loop(1, NEP, greet, 0)

    loads["ids"].wait()
    loads["route"].wait()
    first, second = v_ids[:, 0:1], v_ids[:, 1:2]
    lane = iota((SEQ, NEP), 1)
    chosen = jnp.where((first == lane) | (second == lane), 1.0, 0.0)
    earlier = jnp.where(iota((SEQ, SEQ), 0) > iota((SEQ, SEQ), 1), 1.0, 0.0).astype(BF16)
    before = dot(earlier, chosen.astype(BF16))
    place = (chosen * (before + 1.0)).astype(BF16)
    row = iota((NEP * 8, NEP), 0)
    spread = jnp.where(row // 8 == iota((NEP * 8, NEP), 1), 1.0, 0.0).astype(BF16)
    by_row = lax.dot_general(spread, place, (((1,), (1,)), ((), ())), preferred_element_type=F32)
    want = ((row % 8) // 2 + 1).astype(F32)
    hit = by_row == want
    for h in range(2):
        send_mat[h] = jnp.where(hit & (row % 2 == h), 1.0, 0.0).astype(BF16)
    col = iota((SEQ, NEP * 8), 1)
    col_row = iota((NEP, NEP * 8), 1)
    spread_t = jnp.where(col_row // 8 == iota((NEP, NEP * 8), 0), 1.0, 0.0).astype(BF16)
    by_col = dot(place, spread_t)
    hit_t = by_col == ((col % 8) // 2 + 1).astype(F32)
    weight = jnp.where(first == col // 8, v_route[:, 0:1], 0.0) + jnp.where(second == col // 8, v_route[:, 1:2], 0.0)
    weight = jnp.where(hit_t, weight, 0.0)
    for h in range(2):
        part = jnp.where(col % 2 == h, weight, 0.0)
        high = part.astype(BF16)
        take_mat[2 * h] = high
        take_mat[2 * h + 1] = (part - high.astype(F32)).astype(BF16)

    loads["hid"].wait()
    pl.semaphore_wait(barrier, NTP - 1 + NEP - 1)

    copies = []
    for d in (4, 3, 5, 2, 6, 1, 7):
        copy = remote(hid_all.at[t], hid_all.at[t], a_send.at[d - 1], a_recv, tp_peer(d))
        copy.start()
        copies.append(copy)
    sends = copies
    loads["again"].wait()
    take(hid_all.at[pl.ds(0, 7)], a_recv)

    square = jnp.zeros((SEQ, WIDTH), F32)
    for b in range(NTP):
        wide = hid_all[b].astype(F32)
        square = square + wide * wide
    scale = lax.rsqrt(jnp.sum(square, axis=-1, keepdims=True) * (1.0 / D) + EPS)
    for b in range(NTP):
        cols = slice(b * WIDTH, (b + 1) * WIDTH)
        xn_a[:, cols] = (hid_all[b].astype(F32) * scale * v_again[:, cols]).astype(BF16)
    for name in ("wq", "wk", "wv", "wg", "wb", "wd", "dscale", "hgain"):
        loads[name].wait()
    normed = xn_a[...]
    queries = dot(normed, v_wq[...])
    queries = queries * lax.rsqrt(jnp.sum(queries * queries, axis=-1, keepdims=True) + EPS) * DK ** (-0.5)
    keys = dot(normed, v_wk[...])
    keys = keys * lax.rsqrt(jnp.sum(keys * keys, axis=-1, keepdims=True) + EPS)
    values = dot(normed, v_wv[...])
    gates = dot(normed, v_wg[...])
    mine = iota((SEQ, NTP), 1) == t
    beta = jax.nn.sigmoid(jnp.sum(jnp.where(mine, dot(normed, v_wb[...]), 0.0), axis=-1, keepdims=True))
    logit = jnp.sum(jnp.where(mine, dot(normed, v_wd[...]), 0.0), axis=-1, keepdims=True)
    d_scale = jnp.sum(jnp.where(iota((1, NTP), 1) == t, v_dscale[...], 0.0), axis=-1, keepdims=True)
    soft = jnp.maximum(logit, 0.0) + jnp.log(1.0 + jnp.exp(-jnp.abs(logit)))
    decay = jnp.exp(-d_scale * soft)

    loads["state"].wait()
    qb, kb = queries.astype(BF16), keys.astype(BF16)
    diag = iota((16, 1024), 1) // DK == iota((16, 1024), 0) % 8
    by_query, by_key = [], []
    for i in range(SEQ // 8):
        both = jnp.concatenate([qb[8 * i : 8 * i + 8].astype(F32), kb[8 * i : 8 * i + 8].astype(F32)], axis=0)
        lhs = jnp.where(diag, jnp.concatenate([both] * 8, axis=1), 0.0).astype(BF16)
        rhs = v_state[8 * i : 8 * i + 8].reshape(1024, DK).astype(BF16)
        out = dot(lhs, rhs)
        by_query.append(out[:8])
        by_key.append(out[8:])
    s_q = jnp.concatenate(by_query, axis=0)
    s_k = jnp.concatenate(by_key, axis=0)
    match = beta * jnp.sum(queries * keys, axis=-1, keepdims=True)
    read = decay * (s_q - match * s_k) + match * values
    read = read * lax.rsqrt(jnp.mean(read * read, axis=-1, keepdims=True) + EPS) * v_hgain[...]
    heads_all[t] = (read * silu(gates)).astype(BF16)
    for d in (4, 3, 5, 2, 6, 1, 7):
        copy = remote(heads_all.at[t], heads_all.at[t], h_send.at[d - 1], h_recv, tp_peer(d))
        copy.start()
        sends.append(copy)

    update = beta * (values - decay * s_k)
    keys_t = jnp.concatenate([keys, jnp.zeros((DK - SEQ, DK), F32)], axis=0).T
    decay_rows = jnp.broadcast_to(decay, (SEQ, DK))
    for s in range(SEQ):
        v_state[s] = decay_rows[s : s + 1] * v_state[s] + keys_t[:, s : s + 1] * update[s : s + 1]
    state_out = pltpu.make_async_copy(v_state, new_state, out_sem)
    state_out.start()

    loads["wo"].wait()
    take(heads_all.at[pl.ds(0, 7)], h_recv)
    wide = hid_all[t].astype(F32)
    for b in range(NTP):
        wide = wide + dot(heads_all[b], v_wo[b * DK : (b + 1) * DK, :])
    mixed = wide.astype(BF16)
    mixed_s[...] = mixed
    low, high = mixed[:, :128], mixed[:, 128:]

    t_row, t_col = iota((NTP * 8, SEQ), 0), iota((NTP * 8, SEQ), 1)
    pick = t_row // 2 == t_col
    pick_low = jnp.where(pick & (t_row % 2 == 0), 1.0, 0.0).astype(BF16)
    pick_high = jnp.where(pick & (t_row % 2 == 1), 1.0, 0.0).astype(BF16)
    tokens = (dot(pick_low, low) + dot(pick_high, high)).reshape(NTP, 8, 128).astype(BF16)
    own_tok[...] = tokens
    for d in (4, 3, 5, 2, 6, 1, 7):
        to = lax.rem(t + d, NTP)
        copy = remote(own_tok.at[to], dx.at[ep, t], t_send.at[d - 1], t_recv, tp_peer(d))
        copy.start()
        sends.append(copy)
    dx[ep, t] = own_tok[t]

    routed = dot(send_mat[0], low) + dot(send_mat[1], high)
    disp[...] = routed.reshape(NEP, 8, 128).astype(BF16)

    def dispatch(d, carry):
        to = lax.rem(ep + d, NEP)
        remote(disp.at[to], xa.at[t, ep], d_send, d_recv, ep_peer(d)).start()
        return carry

    lax.fori_loop(1, NEP, dispatch, 0)
    xa[t, ep] = disp[ep]

    take(dx.at[0, pl.ds(0, 7)], t_recv)

    def over_x(dz):
        block = lax.rem(z + NZ - dz, NZ) * NX + x
        for d in (2, 1, 3):
            copy = remote(dx.at[block], dx.at[block], x_send.at[d - 1, dz], x_recv.at[d - 1, dz], x_peer(d))
            copy.start()
            sends.append(copy)

    z_copies = {}
    for d in (4, 3, 5, 2, 6, 1, 7):
        copy = remote(dx.at[ep], dx.at[ep], z_send.at[d - 1], z_recv.at[d - 1], z_peer(d))
        copy.start()
        sends.append(copy)
        z_copies[d] = copy
    over_x(0)
    for d in (1, 7, 2, 6):
        z_copies[d].wait_recv()
        over_x(d)

    take(xa.at[0, pl.ds(0, NEP - 1)], d_recv)
    y_copies = {}
    for d in (2, 1, 3):
        copy = remote(xa.at[t], xa.at[t], y_send.at[d - 1], y_recv.at[d - 1], y_peer(d))
        copy.start()
        sends.append(copy)
        y_copies[d] = copy

    c_copies = []

    def across(d):
        slot = lax.rem(y + 4 - d, 4) * 2 + c
        copy = remote(xa.at[slot], xa.at[slot], c_send.at[d], c_recv.at[d], partner)
        copy.start()
        sends.append(copy)
        c_copies.append(copy)

    across(0)
    for d in (3, 5, 4):
        z_copies[d].wait_recv()
        over_x(d)
    for d in (1, 3, 2):
        y_copies[d].wait_recv()
        across(d)

    loads["fgain"].wait()
    for name in ("dg", "du", "dd"):
        loads[name].wait()
    for d in range(1, NX):
        for dz in range(NZ):
            remote(dx.at[0], dx.at[0], x_send.at[d - 1, dz], x_recv.at[d - 1, dz], x_peer(d)).wait_recv()
    for xx in range(NX):
        for zz in range(NZ):
            stage[pl.ds(zz * PITCH, 64), :] = dx[zz * NX + xx].astype(F32).reshape(64, 128)
        square = [jnp.zeros((8, 128), F32) for _ in range(4)]
        for j in range(4):
            for b in range(16):
                part = stage[pl.ds((b // 2) * 8 + j * 2 + b % 2, 8, stride=PITCH), :]
                square[j] = square[j] + part * part
        scales = [lax.rsqrt(jnp.sum(sq, axis=-1, keepdims=True) * (1.0 / D) + EPS) for sq in square]
        for b in range(16):
            cols = slice(b * 128, (b + 1) * 128)
            parts = [
                stage[pl.ds((b // 2) * 8 + j * 2 + b % 2, 8, stride=PITCH), :] * scales[j] * v_fgain[:, cols]
                for j in range(4)
            ]
            xn_d[xx * 32 : (xx + 1) * 32, cols] = jnp.concatenate(parts, axis=0).astype(BF16)
    rows_d = xn_d[...]
    hidden_d = (silu(dot(rows_d, v_dg[...])) * dot(rows_d, v_du[...])).astype(BF16)
    wide_f = D // CHUNKS
    for f in range(CHUNKS):
        out = dot(hidden_d, v_dd[:, f * wide_f : (f + 1) * wide_f]).astype(BF16)
        for xx in range(NX):
            px[xx, f] = out[xx * 32 : (xx + 1) * 32]
    u_copies = {}
    for f in range(CHUNKS):
        for d in (2, 1, 3):
            copy = remote(
                px.at[lax.rem(x + d, NX), f], xr.at[d - 1, f], u_send.at[d - 1, f], u_recv.at[d - 1, f], x_peer(d)
            )
            copy.start()
            sends.append(copy)
            u_copies[d, f] = copy

    for name in ("eg", "eu", "ed"):
        loads[name].wait()
    for copy in c_copies:
        copy.wait_recv()
    square = jnp.zeros((ROWS, 128), F32)
    for b in range(NTP):
        stage[pl.ds(0, 256), :] = xa[b].astype(F32).reshape(256, 128)
        for h in range(2):
            part = stage[pl.ds(h, ROWS, stride=2), :]
            square = square + part * part
            xn_e[:, b * WIDTH + h * 128 : b * WIDTH + (h + 1) * 128] = part.astype(BF16)
    scale = lax.rsqrt(jnp.sum(square, axis=-1, keepdims=True) * (1.0 / D) + EPS)
    for b in range(NTP):
        cols = slice(b * WIDTH, (b + 1) * WIDTH)
        xn_e[:, cols] = (xn_e[:, cols].astype(F32) * scale * v_fgain[:, cols]).astype(BF16)
    rows_e = xn_e[...]
    inner_s[...] = (silu(dot(rows_e, v_eg[...])) * dot(rows_e, v_eu[...])).astype(BF16)
    inner = inner_s[...]
    for b in range(NTP):
        pb[b] = dot(inner, v_ed[:, b * WIDTH : (b + 1) * WIDTH]).astype(BF16)
    p_copies = {}
    for d in (2, 1, 3, 0):
        there = lax.rem(y + d, 4)
        copy = remote(pb.at[there * 2 + 1 - c], pr.at[there], p_send.at[d], p_recv.at[d], partner)
        copy.start()
        sends.append(copy)
        p_copies[d] = copy
    q_copies = {}
    for d in (2, 1, 3, 0):
        there = lax.rem(y + d, 4)
        p_copies[d].wait_recv()
        qs[there] = (pb[there * 2 + c].astype(F32) + pr[there].astype(F32)).astype(BF16)
        if d > 0:
            copy = remote(qs.at[there], yr.at[d - 1], q_send.at[d - 1], q_recv.at[d - 1], y_peer(d))
            copy.start()
            sends.append(copy)
            q_copies[d] = copy

    def sum_x(f):
        for d in (1, 3, 2):
            u_copies[d, f].wait_recv()
        total = px[x, f].astype(F32)
        for d in range(3):
            total = total + xr[d, f].astype(F32)
        for tt in range(2):
            for h in range(2):
                cols = slice(tt * WIDTH + h * 128, tt * WIDTH + (h + 1) * 128)
                for j in range(4):
                    stage[pl.ds(tt * 8 + j * 2 + h, 8, stride=PITCH), :] = total[j * 8 : (j + 1) * 8, cols]
        for zz in range(NZ):
            zs[zz, 2 * f : 2 * f + 2] = stage[pl.ds(zz * PITCH, 16), :].reshape(2, 8, 128).astype(BF16)
        for d in (4, 3, 5, 2, 6, 1, 7):
            to = lax.rem(z + d, NZ)
            copy = remote(
                zs.at[to, pl.ds(2 * f, 2)], zr.at[d - 1, pl.ds(2 * f, 2)], w_send.at[d - 1, f], w_recv.at[f], z_peer(d)
            )
            copy.start()
            sends.append(copy)

    for f in range(CHUNKS):
        sum_x(f)

    for d in (1, 3, 2):
        q_copies[d].wait_recv()
    total = qs[y].astype(F32)
    for d in range(3):
        total = total + yr[d].astype(F32)
    total = total.astype(BF16).astype(F32)
    for h in range(2):
        stage[pl.ds(h, ROWS, stride=2), :] = total[:, h * 128 : (h + 1) * 128]
    ret[...] = stage[pl.ds(0, 256), :].reshape(NEP, 8, 128).astype(BF16)

    def give_back(d, carry):
        to = lax.rem(ep + d, NEP)
        remote(ret.at[to], rb.at[ep], b_send, b_recv, ep_peer(d)).start()
        return carry

    lax.fori_loop(1, NEP, give_back, 0)
    rb[ep] = ret[ep]

    for f in range(CHUNKS):
        take(zr.at[:, pl.ds(2 * f, 2)], w_recv.at[f])
    total = zs[z].astype(F32)
    for d in range(NZ - 1):
        total = total + zr[d].astype(F32)
    fs[...] = total.astype(BF16)
    for d in (4, 3, 5, 2, 6, 1, 7):
        to = lax.rem(t + d, NTP)
        copy = remote(fs.at[to], fr.at[t], f_send.at[d - 1], f_recv, tp_peer(d))
        copy.start()
        sends.append(copy)
    fr[t] = fs[t]

    loads["mix"].wait()
    take(rb.at[pl.ds(0, NEP - 1)], b_recv)
    back = rb[...].astype(F32).reshape(NEP * 8, 128).astype(BF16)
    moe = []
    for h in range(2):
        moe.append(dot(take_mat[2 * h], back) + dot(take_mat[2 * h + 1], back))
    take(fr.at[pl.ds(0, 7)], f_recv)
    stage[pl.ds(0, 64), :] = fr[...].astype(F32).reshape(64, 128)
    for h in range(2):
        cols = slice(h * 128, (h + 1) * 128)
        dense = stage[pl.ds(h, SEQ, stride=2), :]
        result[:, cols] = (
            mixed_s[:, cols].astype(F32) + moe[h] + jax.nn.sigmoid(v_mix[:, cols]) * dense
        ).astype(BF16)

    for copy in sends:
        copy.wait_send()
    take(disp.at[pl.ds(0, NEP - 1)], d_send)
    take(ret.at[pl.ds(0, NEP - 1)], b_send)
    state_out.wait()


def per_device(
    hidden_in, state_in, attn_gain, w_query, w_key, w_value, w_gate, w_beta, w_decay, decay_scale, head_gain, w_output,
    ffn_gain, expert_ids, route_weight, expert_gate, expert_up, expert_down, dense_gate, dense_up, dense_down, dense_mix,
):
    operands = (
        hidden_in, state_in.reshape(SEQ, DK, DK), attn_gain.reshape(1, D), w_query, w_key, w_value, w_gate, w_beta,
        w_decay, decay_scale.reshape(1, NTP), head_gain.reshape(1, DK), w_output, ffn_gain.reshape(1, D), expert_ids,
        route_weight, expert_gate[0], expert_up[0], expert_down[0], dense_gate, dense_up, dense_down,
        dense_mix.reshape(1, WIDTH),
    )
    V = pltpu.VMEM
    vmem_of = [V((NTP, SEQ, WIDTH), BF16)] + [V(o.shape, o.dtype) for o in operands[1:]]
    dma = pltpu.SemaphoreType.DMA
    scratch = vmem_of + [
        V((SEQ, D), BF16), V((NTP, SEQ, DK), BF16), V((SEQ, WIDTH), BF16),
        V((2, NEP * 8, SEQ), BF16), V((4, SEQ, NEP * 8), BF16),
        V((NEP, 8, 128), BF16), V((NTP, NEP, 8, 128), BF16), V((NZ * PITCH, 128), F32), V((ROWS, D), BF16),
        V((ROWS, FE), BF16), V((NTP, ROWS, WIDTH), BF16), V((4, ROWS, WIDTH), BF16), V((4, ROWS, WIDTH), BF16),
        V((3, ROWS, WIDTH), BF16), V((NEP, 8, 128), BF16), V((NEP, 8, 128), BF16),
        V((NTP, 8, 128), BF16), V((NEP, NTP, 8, 128), BF16), V((ROWS, D), BF16),
        V((NX, CHUNKS, 32, D // CHUNKS), BF16), V((3, CHUNKS, 32, D // CHUNKS), BF16),
        V((NZ, NTP, 8, 128), BF16), V((NZ - 1, NTP, 8, 128), BF16), V((NTP, 8, 128), BF16), V((NTP, 8, 128), BF16),
        dma((22,)), dma,
        dma((7,)), dma, dma((7,)), dma, dma((7,)), dma, dma, dma, dma((7,)), dma((7,)), dma((3, 8)), dma((3, 8)),
        dma((3,)), dma((3,)), dma((4,)), dma((4,)), dma((4,)), dma((4,)), dma((3,)), dma((3,)), dma, dma,
        dma((3, CHUNKS)), dma((3, CHUNKS)), dma((7, CHUNKS)), dma((CHUNKS,)), dma((7,)), dma,
    ]
    result, new_state = pl.pallas_call(
        kernel,
        out_shape=(
            jax.ShapeDtypeStruct((SEQ, WIDTH), BF16),
            jax.ShapeDtypeStruct((SEQ, DK, DK), F32),
        ),
        in_specs=[pl.BlockSpec(memory_space=pl.ANY)] * len(operands),
        out_specs=(pl.BlockSpec(memory_space=pltpu.VMEM), pl.BlockSpec(memory_space=pl.ANY)),
        scratch_shapes=scratch,
        compiler_params=pltpu.CompilerParams(
            collective_id=0, has_side_effects=True, vmem_limit_bytes=56 * 1024 * 1024
        ),
    )(*operands)
    return result, new_state.reshape(state_in.shape)


def solution(mesh):
    return jax.shard_map(
        per_device,
        mesh=mesh,
        in_specs=(
            P("ep", "tp"), P("ep", "tp", None, None), P(), P(None, "tp"), P(None, "tp"), P(None, "tp"), P(None, "tp"),
            P(), P(), P(), P(), P(None, "tp"), P(), P("ep", None), P("ep", None), P("ep", None, "tp"),
            P("ep", None, "tp"), P("ep", "tp", None), P(None, "ep"), P(None, "ep"), P("ep", None), P("tp"),
        ),
        out_specs=(P("ep", "tp"), P("ep", "tp", None, None)),
        check_vma=False,
    )
```

```python
import functools

import jax
import jax.numpy as jnp
from jax import lax
from jax.experimental import pallas as pl
from jax.experimental.pallas import tpu as pltpu
from jax.sharding import PartitionSpec as P

EPS = 1e-06
MESH = pl.DeviceIdType.MESH
F32, BF16, I32 = jnp.float32, jnp.bfloat16, jnp.int32

NX, NZ, NTP, NEP = 4, 8, 8, 32
SEQ, D, WIDTH, DK, CAP = 32, 2048, 256, 128, 4
ROWS = NEP * CAP
FE, FD = 384, 128
PITCH = 72
CHUNKS = 4


def silu(v):
    return v * jax.nn.sigmoid(v)


def dot(a, b):
    return jnp.dot(a, b, preferred_element_type=F32)


def dot_t(a, b):
    return lax.dot_general(a, b, (((1,), (1,)), ((), ())), preferred_element_type=F32)


def t_dot(a, b):
    return lax.dot_general(a, b, (((0,), (0,)), ((), ())), preferred_element_type=F32)


def iota(shape, dim):
    return lax.broadcasted_iota(I32, shape, dim)


def kernel(
    hidden, state, attn_gain, wq, wk, wv, wg, w_beta, w_decay, decay_scale, head_gain, w_out, ffn_gain, ids, route,
    eg, eu, ed, dg, du, dd, mix,
    result, new_state,
    hid_all, v_state, v_again, v_wq, v_wk, v_wv, v_wg, v_wb, v_wd, v_dscale, v_hgain, v_wo, v_fgain, v_ids, v_route,
    v_eg, v_eu, v_ed, v_dg, v_du, v_dd, v_mix,
    xn_a, heads_all, mixed_s, send_mat, take_mat,
    disp, xa, stage, xn_e, inner_s, pb, pr, qs, yr, ret, rb,
    own_tok, dx, xn_d, px, xr, zs, zr, fs, fr,
    l_sem,
    a_send, a_recv, h_send, h_recv, t_send, t_recv, d_send, d_recv, z_send, z_recv, x_send, x_recv,
    y_send, y_recv, c_send, c_recv, p_send, p_recv, q_send, q_recv, b_send, b_recv,
    u_send, u_recv, w_send, w_recv, f_send, f_recv, met,
):
    ep = lax.axis_index("ep")
    t = lax.axis_index("tp")
    z, x = lax.div(ep, NX), lax.rem(ep, NX)
    y, c = lax.div(t, 2), lax.rem(t, 2)

    def tp_peer(d):
        return ep, lax.rem(t + d, NTP)

    def ep_peer(d):
        return lax.rem(ep + d, NEP), t

    def z_peer(d):
        return lax.rem(z + d, NZ) * NX + x, t

    def x_peer(d):
        return z * NX + lax.rem(x + d, NX), t

    def y_peer(d):
        return ep, lax.rem(y + d, 4) * 2 + c

    partner = (ep, y * 2 + 1 - c)

    def remote(src, dst, send, recv, peer):
        return pltpu.make_async_remote_copy(
            src_ref=src, dst_ref=dst, send_sem=send, recv_sem=recv, device_id=peer, device_id_type=MESH
        )

    def take(view, sem):
        pltpu.make_async_copy(view, view, sem).wait()

    loads = {}
    pairs = (
        ("hid", hidden, hid_all.at[t]), ("ids", ids, v_ids), ("route", route, v_route), ("again", attn_gain, v_again),
        ("wq", wq, v_wq), ("wk", wk, v_wk), ("wv", wv, v_wv), ("wg", wg, v_wg), ("wb", w_beta, v_wb),
        ("wd", w_decay, v_wd), ("dscale", decay_scale, v_dscale), ("hgain", head_gain, v_hgain),
        ("state", state, v_state), ("wo", w_out, v_wo), ("fgain", ffn_gain, v_fgain), ("mix", mix, v_mix),
        ("dg", dg, v_dg), ("du", du, v_du), ("dd", dd, v_dd), ("eg", eg, v_eg), ("eu", eu, v_eu), ("ed", ed, v_ed),
    )
    for number, (name, src, dst) in enumerate(pairs):
        loads[name] = pltpu.make_async_copy(src, dst, l_sem.at[number])
        loads[name].start()

    barrier = pltpu.get_barrier_semaphore()
    near = [tp_peer(d) for d in range(1, NTP)] + [z_peer(1), z_peer(NZ - 1), x_peer(1), x_peer(NX - 1)]
    for peer in near:
        pl.semaphore_signal(barrier, inc=1, device_id=peer, device_id_type=MESH)

    def tell(number, peers):
        for peer in peers:
            pl.semaphore_signal(met.at[number], inc=1, device_id=peer, device_id_type=MESH)

    loads["ids"].wait()
    loads["route"].wait()
    first, second = v_ids[0:1, :], v_ids[1:2, :]
    expert = iota((NEP, SEQ), 0)
    is_first, is_second = first == expert, second == expert
    chosen = jnp.where(is_first | is_second, 1.0, 0.0)
    earlier = jnp.where(iota((SEQ, SEQ), 0) < iota((SEQ, SEQ), 1), 1.0, 0.0).astype(BF16)
    before = dot(chosen.astype(BF16), earlier)
    place = (chosen * (before + 1.0)).astype(BF16)
    row = iota((NEP * 8, NEP), 0)
    spread = jnp.where(row // 8 == iota((NEP * 8, NEP), 1), 1.0, 0.0).astype(BF16)
    hit = dot(spread, place) == ((row % 8) // 2 + 1).astype(F32)
    weight = jnp.where(is_first, v_route[0:1, :], 0.0) + jnp.where(is_second, v_route[1:2, :], 0.0)
    coarse = weight.astype(BF16)
    fine = (weight - coarse.astype(F32)).astype(BF16)
    coarse, fine = dot(spread, coarse), dot(spread, fine)
    for h in range(2):
        here = hit & (row % 2 == h)
        send_mat[h] = jnp.where(here, 1.0, 0.0).astype(BF16)
        take_mat[2 * h] = jnp.where(here, coarse, 0.0).astype(BF16)
        take_mat[2 * h + 1] = jnp.where(here, fine, 0.0).astype(BF16)

    loads["hid"].wait()
    pl.semaphore_wait(barrier, len(near))

    copies = []
    for d in (4, 3, 5, 2, 6, 1, 7):
        copy = remote(hid_all.at[t], hid_all.at[t], a_send.at[d - 1], a_recv, tp_peer(d))
        copy.start()
        copies.append(copy)
    sends = copies
    tell(0, (z_peer(1), z_peer(NZ - 1), x_peer(1), x_peer(NX - 1)))
    loads["again"].wait()
    take(hid_all.at[pl.ds(0, 7)], a_recv)

    pl.semaphore_wait(met.at[0], 4)
    tell(1, (z_peer(2), z_peer(NZ - 2)))
    square = jnp.zeros((SEQ, WIDTH), F32)
    for b in range(NTP):
        wide = hid_all[b].astype(F32)
        square = square + wide * wide
    scale = lax.rsqrt(jnp.sum(square, axis=-1, keepdims=True) * (1.0 / D) + EPS)
    for b in range(NTP):
        cols = slice(b * WIDTH, (b + 1) * WIDTH)
        xn_a[:, cols] = (hid_all[b].astype(F32) * scale * v_again[:, cols]).astype(BF16)
    for name in ("wq", "wk", "wv", "wg", "wb", "wd", "dscale", "hgain"):
        loads[name].wait()
    normed = xn_a[...]
    queries = dot(normed, v_wq[...])
    queries = queries * lax.rsqrt(jnp.sum(queries * queries, axis=-1, keepdims=True) + EPS) * DK ** (-0.5)
    keys = dot(normed, v_wk[...])
    keys = keys * lax.rsqrt(jnp.sum(keys * keys, axis=-1, keepdims=True) + EPS)
    values = dot(normed, v_wv[...])
    gates = dot(normed, v_wg[...])
    mine = iota((SEQ, NTP), 1) == t
    beta = jax.nn.sigmoid(jnp.sum(jnp.where(mine, dot_t(normed, v_wb[...]), 0.0), axis=-1, keepdims=True))
    logit = jnp.sum(jnp.where(mine, dot_t(normed, v_wd[...]), 0.0), axis=-1, keepdims=True)
    d_scale = jnp.sum(jnp.where(iota((1, NTP), 1) == t, v_dscale[...], 0.0), axis=-1, keepdims=True)
    soft = jnp.maximum(logit, 0.0) + jnp.log(1.0 + jnp.exp(-jnp.abs(logit)))
    decay = jnp.exp(-d_scale * soft)

    loads["state"].wait()
    qb, kb = queries.astype(BF16), keys.astype(BF16)
    diag = iota((16, 1024), 1) // DK == iota((16, 1024), 0) % 8
    by_query, by_key = [], []
    for i in range(SEQ // 8):
        both = jnp.concatenate([qb[8 * i : 8 * i + 8].astype(F32), kb[8 * i : 8 * i + 8].astype(F32)], axis=0)
        lhs = jnp.where(diag, jnp.concatenate([both] * 8, axis=1), 0.0).astype(BF16)
        rhs = v_state[8 * i : 8 * i + 8].reshape(1024, DK).astype(BF16)
        out = dot(lhs, rhs)
        by_query.append(out[:8])
        by_key.append(out[8:])
    s_q = jnp.concatenate(by_query, axis=0)
    s_k = jnp.concatenate(by_key, axis=0)
    match = beta * jnp.sum(queries * keys, axis=-1, keepdims=True)
    read = decay * (s_q - match * s_k) + match * values
    read = read * lax.rsqrt(jnp.mean(read * read, axis=-1, keepdims=True) + EPS) * v_hgain[...]
    heads_all[t] = (read * silu(gates)).astype(BF16)
    for d in (4, 3, 5, 2, 6, 1, 7):
        copy = remote(heads_all.at[t], heads_all.at[t], h_send.at[d - 1], h_recv, tp_peer(d))
        copy.start()
        sends.append(copy)

    pl.semaphore_wait(met.at[1], 2)
    tell(2, (x_peer(1), x_peer(2), x_peer(3)))
    update = beta * (values - decay * s_k)
    keys_t = jnp.concatenate([keys, jnp.zeros((DK - SEQ, DK), F32)], axis=0).T
    decay_rows = jnp.broadcast_to(decay, (SEQ, DK))
    for s in range(SEQ):
        new_state[s] = decay_rows[s : s + 1] * v_state[s] + keys_t[:, s : s + 1] * update[s : s + 1]

    pl.semaphore_wait(met.at[2], 3)
    loads["wo"].wait()
    take(heads_all.at[pl.ds(0, 7)], h_recv)
    wide = hid_all[t].astype(F32)
    for b in range(NTP):
        wide = wide + dot(heads_all[b], v_wo[b * DK : (b + 1) * DK, :])
    mixed = wide.astype(BF16)
    mixed_s[...] = mixed
    low, high = mixed[:, :128], mixed[:, 128:]

    t_row, t_col = iota((NTP * 8, SEQ), 0), iota((NTP * 8, SEQ), 1)
    pick = t_row // 2 == t_col
    pick_low = jnp.where(pick & (t_row % 2 == 0), 1.0, 0.0).astype(BF16)
    pick_high = jnp.where(pick & (t_row % 2 == 1), 1.0, 0.0).astype(BF16)
    tokens = (dot(pick_low, low) + dot(pick_high, high)).reshape(NTP, 8, 128).astype(BF16)
    own_tok[...] = tokens
    for d in (4, 3, 5, 2, 6, 1, 7):
        to = lax.rem(t + d, NTP)
        copy = remote(own_tok.at[to], dx.at[ep, t], t_send.at[d - 1], t_recv, tp_peer(d))
        copy.start()
        sends.append(copy)
    dx[ep, t] = own_tok[t]

    routed = dot(send_mat[0], low) + dot(send_mat[1], high)
    disp[...] = routed.reshape(NEP, 8, 128).astype(BF16)

    def dispatch(d, carry):
        to = lax.rem(ep + d, NEP)
        remote(disp.at[to], xa.at[t, ep], d_send, d_recv, ep_peer(d)).start()
        return carry

    lax.fori_loop(1, NEP, dispatch, 0)
    xa[t, ep] = disp[ep]

    take(dx.at[0, pl.ds(0, 7)], t_recv)

    def over_x(dz):
        block = lax.rem(z + NZ - dz, NZ) * NX + x
        for d in (2, 1, 3):
            copy = remote(dx.at[block], dx.at[block], x_send.at[d - 1, dz], x_recv.at[d - 1, dz], x_peer(d))
            copy.start()
            sends.append(copy)

    z_copies = {}
    for d in (4, 3, 5, 2, 6, 1, 7):
        copy = remote(dx.at[ep], dx.at[ep], z_send.at[d - 1], z_recv.at[d - 1], z_peer(d))
        copy.start()
        sends.append(copy)
        z_copies[d] = copy
    over_x(0)
    for d in (1, 7, 2, 6):
        z_copies[d].wait_recv()
        over_x(d)

    take(xa.at[0, pl.ds(0, NEP - 1)], d_recv)
    y_copies = {}
    for d in (2, 1, 3):
        copy = remote(xa.at[t], xa.at[t], y_send.at[d - 1], y_recv.at[d - 1], y_peer(d))
        copy.start()
        sends.append(copy)
        y_copies[d] = copy

    c_copies = []

    def across(d):
        slot = lax.rem(y + 4 - d, 4) * 2 + c
        copy = remote(xa.at[slot], xa.at[slot], c_send.at[d], c_recv.at[d], partner)
        copy.start()
        sends.append(copy)
        c_copies.append(copy)

    across(0)
    for d in (3, 5, 4):
        z_copies[d].wait_recv()
        over_x(d)
    for d in (1, 3, 2):
        y_copies[d].wait_recv()
        across(d)

    loads["fgain"].wait()
    for name in ("dg", "du", "dd"):
        loads[name].wait()
    for d in range(1, NX):
        for dz in range(NZ):
            remote(dx.at[0], dx.at[0], x_send.at[d - 1, dz], x_recv.at[d - 1, dz], x_peer(d)).wait_recv()
    for xx in range(NX):
        for zz in range(NZ):
            stage[pl.ds(zz * PITCH, 64), :] = dx[zz * NX + xx].astype(F32).reshape(64, 128)
        square = [jnp.zeros((8, 128), F32) for _ in range(4)]
        for j in range(4):
            for b in range(16):
                part = stage[pl.ds((b // 2) * 8 + j * 2 + b % 2, 8, stride=PITCH), :]
                square[j] = square[j] + part * part
        scales = [lax.rsqrt(jnp.sum(sq, axis=-1, keepdims=True) * (1.0 / D) + EPS) for sq in square]
        for b in range(16):
            cols = slice(b * 128, (b + 1) * 128)
            parts = [
                stage[pl.ds((b // 2) * 8 + j * 2 + b % 2, 8, stride=PITCH), :] * scales[j] * v_fgain[:, cols]
                for j in range(4)
            ]
            xn_d[xx * 32 : (xx + 1) * 32, cols] = jnp.concatenate(parts, axis=0).astype(BF16)
    rows_d = xn_d[...]
    hidden_d = (silu(dot(rows_d, v_dg[...])) * dot(rows_d, v_du[...])).astype(BF16)
    wide_f = D // CHUNKS
    for f in range(CHUNKS):
        out = dot(hidden_d, v_dd[:, f * wide_f : (f + 1) * wide_f]).astype(BF16)
        for xx in range(NX):
            px[xx, f] = out[xx * 32 : (xx + 1) * 32]
    u_copies = {}
    for f in range(CHUNKS):
        for d in (2, 1, 3):
            copy = remote(
                px.at[lax.rem(x + d, NX), f], xr.at[d - 1, f], u_send.at[d - 1, f], u_recv.at[d - 1, f], x_peer(d)
            )
            copy.start()
            sends.append(copy)
            u_copies[d, f] = copy

    for name in ("eg", "eu", "ed"):
        loads[name].wait()
    for copy in c_copies:
        copy.wait_recv()
    square = jnp.zeros((ROWS, 128), F32)
    for b in range(NTP):
        stage[pl.ds(0, 256), :] = xa[b].astype(F32).reshape(256, 128)
        for h in range(2):
            part = stage[pl.ds(h, ROWS, stride=2), :]
            square = square + part * part
            xn_e[:, b * WIDTH + h * 128 : b * WIDTH + (h + 1) * 128] = part.astype(BF16)
    scale = lax.rsqrt(jnp.sum(square, axis=-1, keepdims=True) * (1.0 / D) + EPS)
    for b in range(NTP):
        cols = slice(b * WIDTH, (b + 1) * WIDTH)
        xn_e[:, cols] = (xn_e[:, cols].astype(F32) * scale * v_fgain[:, cols]).astype(BF16)
    rows_e = xn_e[...]
    inner_s[...] = (silu(dot(rows_e, v_eg[...])) * dot(rows_e, v_eu[...])).astype(BF16)
    inner = inner_s[...]
    for b in range(NTP):
        pb[b] = dot(inner, v_ed[:, b * WIDTH : (b + 1) * WIDTH]).astype(BF16)
    p_copies = {}
    for d in (2, 1, 3, 0):
        there = lax.rem(y + d, 4)
        copy = remote(pb.at[there * 2 + 1 - c], pr.at[there], p_send.at[d], p_recv.at[d], partner)
        copy.start()
        sends.append(copy)
        p_copies[d] = copy
    q_copies = {}
    for d in (2, 1, 3, 0):
        there = lax.rem(y + d, 4)
        p_copies[d].wait_recv()
        qs[there] = (pb[there * 2 + c].astype(F32) + pr[there].astype(F32)).astype(BF16)
        if d > 0:
            copy = remote(qs.at[there], yr.at[d - 1], q_send.at[d - 1], q_recv.at[d - 1], y_peer(d))
            copy.start()
            sends.append(copy)
            q_copies[d] = copy

    def sum_x(f):
        for d in (1, 3, 2):
            u_copies[d, f].wait_recv()
        total = px[x, f].astype(F32)
        for d in range(3):
            total = total + xr[d, f].astype(F32)
        for tt in range(2):
            for h in range(2):
                cols = slice(tt * WIDTH + h * 128, tt * WIDTH + (h + 1) * 128)
                for j in range(4):
                    stage[pl.ds(tt * 8 + j * 2 + h, 8, stride=PITCH), :] = total[j * 8 : (j + 1) * 8, cols]
        for zz in range(NZ):
            zs[zz, 2 * f : 2 * f + 2] = stage[pl.ds(zz * PITCH, 16), :].reshape(2, 8, 128).astype(BF16)
        for d in (4, 3, 5, 2, 6, 1, 7):
            to = lax.rem(z + d, NZ)
            copy = remote(
                zs.at[to, pl.ds(2 * f, 2)], zr.at[d - 1, pl.ds(2 * f, 2)], w_send.at[d - 1, f], w_recv.at[f], z_peer(d)
            )
            copy.start()
            sends.append(copy)

    for f in range(CHUNKS):
        sum_x(f)

    for d in (1, 3, 2):
        q_copies[d].wait_recv()
    total = qs[y].astype(F32)
    for d in range(3):
        total = total + yr[d].astype(F32)
    total = total.astype(BF16).astype(F32)
    for h in range(2):
        stage[pl.ds(h, ROWS, stride=2), :] = total[:, h * 128 : (h + 1) * 128]
    ret[...] = stage[pl.ds(0, 256), :].reshape(NEP, 8, 128).astype(BF16)

    def give_back(d, carry):
        to = lax.rem(ep + d, NEP)
        remote(ret.at[to], rb.at[ep], b_send, b_recv, ep_peer(d)).start()
        return carry

    lax.fori_loop(1, NEP, give_back, 0)
    rb[ep] = ret[ep]

    for f in range(CHUNKS):
        take(zr.at[:, pl.ds(2 * f, 2)], w_recv.at[f])
    total = zs[z].astype(F32)
    for d in range(NZ - 1):
        total = total + zr[d].astype(F32)
    fs[...] = total.astype(BF16)
    for d in (4, 3, 5, 2, 6, 1, 7):
        to = lax.rem(t + d, NTP)
        copy = remote(fs.at[to], fr.at[t], f_send.at[d - 1], f_recv, tp_peer(d))
        copy.start()
        sends.append(copy)
    fr[t] = fs[t]

    loads["mix"].wait()
    take(rb.at[pl.ds(0, NEP - 1)], b_recv)
    back = rb[...].astype(F32).reshape(NEP * 8, 128).astype(BF16)
    moe = []
    for h in range(2):
        moe.append(t_dot(take_mat[2 * h], back) + t_dot(take_mat[2 * h + 1], back))
    take(fr.at[pl.ds(0, 7)], f_recv)
    stage[pl.ds(0, 64), :] = fr[...].astype(F32).reshape(64, 128)
    for h in range(2):
        cols = slice(h * 128, (h + 1) * 128)
        dense = stage[pl.ds(h, SEQ, stride=2), :]
        result[:, cols] = (
            mixed_s[:, cols].astype(F32) + moe[h] + jax.nn.sigmoid(v_mix[:, cols]) * dense
        ).astype(BF16)

    for copy in sends:
        copy.wait_send()
    take(disp.at[pl.ds(0, NEP - 1)], d_send)
    take(ret.at[pl.ds(0, NEP - 1)], b_send)


def write_out(result, new_state, result_out, state_out, sem):
    first = pltpu.make_async_copy(result, result_out, sem.at[0])
    second = pltpu.make_async_copy(new_state, state_out, sem.at[1])
    first.start()
    second.start()
    first.wait()
    second.wait()


def per_device(
    hidden_in, state_in, attn_gain, w_query, w_key, w_value, w_gate, w_beta, w_decay, decay_scale, head_gain, w_output,
    ffn_gain, expert_ids, route_weight, expert_gate, expert_up, expert_down, dense_gate, dense_up, dense_down, dense_mix,
):
    operands = (
        hidden_in, state_in.reshape(SEQ, DK, DK), attn_gain.reshape(1, D), w_query, w_key, w_value, w_gate, w_beta.T,
        w_decay.T, decay_scale.reshape(1, NTP), head_gain.reshape(1, DK), w_output, ffn_gain.reshape(1, D), expert_ids.T,
        route_weight.T, expert_gate[0], expert_up[0], expert_down[0], dense_gate, dense_up, dense_down,
        dense_mix.reshape(1, WIDTH),
    )
    V = pltpu.VMEM
    vmem_of = [V((NTP, SEQ, WIDTH), BF16)] + [V(o.shape, o.dtype) for o in operands[1:]]
    dma = pltpu.SemaphoreType.DMA
    scratch = vmem_of + [
        V((SEQ, D), BF16), V((NTP, SEQ, DK), BF16), V((SEQ, WIDTH), BF16),
        V((2, NEP * 8, SEQ), BF16), V((4, NEP * 8, SEQ), BF16),
        V((NEP, 8, 128), BF16), V((NTP, NEP, 8, 128), BF16), V((NZ * PITCH, 128), F32), V((ROWS, D), BF16),
        V((ROWS, FE), BF16), V((NTP, ROWS, WIDTH), BF16), V((4, ROWS, WIDTH), BF16), V((4, ROWS, WIDTH), BF16),
        V((3, ROWS, WIDTH), BF16), V((NEP, 8, 128), BF16), V((NEP, 8, 128), BF16),
        V((NTP, 8, 128), BF16), V((NEP, NTP, 8, 128), BF16), V((ROWS, D), BF16),
        V((NX, CHUNKS, 32, D // CHUNKS), BF16), V((3, CHUNKS, 32, D // CHUNKS), BF16),
        V((NZ, NTP, 8, 128), BF16), V((NZ - 1, NTP, 8, 128), BF16), V((NTP, 8, 128), BF16), V((NTP, 8, 128), BF16),
        dma((22,)),
        dma((7,)), dma, dma((7,)), dma, dma((7,)), dma, dma, dma, dma((7,)), dma((7,)), dma((3, 8)), dma((3, 8)),
        dma((3,)), dma((3,)), dma((4,)), dma((4,)), dma((4,)), dma((4,)), dma((3,)), dma((3,)), dma, dma,
        dma((3, CHUNKS)), dma((3, CHUNKS)), dma((7, CHUNKS)), dma((CHUNKS,)), dma((7,)), dma,
        pltpu.SemaphoreType.REGULAR((3,)),
    ]
    kept = (V((SEQ, WIDTH), BF16), V((SEQ, DK, DK), F32))
    result, new_state = pl.pallas_call(
        kernel,
        out_shape=kept,
        in_specs=[pl.BlockSpec(memory_space=pltpu.HBM)] * len(operands),
        out_specs=tuple(pl.BlockSpec(memory_space=pltpu.VMEM) for _ in kept),
        scratch_shapes=scratch,
        compiler_params=pltpu.CompilerParams(
            collective_id=0, has_side_effects=True, vmem_limit_bytes=64000000
        ),
    )(*operands)
    result, new_state = pl.pallas_call(
        write_out,
        out_shape=tuple(jax.ShapeDtypeStruct(k.shape, k.dtype) for k in kept),
        in_specs=[pl.BlockSpec(memory_space=pltpu.VMEM)] * 2,
        out_specs=tuple(pl.BlockSpec(memory_space=pltpu.HBM) for _ in kept),
        scratch_shapes=[dma((2,))],
        compiler_params=pltpu.CompilerParams(vmem_limit_bytes=8 * 1024 * 1024),
    )(result, new_state)
    return result, new_state.reshape(state_in.shape)


def solution(mesh):
    return jax.shard_map(
        per_device,
        mesh=mesh,
        in_specs=(
            P("ep", "tp"), P("ep", "tp", None, None), P(), P(None, "tp"), P(None, "tp"), P(None, "tp"), P(None, "tp"),
            P(), P(), P(), P(), P(None, "tp"), P(), P("ep", None), P("ep", None), P("ep", None, "tp"),
            P("ep", None, "tp"), P("ep", "tp", None), P(None, "ep"), P(None, "ep"), P("ep", None), P("tp"),
        ),
        out_specs=(P("ep", "tp"), P("ep", "tp", None, None)),
        check_vma=False,
    )
```

```python
import functools

import jax
import jax.numpy as jnp
from jax import lax
from jax.experimental import pallas as pl
from jax.experimental.pallas import tpu as pltpu
from jax.sharding import PartitionSpec as P

EPS = 1e-06
MESH = pl.DeviceIdType.MESH
F32, BF16, I32 = jnp.float32, jnp.bfloat16, jnp.int32

NX, NZ, NTP, NEP = 4, 8, 8, 32
SEQ, D, WIDTH, DK, CAP = 32, 2048, 256, 128, 4
ROWS = NEP * CAP
FE, FD = 384, 128
PITCH = 72
CHUNKS = 4
WIDE = D // CHUNKS
FAR_TP = FAR_Z = (4, 3, 5, 2, 6, 1, 7)


def silu(v):
    return v * jax.nn.sigmoid(v)


def dot(a, b):
    return jnp.dot(a, b, preferred_element_type=F32)


def dot_t(a, b):
    return lax.dot_general(a, b, (((1,), (1,)), ((), ())), preferred_element_type=F32)


def t_dot(a, b):
    return lax.dot_general(a, b, (((0,), (0,)), ((), ())), preferred_element_type=F32)


def iota(shape, dim):
    return lax.broadcasted_iota(I32, shape, dim)


def kernel(
    hidden, state, attn_gain, wq, wk, wv, wg, w_beta, w_decay, decay_scale, head_gain, w_out, ffn_gain, ids, route,
    eg, eu, ed, dg, du, dd, mix,
    result, new_state,
    hid_all, v_state, v_again, v_wq, v_wk, v_wv, v_wg, v_wb, v_wd, v_dscale, v_hgain, v_wo, v_fgain, v_ids, v_route,
    v_eg, v_eu, v_ed, v_dg, v_du, v_dd, v_mix,
    xn_a, heads_all, mixed_s, send_mat, take_mat,
    disp, xa, stage, xn_e, inner_s, pb, pr, qs, yr, ret, rb,
    own_tok, dx, xn_d, px, xr, zs, fr,
    l_sem, send, a_recv, h_recv, t_recv, d_recv, x_recv, y_recv, c_recv, p_recv, q_recv, b_recv, u_recv, w_recv, met,
):
    ep = lax.axis_index("ep")
    t = lax.axis_index("tp")
    z, x = lax.div(ep, NX), lax.rem(ep, NX)
    y, c = lax.div(t, 2), lax.rem(t, 2)

    def tp_peer(d):
        return ep, lax.rem(t + d, NTP)

    def ep_peer(d):
        return lax.rem(ep + d, NEP), t

    def z_peer(d):
        return lax.rem(z + d, NZ) * NX + x, t

    def x_peer(d):
        return z * NX + lax.rem(x + d, NX), t

    def y_peer(d):
        return ep, lax.rem(y + d, 4) * 2 + c

    partner = (ep, y * 2 + 1 - c)

    def remote(src, dst, phase, recv, peer):
        pltpu.make_async_remote_copy(
            src_ref=src, dst_ref=dst, send_sem=send.at[phase], recv_sem=recv, device_id=peer, device_id_type=MESH
        ).start()

    def take(view, sem):
        pltpu.make_async_copy(view, view, sem).wait()

    loads = {}
    pairs = (
        ("hid", hidden, hid_all.at[t]), ("ids", ids, v_ids), ("route", route, v_route), ("again", attn_gain, v_again),
        ("wq", wq, v_wq), ("wk", wk, v_wk), ("wv", wv, v_wv), ("wg", wg, v_wg), ("wb", w_beta, v_wb),
        ("wd", w_decay, v_wd), ("dscale", decay_scale, v_dscale), ("hgain", head_gain, v_hgain),
        ("state", state, v_state), ("wo", w_out, v_wo), ("fgain", ffn_gain, v_fgain), ("mix", mix, v_mix),
        ("dg", dg, v_dg), ("du", du, v_du), ("dd", dd, v_dd), ("eg", eg, v_eg), ("eu", eu, v_eu), ("ed", ed, v_ed),
    )
    for number, (name, src, dst) in enumerate(pairs):
        loads[name] = pltpu.make_async_copy(src, dst, l_sem.at[number])
        loads[name].start()

    barrier = pltpu.get_barrier_semaphore()
    near = [tp_peer(d) for d in range(1, NTP)] + [z_peer(1), z_peer(NZ - 1), x_peer(1), x_peer(NX - 1)]
    for peer in near:
        pl.semaphore_signal(barrier, inc=1, device_id=peer, device_id_type=MESH)

    def tell(number, peers):
        for peer in peers:
            pl.semaphore_signal(met.at[number], inc=1, device_id=peer, device_id_type=MESH)

    loads["ids"].wait()
    loads["route"].wait()
    first, second = v_ids[0:1, :], v_ids[1:2, :]
    expert = iota((NEP, SEQ), 0)
    is_first, is_second = first == expert, second == expert
    chosen = jnp.where(is_first | is_second, 1.0, 0.0)
    earlier = jnp.where(iota((SEQ, SEQ), 0) < iota((SEQ, SEQ), 1), 1.0, 0.0).astype(BF16)
    before = dot(chosen.astype(BF16), earlier)
    place = (chosen * (before + 1.0)).astype(BF16)
    row = iota((NEP * 8, NEP), 0)
    spread = jnp.where(row // 8 == iota((NEP * 8, NEP), 1), 1.0, 0.0).astype(BF16)
    hit = dot(spread, place) == ((row % 8) // 2 + 1).astype(F32)
    weight = jnp.where(is_first, v_route[0:1, :], 0.0) + jnp.where(is_second, v_route[1:2, :], 0.0)
    coarse = weight.astype(BF16)
    fine = (weight - coarse.astype(F32)).astype(BF16)
    coarse, fine = dot(spread, coarse), dot(spread, fine)
    for h in range(2):
        here = hit & (row % 2 == h)
        send_mat[h] = jnp.where(here, 1.0, 0.0).astype(BF16)
        take_mat[2 * h] = jnp.where(here, coarse, 0.0).astype(BF16)
        take_mat[2 * h + 1] = jnp.where(here, fine, 0.0).astype(BF16)

    loads["hid"].wait()
    pl.semaphore_wait(barrier, len(near))

    for d in FAR_TP:
        remote(hid_all.at[t], hid_all.at[t], 0, a_recv, tp_peer(d))
    tell(0, (z_peer(1), z_peer(NZ - 1), x_peer(1), x_peer(NX - 1)))
    loads["again"].wait()
    take(hid_all.at[pl.ds(0, 7)], a_recv)

    pl.semaphore_wait(met.at[0], 4)
    tell(1, (z_peer(2), z_peer(NZ - 2)))
    square = jnp.zeros((SEQ, WIDTH), F32)
    for b in range(NTP):
        wide = hid_all[b].astype(F32)
        square = square + wide * wide
    scale = lax.rsqrt(jnp.sum(square, axis=-1, keepdims=True) * (1.0 / D) + EPS)
    for b in range(NTP):
        cols = slice(b * WIDTH, (b + 1) * WIDTH)
        xn_a[:, cols] = (hid_all[b].astype(F32) * scale * v_again[:, cols]).astype(BF16)
    for name in ("wq", "wk", "wv", "wg", "wb", "wd", "dscale", "hgain"):
        loads[name].wait()
    normed = xn_a[...]
    queries = dot(normed, v_wq[...])
    queries = queries * lax.rsqrt(jnp.sum(queries * queries, axis=-1, keepdims=True) + EPS) * DK ** (-0.5)
    keys = dot(normed, v_wk[...])
    keys = keys * lax.rsqrt(jnp.sum(keys * keys, axis=-1, keepdims=True) + EPS)
    values = dot(normed, v_wv[...])
    gates = dot(normed, v_wg[...])
    mine = iota((SEQ, NTP), 1) == t
    beta = jax.nn.sigmoid(jnp.sum(jnp.where(mine, dot_t(normed, v_wb[...]), 0.0), axis=-1, keepdims=True))
    logit = jnp.sum(jnp.where(mine, dot_t(normed, v_wd[...]), 0.0), axis=-1, keepdims=True)
    d_scale = jnp.sum(jnp.where(iota((1, NTP), 1) == t, v_dscale[...], 0.0), axis=-1, keepdims=True)
    soft = jnp.maximum(logit, 0.0) + jnp.log(1.0 + jnp.exp(-jnp.abs(logit)))
    decay = jnp.exp(-d_scale * soft)

    loads["state"].wait()
    qb, kb = queries.astype(BF16), keys.astype(BF16)
    diag = iota((16, 1024), 1) // DK == iota((16, 1024), 0) % 8
    by_query, by_key = [], []
    for i in range(SEQ // 8):
        both = jnp.concatenate([qb[8 * i : 8 * i + 8].astype(F32), kb[8 * i : 8 * i + 8].astype(F32)], axis=0)
        lhs = jnp.where(diag, jnp.concatenate([both] * 8, axis=1), 0.0).astype(BF16)
        rhs = v_state[8 * i : 8 * i + 8].reshape(1024, DK).astype(BF16)
        out = dot(lhs, rhs)
        by_query.append(out[:8])
        by_key.append(out[8:])
    s_q = jnp.concatenate(by_query, axis=0)
    s_k = jnp.concatenate(by_key, axis=0)
    match = beta * jnp.sum(queries * keys, axis=-1, keepdims=True)
    read = decay * (s_q - match * s_k) + match * values
    read = read * lax.rsqrt(jnp.mean(read * read, axis=-1, keepdims=True) + EPS) * v_hgain[...]
    heads_all[t] = (read * silu(gates)).astype(BF16)
    for d in FAR_TP:
        remote(heads_all.at[t], heads_all.at[t], 1, h_recv, tp_peer(d))
    pl.semaphore_wait(met.at[1], 2)
    tell(2, (x_peer(1), x_peer(2), x_peer(3), z_peer(NZ // 2)))
    update = beta * (values - decay * s_k)
    keys_t = jnp.concatenate([keys, jnp.zeros((DK - SEQ, DK), F32)], axis=0).T
    decay_rows = jnp.broadcast_to(decay, (SEQ, DK))
    for s in range(SEQ):
        new_state[s] = decay_rows[s : s + 1] * v_state[s] + keys_t[:, s : s + 1] * update[s : s + 1]

    pl.semaphore_wait(met.at[2], 4)
    loads["wo"].wait()
    take(heads_all.at[pl.ds(0, 7)], h_recv)
    wide = hid_all[t].astype(F32)
    for b in range(NTP):
        wide = wide + dot(heads_all[b], v_wo[b * DK : (b + 1) * DK, :])
    mixed = wide.astype(BF16)
    mixed_s[...] = mixed
    low, high = mixed[:, :128], mixed[:, 128:]

    t_row, t_col = iota((NTP * 8, SEQ), 0), iota((NTP * 8, SEQ), 1)
    pick = t_row // 2 == t_col
    pick_low = jnp.where(pick & (t_row % 2 == 0), 1.0, 0.0).astype(BF16)
    pick_high = jnp.where(pick & (t_row % 2 == 1), 1.0, 0.0).astype(BF16)
    own_tok[...] = (dot(pick_low, low) + dot(pick_high, high)).reshape(NTP, 8, 128).astype(BF16)

    def tokens(dz):
        def body(d, carry):
            to = lax.rem(t + d, NTP)
            remote(own_tok.at[to], dx.at[ep, t], 2, t_recv.at[dz], (z_peer(dz)[0], to))
            return carry

        lax.fori_loop(1 if dz == 0 else 0, NTP, body, 0)

    for dz in FAR_Z:
        tokens(dz)
    tokens(0)
    dx[ep, t] = own_tok[t]
    disp[...] = (dot(send_mat[0], low) + dot(send_mat[1], high)).reshape(NEP, 8, 128).astype(BF16)

    def dispatch(dz):
        def body(d, carry):
            to = z_peer(dz)[0] - x + lax.rem(x + d, NX)
            remote(disp.at[to], xa.at[t, ep], 3, d_recv.at[dz], (to, t))
            return carry

        lax.fori_loop(1 if dz == 0 else 0, NX, body, 0)

    for dz in FAR_Z:
        dispatch(dz)
    dispatch(0)
    xa[t, ep] = disp[ep]
    for dz in (0, 1, 7, 2, 6, 3, 5, 4):
        from_z = lax.rem(z + NZ - dz, NZ)
        take(dx.at[0] if dz else dx.at[0, pl.ds(0, 7)], t_recv.at[dz])
        block = dx.at[from_z * NX + x]
        for d in (2, 1, 3):
            remote(block, block, 4, x_recv.at[d - 1], x_peer(d))
        take(disp.at[pl.ds(0, NX if dz else NX - 1)], d_recv.at[dz])
        block = xa.at[t, pl.ds(from_z * NX, NX)]
        for d in (2, 1, 3):
            remote(block, block, 5, y_recv.at[d - 1], y_peer(d))
        remote(block, block, 6, c_recv.at[0], partner)
    loads["fgain"].wait()
    for name in ("dg", "du", "dd"):
        loads[name].wait()

    def dense(d):
        xx = lax.rem(x + NX - d, NX)
        for zz in range(NZ):
            stage[pl.ds(zz * PITCH, 64), :] = dx[zz * NX + xx].astype(F32).reshape(64, 128)
        square = [jnp.zeros((8, 128), F32) for _ in range(4)]
        for j in range(4):
            for b in range(16):
                part = stage[pl.ds((b // 2) * 8 + j * 2 + b % 2, 8, stride=PITCH), :]
                square[j] = square[j] + part * part
        scales = [lax.rsqrt(jnp.sum(sq, axis=-1, keepdims=True) * (1.0 / D) + EPS) for sq in square]
        for b in range(16):
            cols = slice(b * 128, (b + 1) * 128)
            parts = [
                stage[pl.ds((b // 2) * 8 + j * 2 + b % 2, 8, stride=PITCH), :] * scales[j] * v_fgain[:, cols]
                for j in range(4)
            ]
            xn_d[d, :, cols] = jnp.concatenate(parts, axis=0).astype(BF16)
        rows = xn_d[d]
        hidden_d = (silu(dot(rows, v_dg[...])) * dot(rows, v_du[...])).astype(BF16)
        for f in range(CHUNKS):
            px[d, f] = dot(hidden_d, v_dd[:, f * WIDE : (f + 1) * WIDE]).astype(BF16)
            if d:
                back = NX - d
                remote(px.at[d, f], xr.at[back - 1, f], 7, u_recv.at[back - 1, f], x_peer(back))

    dense(0)
    for d in (1, 3, 2):
        take(xa.at[0], y_recv.at[d - 1])
        block = xa.at[lax.rem(y + 4 - d, 4) * 2 + c]
        remote(block, block, 6, c_recv.at[d], partner)
    for d in (1, 3, 2):
        take(dx.at[pl.ds(0, NZ)], x_recv.at[d - 1])
        dense(d)
    for name in ("eg", "eu", "ed"):
        loads[name].wait()
    for d in range(4):
        take(xa.at[0], c_recv.at[d])
    square = jnp.zeros((ROWS, 128), F32)
    for b in range(NTP):
        stage[pl.ds(0, 256), :] = xa[b].astype(F32).reshape(256, 128)
        for h in range(2):
            part = stage[pl.ds(h, ROWS, stride=2), :]
            square = square + part * part
            xn_e[:, b * WIDTH + h * 128 : b * WIDTH + (h + 1) * 128] = part.astype(BF16)
    scale = lax.rsqrt(jnp.sum(square, axis=-1, keepdims=True) * (1.0 / D) + EPS)
    for b in range(NTP):
        cols = slice(b * WIDTH, (b + 1) * WIDTH)
        xn_e[:, cols] = (xn_e[:, cols].astype(F32) * scale * v_fgain[:, cols]).astype(BF16)
    rows_e = xn_e[...]
    inner_s[...] = (silu(dot(rows_e, v_eg[...])) * dot(rows_e, v_eu[...])).astype(BF16)
    inner = inner_s[...]
    for b in range(NTP):
        pb[b] = dot(inner, v_ed[:, b * WIDTH : (b + 1) * WIDTH]).astype(BF16)
    for d in (2, 1, 3, 0):
        there = lax.rem(y + d, 4)
        remote(pb.at[there * 2 + 1 - c], pr.at[there], 8, p_recv.at[d], partner)
    for d in (2, 1, 3, 0):
        there = lax.rem(y + d, 4)
        take(pr.at[0], p_recv.at[d])
        qs[there] = (pb[there * 2 + c].astype(F32) + pr[there].astype(F32)).astype(BF16)
        if d > 0:
            remote(qs.at[there], yr.at[d - 1], 9, q_recv.at[d - 1], y_peer(d))

    def sum_x(f):
        for d in (1, 3, 2):
            take(xr.at[0, 0], u_recv.at[d - 1, f])
        total = px[0, f].astype(F32)
        for d in range(3):
            total = total + xr[d, f].astype(F32)
        for tt in range(2):
            for h in range(2):
                cols = slice(tt * WIDTH + h * 128, tt * WIDTH + (h + 1) * 128)
                for j in range(4):
                    stage[pl.ds(tt * 8 + j * 2 + h, 8, stride=PITCH), :] = total[j * 8 : (j + 1) * 8, cols]
        for zz in range(NZ):
            zs[zz, 2 * f : 2 * f + 2] = stage[pl.ds(zz * PITCH, 16), :].reshape(2, 8, 128).astype(BF16)
        for dz in FAR_Z + (0,):
            to = z_peer(dz)[0]

            def piece(tt):
                remote(zs.at[lax.div(to, NX), tt], fr.at[z * NTP + t], 10, w_recv, (to, tt))

            for tt in (2 * f, 2 * f + 1):
                if dz:
                    piece(tt)
                else:
                    pl.when(t != tt)(functools.partial(piece, tt))

    for f in range(CHUNKS):
        sum_x(f)
    fr[z * NTP + t] = zs[z, t]
    for d in (1, 3, 2):
        take(yr.at[0], q_recv.at[d - 1])
    total = qs[y].astype(F32)
    for d in range(3):
        total = total + yr[d].astype(F32)
    total = total.astype(BF16).astype(F32)
    for h in range(2):
        stage[pl.ds(h, ROWS, stride=2), :] = total[:, h * 128 : (h + 1) * 128]
    ret[...] = stage[pl.ds(0, 256), :].reshape(NEP, 8, 128).astype(BF16)

    def give_back(d, carry):
        to = lax.rem(ep + NEP // 2 + d, NEP)

        @pl.when(to != ep)
        def _():
            remote(ret.at[to], rb.at[ep], 11, b_recv, (to, t))

        return carry

    lax.fori_loop(0, NEP, give_back, 0)
    rb[ep] = ret[ep]
    loads["mix"].wait()
    take(fr.at[pl.ds(0, NZ * NTP - 1)], w_recv)
    total = fr[0:NTP].astype(F32)
    for zz in range(1, NZ):
        total = total + fr[zz * NTP : (zz + 1) * NTP].astype(F32)
    stage[pl.ds(0, 64), :] = total.reshape(64, 128)
    take(rb.at[pl.ds(0, NEP - 1)], b_recv)
    back = rb[...].astype(F32).reshape(NEP * 8, 128).astype(BF16)
    for h in range(2):
        cols = slice(h * 128, (h + 1) * 128)
        moe = t_dot(take_mat[2 * h], back) + t_dot(take_mat[2 * h + 1], back)
        dense_out = stage[pl.ds(h, SEQ, stride=2), :]
        result[:, cols] = (
            mixed_s[:, cols].astype(F32) + moe + jax.nn.sigmoid(v_mix[:, cols]) * dense_out
        ).astype(BF16)
    sent = (
        hid_all.at[pl.ds(0, 7)], heads_all.at[pl.ds(0, 7)], fr.at[pl.ds(0, 63)], disp.at[pl.ds(0, 31)],
        dx.at[pl.ds(0, 24)], xa.at[pl.ds(0, 3)], xa.at[pl.ds(0, 4)], px.at[pl.ds(0, 3)], pb.at[pl.ds(0, 4)],
        qs.at[pl.ds(0, 3)], fr.at[pl.ds(0, 63)], ret.at[pl.ds(0, 31)],
    )
    for phase, view in enumerate(sent):
        take(view, send.at[phase])


def write_out(result, new_state, result_out, state_out, sem):
    first = pltpu.make_async_copy(result, result_out, sem.at[0])
    second = pltpu.make_async_copy(new_state, state_out, sem.at[1])
    first.start()
    second.start()
    first.wait()
    second.wait()


def per_device(
    hidden_in, state_in, attn_gain, w_query, w_key, w_value, w_gate, w_beta, w_decay, decay_scale, head_gain, w_output,
    ffn_gain, expert_ids, route_weight, expert_gate, expert_up, expert_down, dense_gate, dense_up, dense_down, dense_mix,
):
    operands = (
        hidden_in, state_in.reshape(SEQ, DK, DK), attn_gain.reshape(1, D), w_query, w_key, w_value, w_gate, w_beta.T,
        w_decay.T, decay_scale.reshape(1, NTP), head_gain.reshape(1, DK), w_output, ffn_gain.reshape(1, D), expert_ids.T,
        route_weight.T, expert_gate[0], expert_up[0], expert_down[0], dense_gate, dense_up, dense_down,
        dense_mix.reshape(1, WIDTH),
    )
    V = pltpu.VMEM
    vmem_of = [V((NTP, SEQ, WIDTH), BF16)] + [V(o.shape, o.dtype) for o in operands[1:]]
    dma = pltpu.SemaphoreType.DMA
    scratch = vmem_of + [
        V((SEQ, D), BF16), V((NTP, SEQ, DK), BF16), V((SEQ, WIDTH), BF16),
        V((2, NEP * 8, SEQ), BF16), V((4, NEP * 8, SEQ), BF16),
        V((NEP, 8, 128), BF16), V((NTP, NEP, 8, 128), BF16), V((NZ * PITCH, 128), F32), V((ROWS, D), BF16),
        V((ROWS, FE), BF16), V((NTP, ROWS, WIDTH), BF16), V((4, ROWS, WIDTH), BF16), V((4, ROWS, WIDTH), BF16),
        V((3, ROWS, WIDTH), BF16), V((NEP, 8, 128), BF16), V((NEP, 8, 128), BF16),
        V((NTP, 8, 128), BF16), V((NEP, NTP, 8, 128), BF16), V((NX, SEQ, D), BF16),
        V((NX, CHUNKS, SEQ, WIDE), BF16), V((NX - 1, CHUNKS, SEQ, WIDE), BF16),
        V((NZ, NTP, 8, 128), BF16), V((NZ * NTP, 8, 128), BF16),
        dma((22,)), dma((12,)), dma, dma, dma((NZ,)), dma((NZ,)), dma((3,)), dma((3,)), dma((4,)), dma((4,)), dma((3,)),
        dma, dma((3, CHUNKS)), dma,
        pltpu.SemaphoreType.REGULAR((3,)),
    ]
    kept = (V((SEQ, WIDTH), BF16), V((SEQ, DK, DK), F32))
    result, new_state = pl.pallas_call(
        kernel,
        out_shape=kept,
        in_specs=[pl.BlockSpec(memory_space=pltpu.HBM)] * len(operands),
        out_specs=tuple(pl.BlockSpec(memory_space=pltpu.VMEM) for _ in kept),
        scratch_shapes=scratch,
        compiler_params=pltpu.CompilerParams(
            collective_id=0, has_side_effects=True, vmem_limit_bytes=64000000
        ),
    )(*operands)
    result, new_state = pl.pallas_call(
        write_out,
        out_shape=tuple(jax.ShapeDtypeStruct(k.shape, k.dtype) for k in kept),
        in_specs=[pl.BlockSpec(memory_space=pltpu.VMEM)] * 2,
        out_specs=tuple(pl.BlockSpec(memory_space=pltpu.HBM) for _ in kept),
        scratch_shapes=[dma((2,))],
        compiler_params=pltpu.CompilerParams(vmem_limit_bytes=8 * 1024 * 1024),
    )(result, new_state)
    return result, new_state.reshape(state_in.shape)


def solution(mesh):
    return jax.shard_map(
        per_device,
        mesh=mesh,
        in_specs=(
            P("ep", "tp"), P("ep", "tp", None, None), P(), P(None, "tp"), P(None, "tp"), P(None, "tp"), P(None, "tp"),
            P(), P(), P(), P(), P(None, "tp"), P(), P("ep", None), P("ep", None), P("ep", None, "tp"),
            P("ep", None, "tp"), P("ep", "tp", None), P(None, "ep"), P(None, "ep"), P("ep", None), P("tp"),
        ),
        out_specs=(P("ep", "tp"), P("ep", "tp", None, None)),
        check_vma=False,
    )
```

```python
import functools

import jax
import jax.numpy as jnp
from jax import lax
from jax.experimental import pallas as pl
from jax.experimental.pallas import tpu as pltpu
from jax.sharding import PartitionSpec as P

EPS = 1e-06
MESH = pl.DeviceIdType.MESH
F32, BF16, I32 = jnp.float32, jnp.bfloat16, jnp.int32

NX, NZ, NTP, NEP = 4, 8, 8, 32
SEQ, D, WIDTH, DK, CAP = 32, 2048, 256, 128, 4
ROWS = NEP * CAP
FE, FD = 384, 128
PITCH = 72
CHUNKS = 4
WIDE = D // CHUNKS
FAR_TP = FAR_Z = (4, 3, 5, 2, 6, 1, 7)


def silu(v):
    return v * jax.nn.sigmoid(v)


def dot(a, b):
    return jnp.dot(a, b, preferred_element_type=F32)


def dot_t(a, b):
    return lax.dot_general(a, b, (((1,), (1,)), ((), ())), preferred_element_type=F32)


def t_dot(a, b):
    return lax.dot_general(a, b, (((0,), (0,)), ((), ())), preferred_element_type=F32)


def iota(shape, dim):
    return lax.broadcasted_iota(I32, shape, dim)


def kernel(
    hidden, state, attn_gain, wq, wk, wv, wg, w_beta, w_decay, decay_scale, head_gain, w_out, ffn_gain, ids, route,
    eg, eu, ed, dg, du, dd, mix,
    result, new_state,
    hid_all, v_state, v_again, v_w, v_wb, v_wd, v_dscale, v_hgain, v_wo, v_fgain, v_ids, v_route,
    v_e, v_ed, v_d, v_dd, v_mix,
    xn_a, heads_all, mixed_s, send_mat, take_mat,
    disp, xa, stage, xn_e, inner_s, pb, pr, qs, yr, ret, rb,
    own_tok, dx, xn_d, px, xr, zs, fr,
    l_sem, send, a_recv, h_recv, t_recv, d_recv, x_recv, y_recv, p_recv, q_recv, b_recv, u_recv, w_recv, met,
):
    ep = lax.axis_index("ep")
    t = lax.axis_index("tp")
    z, x = lax.div(ep, NX), lax.rem(ep, NX)
    y, c = lax.div(t, 2), lax.rem(t, 2)

    def tp_peer(d):
        return ep, lax.rem(t + d, NTP)

    def ep_peer(d):
        return lax.rem(ep + d, NEP), t

    def z_peer(d):
        return lax.rem(z + d, NZ) * NX + x, t

    def x_peer(d):
        return z * NX + lax.rem(x + d, NX), t

    def y_peer(d):
        return ep, lax.rem(y + d, 4) * 2 + c

    partner = (ep, y * 2 + 1 - c)

    def remote(src, dst, phase, recv, peer):
        pltpu.make_async_remote_copy(
            src_ref=src, dst_ref=dst, send_sem=send.at[phase], recv_sem=recv, device_id=peer, device_id_type=MESH
        ).start()

    def take(view, sem):
        pltpu.make_async_copy(view, view, sem).wait()

    barrier = pltpu.get_barrier_semaphore()
    near = [tp_peer(d) for d in range(1, NTP)] + [z_peer(1), z_peer(NZ - 1), x_peer(1), x_peer(NX - 1)]
    for peer in near:
        pl.semaphore_signal(barrier, inc=1, device_id=peer, device_id_type=MESH)

    def tell(number, peers):
        for peer in peers:
            pl.semaphore_signal(met.at[number], inc=1, device_id=peer, device_id_type=MESH)

    loads = {}
    pairs = (
        ("hid", (hidden,), hid_all.at[t]), ("again", (attn_gain,), v_again), ("w", (wq, wk, wv, wg), v_w),
        ("wb", (w_beta,), v_wb), ("wd", (w_decay,), v_wd), ("dscale", (decay_scale,), v_dscale),
        ("hgain", (head_gain,), v_hgain), ("ids", (ids,), v_ids), ("route", (route,), v_route),
        ("state", (state,), v_state), ("wo", (w_out,), v_wo), ("fgain", (ffn_gain,), v_fgain), ("mix", (mix,), v_mix),
        ("d", (dg, du), v_d), ("dd", (dd,), v_dd), ("e", (eg, eu), v_e), ("ed", (ed,), v_ed),
    )
    for number, (name, sources, dst) in enumerate(pairs):
        loads[name] = functools.partial(take, dst, l_sem.at[number])
        for place, src in enumerate(sources):
            part = dst.at[place] if len(sources) > 1 else dst
            pltpu.make_async_copy(src, part, l_sem.at[number]).start()

    loads["hid"]()
    pl.semaphore_wait(barrier, len(near))

    for d in FAR_TP:
        remote(hid_all.at[t], hid_all.at[t], 0, a_recv, tp_peer(d))
    tell(0, (z_peer(1), z_peer(NZ - 1), x_peer(1), x_peer(NX - 1)))
    loads["ids"]()
    loads["route"]()
    first, second = v_ids[0:1, :], v_ids[1:2, :]
    expert = iota((NEP, SEQ), 0)
    is_first, is_second = first == expert, second == expert
    chosen = jnp.where(is_first | is_second, 1.0, 0.0)
    earlier = jnp.where(iota((SEQ, SEQ), 0) < iota((SEQ, SEQ), 1), 1.0, 0.0).astype(BF16)
    before = dot(chosen.astype(BF16), earlier)
    place = (chosen * (before + 1.0)).astype(BF16)
    row = iota((NEP * 8, NEP), 0)
    spread = jnp.where(row // 8 == iota((NEP * 8, NEP), 1), 1.0, 0.0).astype(BF16)
    hit = dot(spread, place) == ((row % 8) // 2 + 1).astype(F32)
    weight = jnp.where(is_first, v_route[0:1, :], 0.0) + jnp.where(is_second, v_route[1:2, :], 0.0)
    coarse = weight.astype(BF16)
    fine = (weight - coarse.astype(F32)).astype(BF16)
    coarse, fine = dot(spread, coarse), dot(spread, fine)
    for h in range(2):
        here = hit & (row % 2 == h)
        send_mat[h, : NEP * 8] = jnp.where(here, 1.0, 0.0).astype(BF16)
        take_mat[2 * h] = jnp.where(here, coarse, 0.0).astype(BF16)
        take_mat[2 * h + 1] = jnp.where(here, fine, 0.0).astype(BF16)
    t_row, t_col = iota((NTP * 8, SEQ), 0), iota((NTP * 8, SEQ), 1)
    for h in range(2):
        send_mat[h, NEP * 8 :] = jnp.where((t_row // 2 == t_col) & (t_row % 2 == h), 1.0, 0.0).astype(BF16)

    pl.semaphore_wait(met.at[0], 4)
    tell(1, (z_peer(2), z_peer(NZ - 2)))
    loads["again"]()
    take(hid_all.at[pl.ds(0, 7)], a_recv)

    pl.semaphore_wait(met.at[1], 2)
    tell(2, (x_peer(1), x_peer(2), x_peer(3), z_peer(NZ // 2)))
    square = jnp.zeros((SEQ, WIDTH), F32)
    for b in range(NTP):
        wide = hid_all[b].astype(F32)
        square = square + wide * wide
    scale = lax.rsqrt(jnp.sum(square, axis=-1, keepdims=True) * (1.0 / D) + EPS)
    for b in range(NTP):
        cols = slice(b * WIDTH, (b + 1) * WIDTH)
        xn_a[:, cols] = (hid_all[b].astype(F32) * scale * v_again[:, cols]).astype(BF16)
    for name in ("w", "wb", "wd", "dscale", "hgain"):
        loads[name]()
    normed = xn_a[...]
    queries, keys, values, gates = (dot(normed, v_w[i]) for i in range(4))
    queries = queries * lax.rsqrt(jnp.sum(queries * queries, axis=-1, keepdims=True) + EPS) * DK ** (-0.5)
    keys = keys * lax.rsqrt(jnp.sum(keys * keys, axis=-1, keepdims=True) + EPS)
    mine = iota((SEQ, NTP), 1) == t
    beta = jax.nn.sigmoid(jnp.sum(jnp.where(mine, dot_t(normed, v_wb[...]), 0.0), axis=-1, keepdims=True))
    logit = jnp.sum(jnp.where(mine, dot_t(normed, v_wd[...]), 0.0), axis=-1, keepdims=True)
    d_scale = jnp.sum(jnp.where(iota((1, NTP), 1) == t, v_dscale[...], 0.0), axis=-1, keepdims=True)
    soft = jnp.maximum(logit, 0.0) + jnp.log(1.0 + jnp.exp(-jnp.abs(logit)))
    decay = jnp.exp(-d_scale * soft)

    loads["state"]()
    qb, kb = queries.astype(BF16), keys.astype(BF16)
    diag = iota((16, 1024), 1) // DK == iota((16, 1024), 0) % 8
    by_query, by_key = [], []
    for i in range(SEQ // 8):
        both = jnp.concatenate([qb[8 * i : 8 * i + 8].astype(F32), kb[8 * i : 8 * i + 8].astype(F32)], axis=0)
        lhs = jnp.where(diag, jnp.concatenate([both] * 8, axis=1), 0.0).astype(BF16)
        rhs = v_state[8 * i : 8 * i + 8].reshape(1024, DK).astype(BF16)
        out = dot(lhs, rhs)
        by_query.append(out[:8])
        by_key.append(out[8:])
    s_q = jnp.concatenate(by_query, axis=0)
    s_k = jnp.concatenate(by_key, axis=0)
    match = beta * jnp.sum(queries * keys, axis=-1, keepdims=True)
    read = decay * (s_q - match * s_k) + match * values
    read = read * lax.rsqrt(jnp.mean(read * read, axis=-1, keepdims=True) + EPS) * v_hgain[...]
    heads_all[t] = (read * silu(gates)).astype(BF16)
    for d in FAR_TP:
        remote(heads_all.at[t], heads_all.at[t], 1, h_recv, tp_peer(d))
    update = beta * (values - decay * s_k)
    keys_t = jnp.concatenate([keys, jnp.zeros((DK - SEQ, DK), F32)], axis=0).T
    decay_rows = jnp.broadcast_to(decay, (SEQ, DK))
    for s in range(SEQ):
        new_state[s] = decay_rows[s : s + 1] * v_state[s] + keys_t[:, s : s + 1] * update[s : s + 1]

    pl.semaphore_wait(met.at[2], 4)
    loads["wo"]()
    take(heads_all.at[pl.ds(0, 7)], h_recv)
    wide = hid_all[t].astype(F32)
    for b in range(NTP):
        wide = wide + dot(heads_all[b], v_wo[b * DK : (b + 1) * DK, :])
    mixed = wide.astype(BF16)
    mixed_s[...] = mixed
    low, high = mixed[:, :128], mixed[:, 128:]

    moved = (dot(send_mat[0], low) + dot(send_mat[1], high)).reshape(NEP + NTP, 8, 128).astype(BF16)
    disp[...] = moved[:NEP]
    own_tok[...] = moved[NEP:]
    for dz in FAR_Z + (0,):
        base = z_peer(dz)[0] - x
        for d in (2, 1, 3, 0):
            if dz or d:
                to = base + lax.rem(x + d, NX)
                remote(disp.at[to], xa.at[t, ep], 3, d_recv.at[dz], (to, t))
    xa[t, ep] = disp[ep]
    for dz in FAR_Z + (0,):
        for d in FAR_TP + (0,):
            if dz or d:
                to = lax.rem(t + d, NTP)
                remote(own_tok.at[to], dx.at[ep, t], 2, t_recv.at[dz], (z_peer(dz)[0], to))
    dx[ep, t] = own_tok[t]
    for dz in (0, 1, 7, 2, 6, 3, 5, 4):
        from_z = lax.rem(z + NZ - dz, NZ)
        take(disp.at[pl.ds(0, NX if dz else NX - 1)], d_recv.at[dz])
        block = xa.at[t, pl.ds(from_z * NX, NX)]
        for d in FAR_TP:
            remote(block, block, 5, y_recv, tp_peer(d))
        take(dx.at[0] if dz else dx.at[0, pl.ds(0, 7)], t_recv.at[dz])
        block = dx.at[from_z * NX + x]
        for d in (2, 1, 3):
            remote(block, block, 4, x_recv, x_peer(d))
    loads["fgain"]()
    for name in ("d", "dd"):
        loads[name]()

    def dense(first, last):
        for d in range(first, last):
            xx = lax.rem(x + NX - d, NX)
            for zz in range(NZ):
                stage[pl.ds(zz * PITCH, 64), :] = dx[zz * NX + xx].astype(F32).reshape(64, 128)
            square = [jnp.zeros((8, 128), F32) for _ in range(4)]
            for j in range(4):
                for b in range(16):
                    part = stage[pl.ds((b // 2) * 8 + j * 2 + b % 2, 8, stride=PITCH), :]
                    square[j] = square[j] + part * part
            scales = [lax.rsqrt(jnp.sum(sq, axis=-1, keepdims=True) * (1.0 / D) + EPS) for sq in square]
            for b in range(16):
                cols = slice(b * 128, (b + 1) * 128)
                parts = [
                    stage[pl.ds((b // 2) * 8 + j * 2 + b % 2, 8, stride=PITCH), :] * scales[j] * v_fgain[:, cols]
                    for j in range(4)
                ]
                xn_d[d * SEQ : (d + 1) * SEQ, cols] = jnp.concatenate(parts, axis=0).astype(BF16)
        rows = xn_d[first * SEQ : last * SEQ]
        hidden_d = (silu(dot(rows, v_d[0])) * dot(rows, v_d[1])).astype(BF16)
        for f in range(CHUNKS):
            out = dot(hidden_d, v_dd[:, f * WIDE : (f + 1) * WIDE]).astype(BF16)
            for d in range(first, last):
                px[d, f] = out[(d - first) * SEQ : (d - first + 1) * SEQ]
            for d in (2, 1, 3):
                if first <= d < last:
                    back = NX - d
                    remote(px.at[d, f], xr.at[back - 1, f], 6, u_recv.at[f], x_peer(back))

    dense(0, 1)
    take(dx.at[pl.ds(0, 24)], x_recv)
    dense(1, NX)
    for name in ("e", "ed"):
        loads[name]()
    take(xa.at[pl.ds(0, 7)], y_recv)
    square = jnp.zeros((ROWS, 128), F32)
    for b in range(NTP):
        stage[pl.ds(0, 256), :] = xa[b].astype(F32).reshape(256, 128)
        for h in range(2):
            part = stage[pl.ds(h, ROWS, stride=2), :]
            square = square + part * part
            xn_e[:, b * WIDTH + h * 128 : b * WIDTH + (h + 1) * 128] = part.astype(BF16)
    scale = lax.rsqrt(jnp.sum(square, axis=-1, keepdims=True) * (1.0 / D) + EPS)
    for b in range(NTP):
        cols = slice(b * WIDTH, (b + 1) * WIDTH)
        xn_e[:, cols] = (xn_e[:, cols].astype(F32) * scale * v_fgain[:, cols]).astype(BF16)
    rows_e = xn_e[...]
    inner_s[...] = (silu(dot(rows_e, v_e[0])) * dot(rows_e, v_e[1])).astype(BF16)
    inner = inner_s[...]
    for b in range(NTP):
        pb[b] = dot(inner, v_ed[:, b * WIDTH : (b + 1) * WIDTH]).astype(BF16)
    for d in (2, 1, 3, 0):
        there = lax.rem(y + d, 4)
        remote(pb.at[there * 2 + 1 - c], pr.at[there], 7, p_recv.at[d], partner)
    for d in (2, 1, 3, 0):
        there = lax.rem(y + d, 4)
        take(pr.at[0], p_recv.at[d])
        qs[there] = (pb[there * 2 + c].astype(F32) + pr[there].astype(F32)).astype(BF16)
        if d > 0:
            remote(qs.at[there], yr.at[d - 1], 8, q_recv.at[d - 1], y_peer(d))

    def sum_x(f):
        take(xr.at[:, f], u_recv.at[f])
        total = px[0, f].astype(F32)
        for d in range(3):
            total = total + xr[d, f].astype(F32)
        for tt in range(2):
            for h in range(2):
                cols = slice(tt * WIDTH + h * 128, tt * WIDTH + (h + 1) * 128)
                for j in range(4):
                    stage[pl.ds(tt * 8 + j * 2 + h, 8, stride=PITCH), :] = total[j * 8 : (j + 1) * 8, cols]
        for zz in range(NZ):
            zs[zz, 2 * f : 2 * f + 2] = stage[pl.ds(zz * PITCH, 16), :].reshape(2, 8, 128).astype(BF16)
        for dz in FAR_Z + (0,):
            to = z_peer(dz)[0]

            def piece(tt):
                remote(zs.at[lax.div(to, NX), tt], fr.at[z * NTP + t], 9, w_recv, (to, tt))

            for tt in (2 * f, 2 * f + 1):
                if dz:
                    piece(tt)
                else:
                    pl.when(t != tt)(functools.partial(piece, tt))

    sum_x(0)
    sum_x(1)
    sum_x(2)
    sum_x(3)
    fr[z * NTP + t] = zs[z, t]
    for d in (1, 3, 2):
        take(yr.at[0], q_recv.at[d - 1])
    total = qs[y].astype(F32)
    for d in range(3):
        total = total + yr[d].astype(F32)
    total = total.astype(BF16).astype(F32)
    for h in range(2):
        stage[pl.ds(h, ROWS, stride=2), :] = total[:, h * 128 : (h + 1) * 128]
    ret[...] = stage[pl.ds(0, 256), :].reshape(NEP, 8, 128).astype(BF16)

    for dz in FAR_Z + (0,):
        base = z_peer(dz)[0] - x
        for d in (2, 1, 3, 0):
            if dz or d:
                to = base + lax.rem(x + d, NX)
                remote(ret.at[to], rb.at[ep], 10, b_recv, (to, t))
    rb[ep] = ret[ep]
    loads["mix"]()
    take(fr.at[pl.ds(0, NZ * NTP - 1)], w_recv)
    total = fr[0:NTP].astype(F32)
    for zz in range(1, NZ):
        total = total + fr[zz * NTP : (zz + 1) * NTP].astype(F32)
    stage[pl.ds(0, 64), :] = total.reshape(64, 128)
    take(rb.at[pl.ds(0, NEP - 1)], b_recv)
    back = rb[...].astype(F32).reshape(NEP * 8, 128).astype(BF16)
    for h in range(2):
        cols = slice(h * 128, (h + 1) * 128)
        moe = t_dot(take_mat[2 * h], back) + t_dot(take_mat[2 * h + 1], back)
        dense_out = stage[pl.ds(h, SEQ, stride=2), :]
        result[:, cols] = (
            mixed_s[:, cols].astype(F32) + moe + jax.nn.sigmoid(v_mix[:, cols]) * dense_out
        ).astype(BF16)
    sent = (
        hid_all.at[pl.ds(0, 7)], heads_all.at[pl.ds(0, 7)], fr.at[pl.ds(0, 63)], disp.at[pl.ds(0, 31)],
        dx.at[pl.ds(0, 24)], xa.at[pl.ds(0, 7)], px.at[pl.ds(0, 3)], pb.at[pl.ds(0, 4)],
        qs.at[pl.ds(0, 3)], fr.at[pl.ds(0, 63)], ret.at[pl.ds(0, 31)],
    )
    for phase, view in enumerate(sent):
        take(view, send.at[phase])


def write_out(result, new_state, result_out, state_out, sem):
    first = pltpu.make_async_copy(new_state, state_out, sem.at[0])
    second = pltpu.make_async_copy(result, result_out, sem.at[1])
    first.start()
    second.start()
    first.wait()
    second.wait()


def per_device(
    hidden_in, state_in, attn_gain, w_query, w_key, w_value, w_gate, w_beta, w_decay, decay_scale, head_gain, w_output,
    ffn_gain, expert_ids, route_weight, expert_gate, expert_up, expert_down, dense_gate, dense_up, dense_down, dense_mix,
):
    operands = (
        hidden_in, state_in.reshape(SEQ, DK, DK), attn_gain.reshape(1, D), w_query, w_key, w_value, w_gate, w_beta.T,
        w_decay.T, decay_scale.reshape(1, NTP), head_gain.reshape(1, DK), w_output, ffn_gain.reshape(1, D), expert_ids.T,
        route_weight.T, expert_gate[0], expert_up[0], expert_down[0], dense_gate, dense_up, dense_down,
        dense_mix.reshape(1, WIDTH),
    )
    V = pltpu.VMEM
    vmem_of = [
        V((NTP, SEQ, WIDTH), BF16), V((SEQ, DK, DK), F32), V((1, D), F32), V((4, D, DK), BF16), V((NTP, D), BF16),
        V((NTP, D), BF16), V((1, NTP), F32), V((1, DK), F32), V((NTP * DK, WIDTH), BF16), V((1, D), F32),
        V((2, SEQ), I32), V((2, SEQ), F32), V((2, D, FE), BF16), V((FE, D), BF16), V((2, D, FD), BF16),
        V((FD, D), BF16), V((1, WIDTH), F32),
    ]
    dma = pltpu.SemaphoreType.DMA
    scratch = vmem_of + [
        V((SEQ, D), BF16), V((NTP, SEQ, DK), BF16), V((SEQ, WIDTH), BF16),
        V((2, (NEP + NTP) * 8, SEQ), BF16), V((4, NEP * 8, SEQ), BF16),
        V((NEP, 8, 128), BF16), V((NTP, NEP, 8, 128), BF16), V((NZ * PITCH, 128), F32), V((ROWS, D), BF16),
        V((ROWS, FE), BF16), V((NTP, ROWS, WIDTH), BF16), V((4, ROWS, WIDTH), BF16), V((4, ROWS, WIDTH), BF16),
        V((3, ROWS, WIDTH), BF16), V((NEP, 8, 128), BF16), V((NEP, 8, 128), BF16),
        V((NTP, 8, 128), BF16), V((NEP, NTP, 8, 128), BF16), V((NX * SEQ, D), BF16),
        V((NX, CHUNKS, SEQ, WIDE), BF16), V((NX - 1, CHUNKS, SEQ, WIDE), BF16),
        V((NZ, NTP, 8, 128), BF16), V((NZ * NTP, 8, 128), BF16),
        dma((17,)), dma((11,)), dma, dma, dma((NZ,)), dma((NZ,)), dma, dma, dma((4,)), dma((3,)),
        dma, dma((CHUNKS,)), dma,
        pltpu.SemaphoreType.REGULAR((3,)),
    ]
    kept = (V((SEQ, WIDTH), BF16), V((SEQ, DK, DK), F32))
    result, new_state = pl.pallas_call(
        kernel,
        out_shape=kept,
        in_specs=[pl.BlockSpec(memory_space=pltpu.HBM)] * len(operands),
        out_specs=tuple(pl.BlockSpec(memory_space=pltpu.VMEM) for _ in kept),
        scratch_shapes=scratch,
        compiler_params=pltpu.CompilerParams(
            collective_id=0, has_side_effects=True, vmem_limit_bytes=64000000
        ),
    )(*operands)
    result, new_state = pl.pallas_call(
        write_out,
        out_shape=tuple(jax.ShapeDtypeStruct(k.shape, k.dtype) for k in kept),
        in_specs=[pl.BlockSpec(memory_space=pltpu.VMEM)] * 2,
        out_specs=tuple(pl.BlockSpec(memory_space=pltpu.HBM) for _ in kept),
        scratch_shapes=[dma((2,))],
        compiler_params=pltpu.CompilerParams(vmem_limit_bytes=8 * 1024 * 1024),
    )(result, new_state)
    return result, new_state.reshape(state_in.shape)


def solution(mesh):
    return jax.shard_map(
        per_device,
        mesh=mesh,
        in_specs=(
            P("ep", "tp"), P("ep", "tp", None, None), P(), P(None, "tp"), P(None, "tp"), P(None, "tp"), P(None, "tp"),
            P(), P(), P(), P(), P(None, "tp"), P(), P("ep", None), P("ep", None), P("ep", None, "tp"),
            P("ep", None, "tp"), P("ep", "tp", None), P(None, "ep"), P(None, "ep"), P("ep", None), P("tp"),
        ),
        out_specs=(P("ep", "tp"), P("ep", "tp", None, None)),
        check_vma=False,
    )
```

```python
import functools

import jax
import jax.numpy as jnp
from jax import lax
from jax.experimental import pallas as pl
from jax.experimental.pallas import tpu as pltpu
from jax.sharding import PartitionSpec as P

EPS = 1e-06
MESH = pl.DeviceIdType.MESH
F32, BF16, I32 = jnp.float32, jnp.bfloat16, jnp.int32

NX, NZ, NTP, NEP = 4, 8, 8, 32
SEQ, D, WIDTH, DK, CAP = 32, 2048, 256, 128, 4
ROWS = NEP * CAP
FE, FD = 384, 128
PITCH = 72
CHUNKS = 4
WIDE = D // CHUNKS
SENT = 7 * 8 + 7 * 4 + 63 + 31 + 24 * 8 + 3 * 32 + 4 * 32 + 12 * 16 + 4 * 32 + 3 * 32 + 63 + 31
FAR_TP = FAR_Z = (4, 3, 5, 2, 6, 1, 7)
NEAR_TP = (1, 7, 2, 6)
ROUND_OF = (0, 1, 2, 3, 4, 3, 2, 1)


def silu(v):
    return v * jax.nn.sigmoid(v)


def dot(a, b):
    return jnp.dot(a, b, preferred_element_type=F32)


def dot_t(a, b):
    return lax.dot_general(a, b, (((1,), (1,)), ((), ())), preferred_element_type=F32)


def t_dot(a, b):
    return lax.dot_general(a, b, (((0,), (0,)), ((), ())), preferred_element_type=F32)


def iota(shape, dim):
    return lax.broadcasted_iota(I32, shape, dim)


def kernel(
    hidden, state, attn_gain, wq, wk, wv, wg, w_beta, w_decay, decay_scale, head_gain, w_out, ffn_gain, ids, route,
    eg, eu, ed, dg, du, dd, mix,
    result, new_state,
    hid_all, v_state, v_again, v_w, v_wb, v_wd, v_dscale, v_hgain, v_wo, v_fgain, v_ids, v_route,
    v_e, v_ed, v_d, v_dd, v_mix,
    heads_all, mixed_s, send_mat, take_mat,
    disp, xa, stage, stage_e, square_e, acc_e, pb, pr, qs, yr, ret, rb,
    own_tok, dx, xn_d, px, xr, zs, fr, count,
    l_sem, send, a_recv, h_recv, t_recv, d_recv, x_recv, y_recv, c_recv, p_recv, q_recv, b_recv, u_recv, w_recv, met,
):
    ep = lax.axis_index("ep")
    t = lax.axis_index("tp")
    z, x = lax.div(ep, NX), lax.rem(ep, NX)
    y, c = lax.div(t, 2), lax.rem(t, 2)

    def tp_peer(d):
        return ep, lax.rem(t + d, NTP)

    def ep_peer(d):
        return lax.rem(ep + d, NEP), t

    def z_peer(d):
        return lax.rem(z + d, NZ) * NX + x, t

    def x_peer(d):
        return z * NX + lax.rem(x + d, NX), t

    def y_peer(d):
        return ep, lax.rem(y + d, 4) * 2 + c

    partner = (ep, y * 2 + 1 - c)

    def remote(src, dst, recv, peer):
        pltpu.make_async_remote_copy(
            src_ref=src, dst_ref=dst, send_sem=send, recv_sem=recv, device_id=peer, device_id_type=MESH
        ).start()

    def take(view, sem):
        pltpu.make_async_copy(view, view, sem).wait()

    barrier = pltpu.get_barrier_semaphore()
    near = [tp_peer(d) for d in range(1, NTP)] + [z_peer(1), z_peer(NZ - 1), x_peer(1), x_peer(NX - 1)]
    for peer in near:
        pl.semaphore_signal(barrier, inc=1, device_id=peer, device_id_type=MESH)

    def tell(number, peers):
        for peer in peers:
            pl.semaphore_signal(met.at[number], inc=1, device_id=peer, device_id_type=MESH)

    loads = {}
    pairs = (
        ("hid", (hidden,), hid_all.at[t]), ("again", (attn_gain,), v_again), ("w", (wq, wk, wv, wg), v_w),
        ("wb", (w_beta,), v_wb), ("wd", (w_decay,), v_wd), ("dscale", (decay_scale,), v_dscale),
        ("hgain", (head_gain,), v_hgain), ("ids", (ids,), v_ids), ("route", (route,), v_route),
        ("state", (state,), v_state), ("wo", (w_out,), v_wo), ("fgain", (ffn_gain,), v_fgain), ("mix", (mix,), v_mix),
        ("d", (dg, du), v_d), ("dd", (dd,), v_dd), ("e", (eg, eu), v_e), ("ed", (ed,), v_ed),
    )
    for number, (name, sources, dst) in enumerate(pairs):
        loads[name] = functools.partial(take, dst, l_sem.at[number])
        for place, src in enumerate(sources):
            part = dst.at[place] if len(sources) > 1 else dst
            pltpu.make_async_copy(src, part, l_sem.at[number]).start()

    loads["hid"]()
    pl.semaphore_wait(barrier, len(near))

    for d in FAR_TP:
        remote(hid_all.at[t], hid_all.at[t], a_recv.at[0 if d in NEAR_TP else 1], tp_peer(d))
    tell(0, (z_peer(1), z_peer(NZ - 1), x_peer(1), x_peer(NX - 1)))
    loads["ids"]()
    loads["route"]()
    first, second = v_ids[0:1, :], v_ids[1:2, :]
    expert = iota((NEP, SEQ), 0)
    is_first, is_second = first == expert, second == expert
    chosen = jnp.where(is_first | is_second, 1.0, 0.0)
    earlier = jnp.where(iota((SEQ, SEQ), 0) < iota((SEQ, SEQ), 1), 1.0, 0.0).astype(BF16)
    before = dot(chosen.astype(BF16), earlier)
    place = (chosen * (before + 1.0)).astype(BF16)
    row = iota((NEP * 8, NEP), 0)
    spread = jnp.where(row // 8 == iota((NEP * 8, NEP), 1), 1.0, 0.0).astype(BF16)
    hit = dot(spread, place) == ((row % 8) // 2 + 1).astype(F32)
    weight = jnp.where(is_first, v_route[0:1, :], 0.0) + jnp.where(is_second, v_route[1:2, :], 0.0)
    coarse = weight.astype(BF16)
    fine = (weight - coarse.astype(F32)).astype(BF16)
    coarse, fine = dot(spread, coarse), dot(spread, fine)
    for h in range(2):
        here = hit & (row % 2 == h)
        send_mat[h, : NEP * 8] = jnp.where(here, 1.0, 0.0).astype(BF16)
        take_mat[2 * h] = jnp.where(here, coarse, 0.0).astype(BF16)
        take_mat[2 * h + 1] = jnp.where(here, fine, 0.0).astype(BF16)
    t_row, t_col = iota((NTP * 8, SEQ), 0), iota((NTP * 8, SEQ), 1)
    for h in range(2):
        send_mat[h, NEP * 8 :] = jnp.where((t_row // 2 == t_col) & (t_row % 2 == h), 1.0, 0.0).astype(BF16)

    pl.semaphore_wait(met.at[0], 4)
    tell(1, (z_peer(2), z_peer(NZ - 2)))
    for name in ("again", "w", "wb", "wd"):
        loads[name]()

    def project(slots):
        sums = None
        for b in slots:
            cols = pl.ds(pl.multiple_of(b * WIDTH, WIDTH), WIDTH)
            wide = hid_all[b].astype(F32)
            part = (wide * v_again[b]).astype(BF16)
            outs = [wide * wide] + [dot(part, v_w[i, cols, :]) for i in range(4)]
            outs += [dot_t(part, v_wb[:, cols]), dot_t(part, v_wd[:, cols])]
            sums = outs if sums is None else [total + out for total, out in zip(sums, outs)]
        return sums

    take(hid_all.at[pl.ds(0, 4)], a_recv.at[0])
    sums = project([t] + [lax.rem(t + NTP - d, NTP) for d in NEAR_TP])
    take(hid_all.at[pl.ds(0, 3)], a_recv.at[1])
    late = project([lax.rem(t + NTP - d, NTP) for d in (3, 5, 4)])
    sums = [total + part for total, part in zip(sums, late)]
    pl.semaphore_wait(met.at[1], 2)
    tell(2, (x_peer(1), x_peer(2), x_peer(3), z_peer(NZ // 2)))
    for name in ("dscale", "hgain"):
        loads[name]()
    scale = lax.rsqrt(jnp.sum(sums[0], axis=-1, keepdims=True) * (1.0 / D) + EPS)
    queries, keys, values, gates, beta_all, decay_all = (total * scale for total in sums[1:])
    queries = queries * lax.rsqrt(jnp.sum(queries * queries, axis=-1, keepdims=True) + EPS) * DK ** (-0.5)
    keys = keys * lax.rsqrt(jnp.sum(keys * keys, axis=-1, keepdims=True) + EPS)
    mine = iota((SEQ, NTP), 1) == t
    beta = jax.nn.sigmoid(jnp.sum(jnp.where(mine, beta_all, 0.0), axis=-1, keepdims=True))
    logit = jnp.sum(jnp.where(mine, decay_all, 0.0), axis=-1, keepdims=True)
    d_scale = jnp.sum(jnp.where(iota((1, NTP), 1) == t, v_dscale[...], 0.0), axis=-1, keepdims=True)
    soft = jnp.maximum(logit, 0.0) + jnp.log(1.0 + jnp.exp(-jnp.abs(logit)))
    decay = jnp.exp(-d_scale * soft)

    loads["state"]()
    qb, kb = queries.astype(BF16), keys.astype(BF16)
    diag = iota((16, 1024), 1) // DK == iota((16, 1024), 0) % 8
    by_query, by_key = [], []
    for i in range(SEQ // 8):
        both = jnp.concatenate([qb[8 * i : 8 * i + 8].astype(F32), kb[8 * i : 8 * i + 8].astype(F32)], axis=0)
        lhs = jnp.where(diag, jnp.concatenate([both] * 8, axis=1), 0.0).astype(BF16)
        rhs = v_state[8 * i : 8 * i + 8].reshape(1024, DK).astype(BF16)
        out = dot(lhs, rhs)
        by_query.append(out[:8])
        by_key.append(out[8:])
    s_q = jnp.concatenate(by_query, axis=0)
    s_k = jnp.concatenate(by_key, axis=0)
    match = beta * jnp.sum(queries * keys, axis=-1, keepdims=True)
    read = decay * (s_q - match * s_k) + match * values
    read = read * lax.rsqrt(jnp.mean(read * read, axis=-1, keepdims=True) + EPS) * v_hgain[...]
    heads_all[t] = (read * silu(gates)).astype(BF16)
    for d in FAR_TP:
        remote(heads_all.at[t], heads_all.at[t], h_recv, tp_peer(d))
    update = beta * (values - decay * s_k)
    keys_t = jnp.concatenate([keys, jnp.zeros((DK - SEQ, DK), F32)], axis=0).T
    decay_rows = jnp.broadcast_to(decay, (SEQ, DK))
    for s in range(SEQ):
        new_state[s] = decay_rows[s : s + 1] * v_state[s] + keys_t[:, s : s + 1] * update[s : s + 1]

    pl.semaphore_wait(met.at[2], 4)
    loads["wo"]()
    take(heads_all.at[pl.ds(0, 7)], h_recv)
    wide = hid_all[t].astype(F32)
    for b in range(NTP):
        wide = wide + dot(heads_all[b], v_wo[b * DK : (b + 1) * DK, :])
    mixed = wide.astype(BF16)
    mixed_s[...] = mixed
    low, high = mixed[:, :128], mixed[:, 128:]

    moved = (dot(send_mat[0], low) + dot(send_mat[1], high)).reshape(NEP + NTP, 8, 128).astype(BF16)
    disp[...] = moved[:NEP]
    own_tok[...] = moved[NEP:]
    for dz in FAR_Z + (0,):
        base = z_peer(dz)[0] - x
        for d in (2, 1, 3, 0):
            if dz or d:
                to = base + lax.rem(x + d, NX)
                remote(disp.at[to], xa.at[t, ep], d_recv.at[ROUND_OF[dz]], (to, t))
    xa[t, ep] = disp[ep]
    for dz in FAR_Z + (0,):
        for d in FAR_TP + (0,):
            if dz or d:
                to = lax.rem(t + d, NTP)
                remote(own_tok.at[to], dx.at[ep, t], t_recv.at[ROUND_OF[dz]], (z_peer(dz)[0], to))
    dx[ep, t] = own_tok[t]
    for distance in range(NZ // 2 + 1):
        group = [dz for dz in range(NZ) if ROUND_OF[dz] == distance]
        blocks = [lax.rem(z + NZ - dz, NZ) for dz in group]
        take(disp.at[pl.ds(0, NX * len(group) if distance else NX - 1)], d_recv.at[distance])
        for from_z in blocks:
            block = xa.at[t, pl.ds(from_z * NX, NX)]
            for d in (2, 1, 3):
                remote(block, block, y_recv.at[d - 1], y_peer(d))
            remote(block, block, c_recv.at[0], partner)
        take(fr.at[pl.ds(0, NTP * len(group) if distance else NTP - 1)], t_recv.at[distance])
        for from_z in blocks:
            block = dx.at[from_z * NX + x]
            for d in (2, 1, 3):
                remote(block, block, x_recv, x_peer(d))
    loads["fgain"]()
    for name in ("d", "dd"):
        loads[name]()

    def dense(first, last):
        for d in range(first, last):
            xx = lax.rem(x + NX - d, NX)
            for zz in range(NZ):
                stage[pl.ds(zz * PITCH, 64), :] = dx[zz * NX + xx].astype(F32).reshape(64, 128)
            square = [jnp.zeros((8, 128), F32) for _ in range(4)]
            for j in range(4):
                for b in range(16):
                    part = stage[pl.ds((b // 2) * 8 + j * 2 + b % 2, 8, stride=PITCH), :]
                    square[j] = square[j] + part * part
            scales = [lax.rsqrt(jnp.sum(sq, axis=-1, keepdims=True) * (1.0 / D) + EPS) for sq in square]
            for b in range(16):
                cols = slice(b * 128, (b + 1) * 128)
                parts = [
                    stage[pl.ds((b // 2) * 8 + j * 2 + b % 2, 8, stride=PITCH), :] * scales[j] * v_fgain[b // 2, :, (b % 2) * 128 : (b % 2 + 1) * 128]
                    for j in range(4)
                ]
                xn_d[d * SEQ : (d + 1) * SEQ, cols] = jnp.concatenate(parts, axis=0).astype(BF16)
        rows = xn_d[first * SEQ : last * SEQ]
        hidden_d = (silu(dot(rows, v_d[0])) * dot(rows, v_d[1])).astype(BF16)
        for f in range(CHUNKS):
            out = dot(hidden_d, v_dd[:, f * WIDE : (f + 1) * WIDE]).astype(BF16)
            for d in range(first, last):
                px[d, f] = out[(d - first) * SEQ : (d - first + 1) * SEQ]
            for d in (2, 1, 3):
                if first <= d < last:
                    back = NX - d
                    remote(px.at[d, f], xr.at[back - 1, f], u_recv.at[f], x_peer(back))

    dense(0, 1)
    for name in ("e", "ed"):
        loads[name]()

    def expert_slices(slots, start):
        square, outs = 0.0, [0.0, 0.0]
        for number, b in enumerate(slots):
            base = pl.multiple_of(b * WIDTH, WIDTH)
            stage_e[number] = xa[b].astype(F32).reshape(256, 128)
            parts = [stage_e[number, pl.ds(h, ROWS, stride=2), :] for h in range(2)]
            square = square + parts[0] * parts[0] + parts[1] * parts[1]
            gain = v_fgain[b]
            rows = jnp.concatenate([parts[h] * gain[:, h * 128 : (h + 1) * 128] for h in range(2)], axis=1).astype(BF16)
            outs = [outs[i] + dot(rows, v_e[i, pl.ds(base, WIDTH), :]) for i in range(2)]
        square_e[...] = square if start else square_e[...] + square
        for i in range(2):
            acc_e[i] = outs[i] if start else acc_e[i] + outs[i]

    expert_slices([t], True)
    take(xa.at[0], c_recv.at[0])
    expert_slices([y * 2 + 1 - c], False)
    for d in (1, 3, 2):
        take(xa.at[0], y_recv.at[d - 1])
        block = xa.at[lax.rem(y + 4 - d, 4) * 2 + c]
        remote(block, block, c_recv.at[1], partner)
    expert_slices([lax.rem(y + 4 - d, 4) * 2 + c for d in (1, 3, 2)], False)
    take(xa.at[pl.ds(0, 3)], c_recv.at[1])
    expert_slices([lax.rem(y + 4 - d, 4) * 2 + 1 - c for d in (1, 3, 2)], False)
    scale = lax.rsqrt(jnp.sum(square_e[...], axis=-1, keepdims=True) * (1.0 / D) + EPS)
    inner = (silu(acc_e[0] * scale) * (acc_e[1] * scale)).astype(BF16)
    for b in range(NTP):
        pb[b] = dot(inner, v_ed[:, b * WIDTH : (b + 1) * WIDTH]).astype(BF16)
    for d in (2, 1, 3, 0):
        there = lax.rem(y + d, 4)
        remote(pb.at[there * 2 + 1 - c], pr.at[there], p_recv.at[d], partner)
    take(dx.at[pl.ds(0, 24)], x_recv)
    dense(1, NX)
    for d in (2, 1, 3, 0):
        there = lax.rem(y + d, 4)
        take(pr.at[0], p_recv.at[d])
        qs[there] = (pb[there * 2 + c].astype(F32) + pr[there].astype(F32)).astype(BF16)
        if d > 0:
            remote(qs.at[there], yr.at[d - 1], q_recv.at[d - 1], y_peer(d))

    def sum_x(f):
        take(xr.at[:, f], u_recv.at[f])
        total = px[0, f].astype(F32)
        for d in range(3):
            total = total + xr[d, f].astype(F32)
        for tt in range(2):
            for h in range(2):
                cols = slice(tt * WIDTH + h * 128, tt * WIDTH + (h + 1) * 128)
                for j in range(4):
                    stage[pl.ds(tt * 8 + j * 2 + h, 8, stride=PITCH), :] = total[j * 8 : (j + 1) * 8, cols]
        for zz in range(NZ):
            zs[zz, 2 * f : 2 * f + 2] = stage[pl.ds(zz * PITCH, 16), :].reshape(2, 8, 128).astype(BF16)
        for dz in FAR_Z + (0,):
            to = z_peer(dz)[0]

            def piece(tt):
                remote(zs.at[lax.div(to, NX), tt], fr.at[z * NTP + t], w_recv, (to, tt))

            for tt in (2 * f, 2 * f + 1):
                if dz:
                    piece(tt)
                else:
                    pl.when(t != tt)(functools.partial(piece, tt))

    sum_x(0)
    sum_x(1)
    for d in (1, 3, 2):
        take(yr.at[0], q_recv.at[d - 1])
    total = qs[y].astype(F32)
    for d in range(3):
        total = total + yr[d].astype(F32)
    total = total.astype(BF16).astype(F32)
    for h in range(2):
        stage[pl.ds(h, ROWS, stride=2), :] = total[:, h * 128 : (h + 1) * 128]
    ret[...] = stage[pl.ds(0, 256), :].reshape(NEP, 8, 128).astype(BF16)

    for dz in FAR_Z + (0,):
        base = z_peer(dz)[0] - x
        for d in (2, 1, 3, 0):
            if dz or d:
                to = base + lax.rem(x + d, NX)
                remote(ret.at[to], rb.at[ep], b_recv, (to, t))
    rb[ep] = ret[ep]
    sum_x(2)
    sum_x(3)
    fr[z * NTP + t] = zs[z, t]
    loads["mix"]()
    take(fr.at[pl.ds(0, NZ * NTP - 1)], w_recv)
    total = fr[0:NTP].astype(F32)
    for zz in range(1, NZ):
        total = total + fr[zz * NTP : (zz + 1) * NTP].astype(F32)
    stage[pl.ds(0, 64), :] = total.reshape(64, 128)
    take(rb.at[pl.ds(0, NEP - 1)], b_recv)
    back = rb[...].astype(F32).reshape(NEP * 8, 128).astype(BF16)
    for h in range(2):
        cols = slice(h * 128, (h + 1) * 128)
        moe = t_dot(take_mat[2 * h], back) + t_dot(take_mat[2 * h + 1], back)
        dense_out = stage[pl.ds(h, SEQ, stride=2), :]
        result[:, cols] = (
            mixed_s[:, cols].astype(F32) + moe + jax.nn.sigmoid(v_mix[:, cols]) * dense_out
        ).astype(BF16)
    take(count, send)


def write_out(result, new_state, result_out, state_out, sem):
    first = pltpu.make_async_copy(new_state, state_out, sem.at[0])
    second = pltpu.make_async_copy(result, result_out, sem.at[1])
    first.start()
    second.start()
    first.wait()
    second.wait()


def per_device(
    hidden_in, state_in, attn_gain, w_query, w_key, w_value, w_gate, w_beta, w_decay, decay_scale, head_gain, w_output,
    ffn_gain, expert_ids, route_weight, expert_gate, expert_up, expert_down, dense_gate, dense_up, dense_down, dense_mix,
):
    operands = (
        hidden_in, state_in.reshape(SEQ, DK, DK), attn_gain.reshape(NTP, 1, WIDTH), w_query, w_key, w_value, w_gate, w_beta.T,
        w_decay.T, decay_scale.reshape(1, NTP), head_gain.reshape(1, DK), w_output, ffn_gain.reshape(NTP, 1, WIDTH), expert_ids.T,
        route_weight.T, expert_gate[0], expert_up[0], expert_down[0], dense_gate, dense_up, dense_down,
        dense_mix.reshape(1, WIDTH),
    )
    V = pltpu.VMEM
    vmem_of = [
        V((NTP, SEQ, WIDTH), BF16), V((SEQ, DK, DK), F32), V((NTP, 1, WIDTH), F32), V((4, D, DK), BF16), V((NTP, D), BF16),
        V((NTP, D), BF16), V((1, NTP), F32), V((1, DK), F32), V((NTP * DK, WIDTH), BF16), V((NTP, 1, WIDTH), F32),
        V((2, SEQ), I32), V((2, SEQ), F32), V((2, D, FE), BF16), V((FE, D), BF16), V((2, D, FD), BF16),
        V((FD, D), BF16), V((1, WIDTH), F32),
    ]
    dma = pltpu.SemaphoreType.DMA
    scratch = vmem_of + [
        V((NTP, SEQ, DK), BF16), V((SEQ, WIDTH), BF16),
        V((2, (NEP + NTP) * 8, SEQ), BF16), V((4, NEP * 8, SEQ), BF16),
        V((NEP, 8, 128), BF16), V((NTP, NEP, 8, 128), BF16), V((NZ * PITCH, 128), F32), V((3, 256, 128), F32),
        V((ROWS, 128), F32), V((2, ROWS, FE), F32), V((NTP, ROWS, WIDTH), BF16), V((4, ROWS, WIDTH), BF16), V((4, ROWS, WIDTH), BF16),
        V((3, ROWS, WIDTH), BF16), V((NEP, 8, 128), BF16), V((NEP, 8, 128), BF16),
        V((NTP, 8, 128), BF16), V((NEP, NTP, 8, 128), BF16), V((NX * SEQ, D), BF16),
        V((NX, CHUNKS, SEQ, WIDE), BF16), V((NX - 1, CHUNKS, SEQ, WIDE), BF16),
        V((NZ, NTP, 8, 128), BF16), V((NZ * NTP, 8, 128), BF16), V((SENT, 8, 128), BF16),
        dma((17,)), dma, dma((2,)), dma, dma((5,)), dma((5,)), dma, dma((3,)), dma((2,)), dma((4,)), dma((3,)),
        dma, dma((CHUNKS,)), dma,
        pltpu.SemaphoreType.REGULAR((3,)),
    ]
    kept = (V((SEQ, WIDTH), BF16), V((SEQ, DK, DK), F32))
    result, new_state = pl.pallas_call(
        kernel,
        out_shape=kept,
        in_specs=[pl.BlockSpec(memory_space=pltpu.HBM)] * len(operands),
        out_specs=tuple(pl.BlockSpec(memory_space=pltpu.VMEM) for _ in kept),
        scratch_shapes=scratch,
        compiler_params=pltpu.CompilerParams(
            collective_id=0, has_side_effects=True, vmem_limit_bytes=64000000
        ),
    )(*operands)
    result, new_state = pl.pallas_call(
        write_out,
        out_shape=tuple(jax.ShapeDtypeStruct(k.shape, k.dtype) for k in kept),
        in_specs=[pl.BlockSpec(memory_space=pltpu.VMEM)] * 2,
        out_specs=tuple(pl.BlockSpec(memory_space=pltpu.HBM) for _ in kept),
        scratch_shapes=[dma((2,))],
        compiler_params=pltpu.CompilerParams(vmem_limit_bytes=8 * 1024 * 1024),
    )(result, new_state)
    return result, new_state.reshape(state_in.shape)


def solution(mesh):
    return jax.shard_map(
        per_device,
        mesh=mesh,
        in_specs=(
            P("ep", "tp"), P("ep", "tp", None, None), P(), P(None, "tp"), P(None, "tp"), P(None, "tp"), P(None, "tp"),
            P(), P(), P(), P(), P(None, "tp"), P(), P("ep", None), P("ep", None), P("ep", None, "tp"),
            P("ep", None, "tp"), P("ep", "tp", None), P(None, "ep"), P(None, "ep"), P("ep", None), P("tp"),
        ),
        out_specs=(P("ep", "tp"), P("ep", "tp", None, None)),
        check_vma=False,
    )
```

```python
import functools

import jax
import jax.numpy as jnp
from jax import lax
from jax.experimental import pallas as pl
from jax.experimental.pallas import tpu as pltpu
from jax.sharding import PartitionSpec as P

EPS = 1e-06
MESH = pl.DeviceIdType.MESH
F32, BF16, I32 = jnp.float32, jnp.bfloat16, jnp.int32

NX, NZ, NTP, NEP = 4, 8, 8, 32
SEQ, D, WIDTH, DK, CAP = 32, 2048, 256, 128, 4
ROWS = NEP * CAP
FE, FD = 384, 128
PITCH = 72
CHUNKS = 4
WIDE = D // CHUNKS
SENT = 7 * 8 + 7 * 4 + 63 + 31 + 24 * 8 + 3 * 32 + 4 * 32 + 12 * 16 + 4 * 32 + 3 * 32 + 63 + 31
FAR_TP = FAR_Z = (4, 3, 5, 2, 6, 1, 7)
NEAR_TP = (1, 7, 2, 6)
ROUND_OF = (0, 1, 2, 3, 4, 3, 2, 1)
HALVES = ((0, 1, 7, 2), (6, 3, 5, 4))


def silu(v):
    return v * jax.nn.sigmoid(v)


def dot(a, b):
    return jnp.dot(a, b, preferred_element_type=F32)


def dot_t(a, b):
    return lax.dot_general(a, b, (((1,), (1,)), ((), ())), preferred_element_type=F32)


def t_dot(a, b):
    return lax.dot_general(a, b, (((0,), (0,)), ((), ())), preferred_element_type=F32)


def iota(shape, dim):
    return lax.broadcasted_iota(I32, shape, dim)


def kernel(
    hidden, state, attn_gain, wq, wk, wv, wg, w_beta, w_decay, decay_scale, head_gain, w_out, ffn_gain, ids, route,
    eg, eu, ed, dg, du, dd, mix,
    result, new_state,
    hid_all, v_state, v_again, v_w, v_wb, v_wd, v_dscale, v_hgain, v_wo, v_fgain, v_ids, v_route,
    v_e, v_ed, v_d, v_dd, v_mix,
    heads_all, mixed_s, send_mat, take_mat,
    disp, xa, stage, stage_e, square_e, acc_e, pb, pr, qs, yr, ret, rb,
    own_tok, dx, xn_d, px, xr, sums_x, zs, fr, count,
    l_sem, send, a_recv, h_recv, t_recv, d_recv, x_recv, y_recv, c_recv, p_recv, q_recv, b_recv, u_recv, w_recv, met,
):
    ep = lax.axis_index("ep")
    t = lax.axis_index("tp")
    z, x = lax.div(ep, NX), lax.rem(ep, NX)
    y, c = lax.div(t, 2), lax.rem(t, 2)

    def tp_peer(d):
        return ep, lax.rem(t + d, NTP)

    def ep_peer(d):
        return lax.rem(ep + d, NEP), t

    def z_peer(d):
        return lax.rem(z + d, NZ) * NX + x, t

    def x_peer(d):
        return z * NX + lax.rem(x + d, NX), t

    def y_peer(d):
        return ep, lax.rem(y + d, 4) * 2 + c

    partner = (ep, y * 2 + 1 - c)

    def remote(src, dst, recv, peer):
        pltpu.make_async_remote_copy(
            src_ref=src, dst_ref=dst, send_sem=send, recv_sem=recv, device_id=peer, device_id_type=MESH
        ).start()

    def take(view, sem):
        pltpu.make_async_copy(view, view, sem).wait()

    barrier = pltpu.get_barrier_semaphore()
    near = [tp_peer(d) for d in range(1, NTP)] + [z_peer(1), z_peer(NZ - 1), x_peer(1), x_peer(NX - 1)]
    for peer in near:
        pl.semaphore_signal(barrier, inc=1, device_id=peer, device_id_type=MESH)

    def tell(number, peers):
        for peer in peers:
            pl.semaphore_signal(met.at[number], inc=1, device_id=peer, device_id_type=MESH)

    loads = {}
    pairs = (
        ("hid", (hidden,), hid_all.at[t]), ("again", (attn_gain,), v_again), ("w", (wq, wk, wv, wg), v_w),
        ("wb", (w_beta,), v_wb), ("wd", (w_decay,), v_wd), ("dscale", (decay_scale,), v_dscale),
        ("hgain", (head_gain,), v_hgain), ("ids", (ids,), v_ids), ("route", (route,), v_route),
        ("state", (state,), v_state), ("wo", (w_out,), v_wo), ("fgain", (ffn_gain,), v_fgain), ("mix", (mix,), v_mix),
        ("d", (dg, du), v_d), ("dd", (dd,), v_dd), ("e", (eg, eu), v_e), ("ed", (ed,), v_ed),
    )
    for number, (name, sources, dst) in enumerate(pairs):
        loads[name] = functools.partial(take, dst, l_sem.at[number])
        for place, src in enumerate(sources):
            part = dst.at[place] if len(sources) > 1 else dst
            pltpu.make_async_copy(src, part, l_sem.at[number]).start()

    loads["hid"]()
    pl.semaphore_wait(barrier, len(near))

    for d in FAR_TP:
        remote(hid_all.at[t], hid_all.at[t], a_recv.at[0 if d in NEAR_TP else 1], tp_peer(d))
    tell(0, (z_peer(1), z_peer(NZ - 1), x_peer(1), x_peer(NX - 1)))
    loads["ids"]()
    loads["route"]()
    first, second = v_ids[0:1, :], v_ids[1:2, :]
    expert = iota((NEP, SEQ), 0)
    is_first, is_second = first == expert, second == expert
    chosen = jnp.where(is_first | is_second, 1.0, 0.0)
    earlier = jnp.where(iota((SEQ, SEQ), 0) < iota((SEQ, SEQ), 1), 1.0, 0.0).astype(BF16)
    before = dot(chosen.astype(BF16), earlier)
    place = (chosen * (before + 1.0)).astype(BF16)
    row = iota((NEP * 8, NEP), 0)
    spread = jnp.where(row // 8 == iota((NEP * 8, NEP), 1), 1.0, 0.0).astype(BF16)
    hit = dot(spread, place) == ((row % 8) // 2 + 1).astype(F32)
    weight = jnp.where(is_first, v_route[0:1, :], 0.0) + jnp.where(is_second, v_route[1:2, :], 0.0)
    coarse = weight.astype(BF16)
    fine = (weight - coarse.astype(F32)).astype(BF16)
    coarse, fine = dot(spread, coarse), dot(spread, fine)
    for h in range(2):
        here = hit & (row % 2 == h)
        send_mat[h, : NEP * 8] = jnp.where(here, 1.0, 0.0).astype(BF16)
        take_mat[2 * h] = jnp.where(here, coarse, 0.0).astype(BF16)
        take_mat[2 * h + 1] = jnp.where(here, fine, 0.0).astype(BF16)
    t_row, t_col = iota((NTP * 8, SEQ), 0), iota((NTP * 8, SEQ), 1)
    for h in range(2):
        send_mat[h, NEP * 8 :] = jnp.where((t_row // 2 == t_col) & (t_row % 2 == h), 1.0, 0.0).astype(BF16)

    pl.semaphore_wait(met.at[0], 4)
    tell(1, (z_peer(2), z_peer(NZ - 2)))
    for name in ("again", "w", "wb", "wd"):
        loads[name]()

    def project(slots):
        sums = None
        for b in slots:
            cols = pl.ds(pl.multiple_of(b * WIDTH, WIDTH), WIDTH)
            wide = hid_all[b].astype(F32)
            part = (wide * v_again[b]).astype(BF16)
            outs = [wide * wide] + [dot(part, v_w[i, cols, :]) for i in range(4)]
            outs += [dot_t(part, v_wb[:, cols]), dot_t(part, v_wd[:, cols])]
            sums = outs if sums is None else [total + out for total, out in zip(sums, outs)]
        return sums

    take(hid_all.at[pl.ds(0, 4)], a_recv.at[0])
    sums = project([t] + [lax.rem(t + NTP - d, NTP) for d in NEAR_TP])
    take(hid_all.at[pl.ds(0, 3)], a_recv.at[1])
    late = project([lax.rem(t + NTP - d, NTP) for d in (3, 5, 4)])
    sums = [total + part for total, part in zip(sums, late)]
    pl.semaphore_wait(met.at[1], 2)
    tell(2, (x_peer(1), x_peer(2), x_peer(3), z_peer(NZ // 2)))
    for name in ("dscale", "hgain"):
        loads[name]()
    scale = lax.rsqrt(jnp.sum(sums[0], axis=-1, keepdims=True) * (1.0 / D) + EPS)
    queries, keys, values, gates, beta_all, decay_all = (total * scale for total in sums[1:])
    queries = queries * lax.rsqrt(jnp.sum(queries * queries, axis=-1, keepdims=True) + EPS) * DK ** (-0.5)
    keys = keys * lax.rsqrt(jnp.sum(keys * keys, axis=-1, keepdims=True) + EPS)
    mine = iota((SEQ, NTP), 1) == t
    beta = jax.nn.sigmoid(jnp.sum(jnp.where(mine, beta_all, 0.0), axis=-1, keepdims=True))
    logit = jnp.sum(jnp.where(mine, decay_all, 0.0), axis=-1, keepdims=True)
    d_scale = jnp.sum(jnp.where(iota((1, NTP), 1) == t, v_dscale[...], 0.0), axis=-1, keepdims=True)
    soft = jnp.maximum(logit, 0.0) + jnp.log(1.0 + jnp.exp(-jnp.abs(logit)))
    decay = jnp.exp(-d_scale * soft)

    loads["state"]()
    qb, kb = queries.astype(BF16), keys.astype(BF16)
    diag = iota((16, 1024), 1) // DK == iota((16, 1024), 0) % 8
    by_query, by_key = [], []
    for i in range(SEQ // 8):
        both = jnp.concatenate([qb[8 * i : 8 * i + 8].astype(F32), kb[8 * i : 8 * i + 8].astype(F32)], axis=0)
        lhs = jnp.where(diag, jnp.concatenate([both] * 8, axis=1), 0.0).astype(BF16)
        rhs = v_state[8 * i : 8 * i + 8].reshape(1024, DK).astype(BF16)
        out = dot(lhs, rhs)
        by_query.append(out[:8])
        by_key.append(out[8:])
    s_q = jnp.concatenate(by_query, axis=0)
    s_k = jnp.concatenate(by_key, axis=0)
    match = beta * jnp.sum(queries * keys, axis=-1, keepdims=True)
    read = decay * (s_q - match * s_k) + match * values
    read = read * lax.rsqrt(jnp.mean(read * read, axis=-1, keepdims=True) + EPS) * v_hgain[...]
    heads_all[t] = (read * silu(gates)).astype(BF16)
    for d in FAR_TP:
        remote(heads_all.at[t], heads_all.at[t], h_recv, tp_peer(d))
    update = beta * (values - decay * s_k)
    keys_t = jnp.concatenate([keys, jnp.zeros((DK - SEQ, DK), F32)], axis=0).T
    decay_rows = jnp.broadcast_to(decay, (SEQ, DK))
    for s in range(SEQ):
        new_state[s] = decay_rows[s : s + 1] * v_state[s] + keys_t[:, s : s + 1] * update[s : s + 1]

    pl.semaphore_wait(met.at[2], 4)
    loads["wo"]()
    take(heads_all.at[pl.ds(0, 7)], h_recv)
    wide = hid_all[t].astype(F32)
    for b in range(NTP):
        wide = wide + dot(heads_all[b], v_wo[b * DK : (b + 1) * DK, :])
    mixed = wide.astype(BF16)
    mixed_s[...] = mixed
    low, high = mixed[:, :128], mixed[:, 128:]

    moved = (dot(send_mat[0], low) + dot(send_mat[1], high)).reshape(NEP + NTP, 8, 128).astype(BF16)
    disp[...] = moved[:NEP]
    own_tok[...] = moved[NEP:]
    for dz in FAR_Z + (0,):
        base = z_peer(dz)[0] - x
        for d in (2, 1, 3, 0):
            if dz or d:
                to = base + lax.rem(x + d, NX)
                remote(disp.at[to], xa.at[t, ep], d_recv.at[ROUND_OF[dz]], (to, t))
    xa[t, ep] = disp[ep]
    for dz in FAR_Z + (0,):
        for d in FAR_TP + (0,):
            if dz or d:
                to = lax.rem(t + d, NTP)
                remote(own_tok.at[to], dx.at[ep, t], t_recv.at[ROUND_OF[dz]], (z_peer(dz)[0], to))
    dx[ep, t] = own_tok[t]
    for distance in range(NZ // 2 + 1):
        group = [dz for dz in range(NZ) if ROUND_OF[dz] == distance]
        blocks = [lax.rem(z + NZ - dz, NZ) for dz in group]
        take(disp.at[pl.ds(0, NX * len(group) if distance else NX - 1)], d_recv.at[distance])
        for from_z in blocks:
            block = xa.at[t, pl.ds(from_z * NX, NX)]
            for d in (2, 1, 3):
                remote(block, block, y_recv.at[d - 1], y_peer(d))
            remote(block, block, c_recv.at[0], partner)
        take(fr.at[pl.ds(0, NTP * len(group) if distance else NTP - 1)], t_recv.at[distance])
        for dz, from_z in zip(group, blocks):
            block = dx.at[from_z * NX + x]
            for d in (2, 1, 3):
                remote(block, block, x_recv.at[int(dz in HALVES[1])], x_peer(d))
    loads["fgain"]()
    for name in ("d", "dd"):
        loads[name]()

    def dense(half):
        take(dx.at[pl.ds(0, 12)], x_recv.at[half])
        for d in range(NX):
            xx = lax.rem(x + NX - d, NX)
            for k, dz in enumerate(HALVES[half]):
                block = dx[lax.rem(z + NZ - dz, NZ) * NX + xx]
                stage[pl.ds((d * 4 + k) * PITCH, 64), :] = block.astype(F32).reshape(64, 128)
            parts = [
                [stage[pl.ds(d * 4 * PITCH + (b // 2) * 8 + j * 2 + b % 2, 4, stride=PITCH), :] for b in range(16)]
                for j in range(4)
            ]
            for j in range(4):
                square = parts[j][0] * parts[j][0]
                for b in range(1, 16):
                    square = square + parts[j][b] * parts[j][b]
                scale = lax.rsqrt(jnp.sum(square, axis=-1, keepdims=True) * (1.0 / D) + EPS)
                row = d * 16 + j * 4
                for b in range(16):
                    gain = v_fgain[b // 2, :, (b % 2) * 128 : (b % 2 + 1) * 128]
                    xn_d[row : row + 4, b * 128 : (b + 1) * 128] = parts[j][b] * scale * gain
        rows = xn_d[...].astype(BF16)
        hidden_d = (silu(dot(rows, v_d[0])) * dot(rows, v_d[1])).astype(BF16)
        for f in range(CHUNKS):
            out = dot(hidden_d, v_dd[:, f * WIDE : (f + 1) * WIDE]).astype(BF16)
            for d in range(NX):
                px[half, d, f] = out[d * 16 : (d + 1) * 16]
            for d in (2, 1, 3):
                back = NX - d
                remote(px.at[half, d, f], xr.at[half, back - 1, f], u_recv.at[half, f], x_peer(back))

    for name in ("e", "ed"):
        loads[name]()

    def expert_slices(slots, start):
        square, outs = 0.0, [0.0, 0.0]
        for number, b in enumerate(slots):
            base = pl.multiple_of(b * WIDTH, WIDTH)
            stage_e[number] = xa[b].astype(F32).reshape(256, 128)
            parts = [stage_e[number, pl.ds(h, ROWS, stride=2), :] for h in range(2)]
            square = square + parts[0] * parts[0] + parts[1] * parts[1]
            gain = v_fgain[b]
            rows = jnp.concatenate([parts[h] * gain[:, h * 128 : (h + 1) * 128] for h in range(2)], axis=1).astype(BF16)
            outs = [outs[i] + dot(rows, v_e[i, pl.ds(base, WIDTH), :]) for i in range(2)]
        square_e[...] = square if start else square_e[...] + square
        for i in range(2):
            acc_e[i] = outs[i] if start else acc_e[i] + outs[i]

    expert_slices([t], True)
    take(xa.at[0], c_recv.at[0])
    expert_slices([y * 2 + 1 - c], False)
    for d in (1, 3, 2):
        take(xa.at[0], y_recv.at[d - 1])
        block = xa.at[lax.rem(y + 4 - d, 4) * 2 + c]
        remote(block, block, c_recv.at[1], partner)
    expert_slices([lax.rem(y + 4 - d, 4) * 2 + c for d in (1, 3, 2)], False)
    dense(0)
    take(xa.at[pl.ds(0, 3)], c_recv.at[1])
    expert_slices([lax.rem(y + 4 - d, 4) * 2 + 1 - c for d in (1, 3, 2)], False)
    scale = lax.rsqrt(jnp.sum(square_e[...], axis=-1, keepdims=True) * (1.0 / D) + EPS)
    inner = (silu(acc_e[0] * scale) * (acc_e[1] * scale)).astype(BF16)
    for b in range(NTP):
        pb[b] = dot(inner, v_ed[:, b * WIDTH : (b + 1) * WIDTH]).astype(BF16)
    for d in (2, 1, 3, 0):
        there = lax.rem(y + d, 4)
        remote(pb.at[there * 2 + 1 - c], pr.at[there], p_recv.at[d], partner)
    dense(1)
    for d in (2, 1, 3, 0):
        there = lax.rem(y + d, 4)
        take(pr.at[0], p_recv.at[d])
        qs[there] = (pb[there * 2 + c].astype(F32) + pr[there].astype(F32)).astype(BF16)
        if d > 0:
            remote(qs.at[there], yr.at[d - 1], q_recv.at[d - 1], y_peer(d))

    def sum_x(half, f):
        take(xr.at[half, :, f], u_recv.at[half, f])
        total = px[half, 0, f].astype(F32)
        for d in range(3):
            total = total + xr[half, d, f].astype(F32)
        sums_x[...] = total
        for tt in range(2):
            for h in range(2):
                cols = slice(tt * WIDTH + h * 128, tt * WIDTH + (h + 1) * 128)
                for j in range(4):
                    stage[pl.ds(tt * 8 + j * 2 + h, 4, stride=PITCH), :] = sums_x[j * 4 : (j + 1) * 4, cols]
        for k, dz in enumerate(HALVES[half]):
            zs[half * 4 + k, 2 * f : 2 * f + 2] = stage[pl.ds(k * PITCH, 16), :].reshape(2, 8, 128).astype(BF16)
        for k, dz in reversed(tuple(enumerate(HALVES[half]))):
            to = z_peer(NZ - dz)[0]

            def piece(tt):
                remote(zs.at[half * 4 + k, tt], fr.at[z * NTP + t], w_recv, (to, tt))

            for tt in (2 * f, 2 * f + 1):
                if dz:
                    piece(tt)
                else:
                    pl.when(t != tt)(functools.partial(piece, tt))

    for f in range(CHUNKS):
        sum_x(0, f)
    sum_x(1, 0)
    sum_x(1, 1)
    sum_x(1, 2)
    sum_x(1, 3)
    fr[z * NTP + t] = zs[0, t]
    for d in (1, 3, 2):
        take(yr.at[0], q_recv.at[d - 1])
    total = qs[y].astype(F32)
    for d in range(3):
        total = total + yr[d].astype(F32)
    total = total.astype(BF16).astype(F32)
    for h in range(2):
        stage[pl.ds(h, ROWS, stride=2), :] = total[:, h * 128 : (h + 1) * 128]
    ret[...] = stage[pl.ds(0, 256), :].reshape(NEP, 8, 128).astype(BF16)

    for dz in FAR_Z + (0,):
        base = z_peer(dz)[0] - x
        for d in (2, 1, 3, 0):
            if dz or d:
                to = base + lax.rem(x + d, NX)
                remote(ret.at[to], rb.at[ep], b_recv, (to, t))
    rb[ep] = ret[ep]
    loads["mix"]()
    take(fr.at[pl.ds(0, NZ * NTP - 1)], w_recv)
    total = fr[0:NTP].astype(F32)
    for zz in range(1, NZ):
        total = total + fr[zz * NTP : (zz + 1) * NTP].astype(F32)
    stage[pl.ds(0, 64), :] = total.reshape(64, 128)
    take(rb.at[pl.ds(0, NEP - 1)], b_recv)
    back = rb[...].astype(F32).reshape(NEP * 8, 128).astype(BF16)
    for h in range(2):
        cols = slice(h * 128, (h + 1) * 128)
        moe = t_dot(take_mat[2 * h], back) + t_dot(take_mat[2 * h + 1], back)
        dense_out = stage[pl.ds(h, SEQ, stride=2), :]
        result[:, cols] = (
            mixed_s[:, cols].astype(F32) + moe + jax.nn.sigmoid(v_mix[:, cols]) * dense_out
        ).astype(BF16)
    take(count, send)


def write_out(result, new_state, result_out, state_out, sem):
    first = pltpu.make_async_copy(new_state, state_out, sem.at[0])
    second = pltpu.make_async_copy(result, result_out, sem.at[1])
    first.start()
    second.start()
    first.wait()
    second.wait()


def per_device(
    hidden_in, state_in, attn_gain, w_query, w_key, w_value, w_gate, w_beta, w_decay, decay_scale, head_gain, w_output,
    ffn_gain, expert_ids, route_weight, expert_gate, expert_up, expert_down, dense_gate, dense_up, dense_down, dense_mix,
):
    operands = (
        hidden_in, state_in.reshape(SEQ, DK, DK), attn_gain.reshape(NTP, 1, WIDTH), w_query, w_key, w_value, w_gate, w_beta.T,
        w_decay.T, decay_scale.reshape(1, NTP), head_gain.reshape(1, DK), w_output, ffn_gain.reshape(NTP, 1, WIDTH), expert_ids.T,
        route_weight.T, expert_gate[0], expert_up[0], expert_down[0], dense_gate, dense_up, dense_down,
        dense_mix.reshape(1, WIDTH),
    )
    V = pltpu.VMEM
    vmem_of = [
        V((NTP, SEQ, WIDTH), BF16), V((SEQ, DK, DK), F32), V((NTP, 1, WIDTH), F32), V((4, D, DK), BF16), V((NTP, D), BF16),
        V((NTP, D), BF16), V((1, NTP), F32), V((1, DK), F32), V((NTP * DK, WIDTH), BF16), V((NTP, 1, WIDTH), F32),
        V((2, SEQ), I32), V((2, SEQ), F32), V((2, D, FE), BF16), V((FE, D), BF16), V((2, D, FD), BF16),
        V((FD, D), BF16), V((1, WIDTH), F32),
    ]
    dma = pltpu.SemaphoreType.DMA
    scratch = vmem_of + [
        V((NTP, SEQ, DK), BF16), V((SEQ, WIDTH), BF16),
        V((2, (NEP + NTP) * 8, SEQ), BF16), V((4, NEP * 8, SEQ), BF16),
        V((NEP, 8, 128), BF16), V((NTP, NEP, 8, 128), BF16), V((16 * PITCH, 128), F32), V((3, 256, 128), F32),
        V((ROWS, 128), F32), V((2, ROWS, FE), F32), V((NTP, ROWS, WIDTH), BF16), V((4, ROWS, WIDTH), BF16), V((4, ROWS, WIDTH), BF16),
        V((3, ROWS, WIDTH), BF16), V((NEP, 8, 128), BF16), V((NEP, 8, 128), BF16),
        V((NTP, 8, 128), BF16), V((NEP, NTP, 8, 128), BF16), V((NX * 16, D), F32),
        V((2, NX, CHUNKS, 16, WIDE), BF16), V((2, NX - 1, CHUNKS, 16, WIDE), BF16), V((16, WIDE), F32),
        V((NZ, NTP, 8, 128), BF16), V((NZ * NTP, 8, 128), BF16), V((SENT, 8, 128), BF16),
        dma((17,)), dma, dma((2,)), dma, dma((5,)), dma((5,)), dma((2,)), dma((3,)), dma((2,)), dma((4,)), dma((3,)),
        dma, dma((2, CHUNKS)), dma,
        pltpu.SemaphoreType.REGULAR((3,)),
    ]
    kept = (V((SEQ, WIDTH), BF16), V((SEQ, DK, DK), F32))
    result, new_state = pl.pallas_call(
        kernel,
        out_shape=kept,
        in_specs=[pl.BlockSpec(memory_space=pltpu.HBM)] * len(operands),
        out_specs=tuple(pl.BlockSpec(memory_space=pltpu.VMEM) for _ in kept),
        scratch_shapes=scratch,
        compiler_params=pltpu.CompilerParams(
            collective_id=0, has_side_effects=True, vmem_limit_bytes=64000000
        ),
    )(*operands)
    result, new_state = pl.pallas_call(
        write_out,
        out_shape=tuple(jax.ShapeDtypeStruct(k.shape, k.dtype) for k in kept),
        in_specs=[pl.BlockSpec(memory_space=pltpu.VMEM)] * 2,
        out_specs=tuple(pl.BlockSpec(memory_space=pltpu.HBM) for _ in kept),
        scratch_shapes=[dma((2,))],
        compiler_params=pltpu.CompilerParams(vmem_limit_bytes=8 * 1024 * 1024),
    )(result, new_state)
    return result, new_state.reshape(state_in.shape)


def solution(mesh):
    return jax.shard_map(
        per_device,
        mesh=mesh,
        in_specs=(
            P("ep", "tp"), P("ep", "tp", None, None), P(), P(None, "tp"), P(None, "tp"), P(None, "tp"), P(None, "tp"),
            P(), P(), P(), P(), P(None, "tp"), P(), P("ep", None), P("ep", None), P("ep", None, "tp"),
            P("ep", None, "tp"), P("ep", "tp", None), P(None, "ep"), P(None, "ep"), P("ep", None), P("tp"),
        ),
        out_specs=(P("ep", "tp"), P("ep", "tp", None, None)),
        check_vma=False,
    )
```

```python
import functools

import jax
import jax.numpy as jnp
from jax import lax
from jax.experimental import pallas as pl
from jax.experimental.pallas import tpu as pltpu
from jax.sharding import PartitionSpec as P

EPS = 1e-06
MESH = pl.DeviceIdType.MESH
F32, BF16, I32 = jnp.float32, jnp.bfloat16, jnp.int32

NX, NZ, NTP, NEP = 4, 8, 8, 32
SEQ, D, WIDTH, DK, CAP = 32, 2048, 256, 128, 4
ROWS = NEP * CAP
FE, FD = 384, 128
PITCH = 72
CHUNKS = 4
WIDE = D // CHUNKS
SENT = 7 * 8 + 7 * 4 + 63 + 31 + 24 * 8 + 3 * 32 + 4 * 32 + 12 * 16 + 4 * 32 + 3 * 32 + 63 + 31
FAR_TP = FAR_Z = (4, 3, 5, 2, 6, 1, 7)
NEAR_TP = (1, 7, 2, 6)
ROUND_OF = (0, 1, 2, 3, 4, 3, 2, 1)
HALVES = ((0, 1, 7, 2), (6, 3, 5, 4))


def silu(v):
    return v * jax.nn.sigmoid(v)


def dot(a, b):
    return jnp.dot(a, b, preferred_element_type=F32)


def dot_t(a, b):
    return lax.dot_general(a, b, (((1,), (1,)), ((), ())), preferred_element_type=F32)


def t_dot(a, b):
    return lax.dot_general(a, b, (((0,), (0,)), ((), ())), preferred_element_type=F32)


def iota(shape, dim):
    return lax.broadcasted_iota(I32, shape, dim)


def kernel(
    hidden, state, attn_gain, wq, wk, wv, wg, w_beta, w_decay, decay_scale, head_gain, w_out, ffn_gain, ids, route,
    eg, eu, ed, dg, du, dd, mix,
    result, new_state,
    hid_all, v_state, v_again, v_w, v_wb, v_wd, v_dscale, v_hgain, v_wo, v_fgain, v_ids, v_route,
    v_e, v_ed, v_d, v_dd, v_mix,
    heads_all, mixed_s, send_mat, take_mat,
    disp, xa, stage, stage_e, square_e, acc_e, pb, pr, qs, yr, ret, rb,
    own_tok, dx, xn_d, square_d, px, xr, sums_x, zs, fr, count,
    l_sem, send, a_recv, h_recv, t_recv, d_recv, x_recv, y_recv, c_recv, p_recv, q_recv, b_recv, u_recv, w_recv, met,
):
    ep = lax.axis_index("ep")
    t = lax.axis_index("tp")
    z, x = lax.div(ep, NX), lax.rem(ep, NX)
    y, c = lax.div(t, 2), lax.rem(t, 2)

    def tp_peer(d):
        return ep, lax.rem(t + d, NTP)

    def ep_peer(d):
        return lax.rem(ep + d, NEP), t

    def z_peer(d):
        return lax.rem(z + d, NZ) * NX + x, t

    def x_peer(d):
        return z * NX + lax.rem(x + d, NX), t

    def y_peer(d):
        return ep, lax.rem(y + d, 4) * 2 + c

    partner = (ep, y * 2 + 1 - c)

    def remote(src, dst, recv, peer):
        pltpu.make_async_remote_copy(
            src_ref=src, dst_ref=dst, send_sem=send, recv_sem=recv, device_id=peer, device_id_type=MESH
        ).start()

    def take(view, sem):
        pltpu.make_async_copy(view, view, sem).wait()

    barrier = pltpu.get_barrier_semaphore()
    near = [tp_peer(d) for d in range(1, NTP)] + [z_peer(1), z_peer(NZ - 1), x_peer(1), x_peer(NX - 1)]
    for peer in near:
        pl.semaphore_signal(barrier, inc=1, device_id=peer, device_id_type=MESH)

    def tell(number, peers):
        for peer in peers:
            pl.semaphore_signal(met.at[number], inc=1, device_id=peer, device_id_type=MESH)

    loads = {}
    pairs = (
        ("hid", (hidden,), hid_all.at[t]), ("again", (attn_gain,), v_again), ("w", (wq, wk, wv, wg), v_w),
        ("wb", (w_beta,), v_wb), ("wd", (w_decay,), v_wd), ("dscale", (decay_scale,), v_dscale),
        ("hgain", (head_gain,), v_hgain), ("ids", (ids,), v_ids), ("route", (route,), v_route),
        ("state", (state,), v_state), ("wo", (w_out,), v_wo), ("fgain", (ffn_gain,), v_fgain), ("mix", (mix,), v_mix),
        ("d", (dg, du), v_d), ("dd", (dd,), v_dd), ("e", (eg, eu), v_e), ("ed", tuple(ed.at[:, pl.ds(b * WIDTH, WIDTH)] for b in range(NTP)), v_ed),
    )
    for number, (name, sources, dst) in enumerate(pairs):
        loads[name] = functools.partial(take, dst, l_sem.at[number])
        for place, src in enumerate(sources):
            part = dst.at[place] if len(sources) > 1 else dst
            pltpu.make_async_copy(src, part, l_sem.at[number]).start()

    loads["hid"]()
    pl.semaphore_wait(barrier, len(near))

    for d in FAR_TP:
        remote(hid_all.at[t], hid_all.at[t], a_recv.at[0 if d in NEAR_TP else 1], tp_peer(d))
    tell(0, (z_peer(1), z_peer(NZ - 1), x_peer(1), x_peer(NX - 1)))
    loads["ids"]()
    loads["route"]()
    first, second = v_ids[0:1, :], v_ids[1:2, :]
    expert = iota((NEP, SEQ), 0)
    is_first, is_second = first == expert, second == expert
    chosen = jnp.where(is_first | is_second, 1.0, 0.0)
    earlier = jnp.where(iota((SEQ, SEQ), 0) < iota((SEQ, SEQ), 1), 1.0, 0.0).astype(BF16)
    before = dot(chosen.astype(BF16), earlier)
    place = (chosen * (before + 1.0)).astype(BF16)
    row = iota((NEP * 8, NEP), 0)
    spread = jnp.where(row // 8 == iota((NEP * 8, NEP), 1), 1.0, 0.0).astype(BF16)
    hit = dot(spread, place) == ((row % 8) // 2 + 1).astype(F32)
    weight = jnp.where(is_first, v_route[0:1, :], 0.0) + jnp.where(is_second, v_route[1:2, :], 0.0)
    coarse = weight.astype(BF16)
    fine = (weight - coarse.astype(F32)).astype(BF16)
    coarse, fine = dot(spread, coarse), dot(spread, fine)
    for h in range(2):
        here = hit & (row % 2 == h)
        send_mat[h, : NEP * 8] = jnp.where(here, 1.0, 0.0).astype(BF16)
        take_mat[2 * h] = jnp.where(here, coarse, 0.0).astype(BF16)
        take_mat[2 * h + 1] = jnp.where(here, fine, 0.0).astype(BF16)
    t_row, t_col = iota((NTP * 8, SEQ), 0), iota((NTP * 8, SEQ), 1)
    for h in range(2):
        send_mat[h, NEP * 8 :] = jnp.where((t_row // 2 == t_col) & (t_row % 2 == h), 1.0, 0.0).astype(BF16)

    pl.semaphore_wait(met.at[0], 4)
    tell(1, (z_peer(2), z_peer(NZ - 2)))
    for name in ("again", "w", "wb", "wd"):
        loads[name]()

    def project(slots):
        sums = None
        for b in slots:
            cols = pl.ds(pl.multiple_of(b * WIDTH, WIDTH), WIDTH)
            wide = hid_all[b].astype(F32)
            part = (wide * v_again[b]).astype(BF16)
            outs = [wide * wide] + [dot(part, v_w[i, cols, :]) for i in range(4)]
            outs += [dot_t(part, v_wb[:, cols]), dot_t(part, v_wd[:, cols])]
            sums = outs if sums is None else [total + out for total, out in zip(sums, outs)]
        return sums

    take(hid_all.at[pl.ds(0, 4)], a_recv.at[0])
    sums = project([t] + [lax.rem(t + NTP - d, NTP) for d in NEAR_TP])
    take(hid_all.at[pl.ds(0, 3)], a_recv.at[1])
    late = project([lax.rem(t + NTP - d, NTP) for d in (3, 5, 4)])
    sums = [total + part for total, part in zip(sums, late)]
    pl.semaphore_wait(met.at[1], 2)
    tell(2, (x_peer(1), x_peer(2), x_peer(3), z_peer(NZ // 2)))
    for name in ("dscale", "hgain"):
        loads[name]()
    scale = lax.rsqrt(jnp.sum(sums[0], axis=-1, keepdims=True) * (1.0 / D) + EPS)
    queries, keys, values, gates, beta_all, decay_all = (total * scale for total in sums[1:])
    queries = queries * lax.rsqrt(jnp.sum(queries * queries, axis=-1, keepdims=True) + EPS) * DK ** (-0.5)
    keys = keys * lax.rsqrt(jnp.sum(keys * keys, axis=-1, keepdims=True) + EPS)
    mine = iota((SEQ, NTP), 1) == t
    beta = jax.nn.sigmoid(jnp.sum(jnp.where(mine, beta_all, 0.0), axis=-1, keepdims=True))
    logit = jnp.sum(jnp.where(mine, decay_all, 0.0), axis=-1, keepdims=True)
    d_scale = jnp.sum(jnp.where(iota((1, NTP), 1) == t, v_dscale[...], 0.0), axis=-1, keepdims=True)
    soft = jnp.maximum(logit, 0.0) + jnp.log(1.0 + jnp.exp(-jnp.abs(logit)))
    decay = jnp.exp(-d_scale * soft)

    loads["state"]()
    qb, kb = queries.astype(BF16), keys.astype(BF16)
    diag = iota((16, 1024), 1) // DK == iota((16, 1024), 0) % 8
    by_query, by_key = [], []
    for i in range(SEQ // 8):
        both = jnp.concatenate([qb[8 * i : 8 * i + 8].astype(F32), kb[8 * i : 8 * i + 8].astype(F32)], axis=0)
        lhs = jnp.where(diag, jnp.concatenate([both] * 8, axis=1), 0.0).astype(BF16)
        rhs = v_state[8 * i : 8 * i + 8].reshape(1024, DK).astype(BF16)
        out = dot(lhs, rhs)
        by_query.append(out[:8])
        by_key.append(out[8:])
    s_q = jnp.concatenate(by_query, axis=0)
    s_k = jnp.concatenate(by_key, axis=0)
    match = beta * jnp.sum(queries * keys, axis=-1, keepdims=True)
    read = decay * (s_q - match * s_k) + match * values
    read = read * lax.rsqrt(jnp.mean(read * read, axis=-1, keepdims=True) + EPS) * v_hgain[...]
    heads_all[t] = (read * silu(gates)).astype(BF16)
    for d in FAR_TP:
        remote(heads_all.at[t], heads_all.at[t], h_recv, tp_peer(d))
    update = beta * (values - decay * s_k)
    keys_t = jnp.concatenate([keys, jnp.zeros((DK - SEQ, DK), F32)], axis=0).T
    decay_rows = jnp.broadcast_to(decay, (SEQ, DK))
    for s in range(SEQ):
        new_state[s] = decay_rows[s : s + 1] * v_state[s] + keys_t[:, s : s + 1] * update[s : s + 1]

    pl.semaphore_wait(met.at[2], 4)
    loads["wo"]()
    take(heads_all.at[pl.ds(0, 7)], h_recv)
    wide = hid_all[t].astype(F32)
    for b in range(NTP):
        wide = wide + dot(heads_all[b], v_wo[b * DK : (b + 1) * DK, :])
    mixed = wide.astype(BF16)
    mixed_s[...] = mixed
    low, high = mixed[:, :128], mixed[:, 128:]

    moved = (dot(send_mat[0], low) + dot(send_mat[1], high)).reshape(NEP + NTP, 8, 128).astype(BF16)
    disp[...] = moved[:NEP]
    own_tok[...] = moved[NEP:]
    for dz in FAR_Z + (0,):
        base = z_peer(dz)[0] - x
        for d in (2, 1, 3, 0):
            if dz or d:
                to = base + lax.rem(x + d, NX)
                remote(disp.at[to], xa.at[t, ep], d_recv.at[ROUND_OF[dz]], (to, t))
    xa[t, ep] = disp[ep]
    for dz in FAR_Z + (0,):
        for d in FAR_TP + (0,):
            if dz or d:
                to = lax.rem(t + d, NTP)
                remote(own_tok.at[to], dx.at[ep, t], t_recv.at[ROUND_OF[dz]], (z_peer(dz)[0], to))
    dx[ep, t] = own_tok[t]
    for distance in range(NZ // 2 + 1):
        group = [dz for dz in range(NZ) if ROUND_OF[dz] == distance]
        blocks = [lax.rem(z + NZ - dz, NZ) for dz in group]
        take(disp.at[pl.ds(0, NX * len(group) if distance else NX - 1)], d_recv.at[distance])
        for from_z in blocks:
            block = xa.at[t, pl.ds(from_z * NX, NX)]
            for d in (2, 1, 3):
                remote(block, block, y_recv.at[d - 1], y_peer(d))
            remote(block, block, c_recv.at[0], partner)
        take(fr.at[pl.ds(0, NTP * len(group) if distance else NTP - 1)], t_recv.at[distance])
        for dz, from_z in zip(group, blocks):
            block = dx.at[from_z * NX + x]
            for d in (2, 1, 3):
                remote(block, block, x_recv.at[int(dz in HALVES[1])], x_peer(d))
    loads["fgain"]()
    for name in ("d", "dd"):
        loads[name]()

    def load_rows(half, d):
        xx = lax.rem(x + NX - d, NX)
        for k, dz in enumerate(HALVES[half]):
            block = dx[lax.rem(z + NZ - dz, NZ) * NX + xx]
            stage[pl.ds((d * 4 + k) * PITCH, 64), :] = block.astype(F32).reshape(64, 128)
        for j in range(4):
            row = d * 16 + j * 4
            square = 0.0
            for b in range(16):
                part = stage[pl.ds(d * 4 * PITCH + (b // 2) * 8 + j * 2 + b % 2, 4, stride=PITCH), :]
                square = square + part * part
                gain = v_fgain[b // 2, :, (b % 2) * 128 : (b % 2 + 1) * 128]
                xn_d[half, row : row + 4, b * 128 : (b + 1) * 128] = part * gain
            square_d[half, row : row + 4] = square

    def dense(half):
        take(dx.at[pl.ds(0, 12)], x_recv.at[half])
        for d in (1, 3, 2):
            load_rows(half, d)
        rows = xn_d[half].astype(BF16)
        scale = lax.rsqrt(jnp.sum(square_d[half], axis=-1, keepdims=True) * (1.0 / D) + EPS)
        hidden_d = (silu(dot(rows, v_d[0]) * scale) * (dot(rows, v_d[1]) * scale)).astype(BF16)
        for f in range(CHUNKS):
            out = dot(hidden_d, v_dd[:, f * WIDE : (f + 1) * WIDE]).astype(BF16)
            for d in range(NX):
                px[half, d, f] = out[d * 16 : (d + 1) * 16]
        for f in range(CHUNKS):
            for d in (2, 1, 3):
                back = NX - d
                remote(px.at[half, d, f], xr.at[half, back - 1, f], u_recv.at[half, f], x_peer(back))

    load_rows(0, 0)
    load_rows(1, 0)
    for name in ("e", "ed"):
        loads[name]()

    def expert_slices(slots, start):
        square, outs = 0.0, [0.0, 0.0]
        for number, b in enumerate(slots):
            base = pl.multiple_of(b * WIDTH, WIDTH)
            stage_e[number] = xa[b].astype(F32).reshape(256, 128)
            parts = [stage_e[number, pl.ds(h, ROWS, stride=2), :] for h in range(2)]
            square = square + parts[0] * parts[0] + parts[1] * parts[1]
            gain = v_fgain[b]
            rows = jnp.concatenate([parts[h] * gain[:, h * 128 : (h + 1) * 128] for h in range(2)], axis=1).astype(BF16)
            outs = [outs[i] + dot(rows, v_e[i, pl.ds(base, WIDTH), :]) for i in range(2)]
        square_e[...] = square if start else square_e[...] + square
        for i in range(2):
            acc_e[i] = outs[i] if start else acc_e[i] + outs[i]

    expert_slices([t], True)
    take(xa.at[0], c_recv.at[0])
    expert_slices([y * 2 + 1 - c], False)
    for d in (1, 3, 2):
        take(xa.at[0], y_recv.at[d - 1])
        block = xa.at[lax.rem(y + 4 - d, 4) * 2 + c]
        remote(block, block, c_recv.at[1], partner)
    expert_slices([lax.rem(y + 4 - d, 4) * 2 + c for d in (1, 3, 2)], False)
    dense(0)
    take(xa.at[pl.ds(0, 3)], c_recv.at[1])
    expert_slices([lax.rem(y + 4 - d, 4) * 2 + 1 - c for d in (1, 3, 2)], False)
    scale = lax.rsqrt(jnp.sum(square_e[...], axis=-1, keepdims=True) * (1.0 / D) + EPS)
    inner = (silu(acc_e[0] * scale) * (acc_e[1] * scale)).astype(BF16)

    def down(core):
        for d in (2, 1, 3, 0):
            b = lax.rem(y + d, 4) * 2 + core
            pb[b] = dot(inner, v_ed[b]).astype(BF16)

    down(1 - c)
    for d in (2, 1, 3, 0):
        there = lax.rem(y + d, 4)
        remote(pb.at[there * 2 + 1 - c], pr.at[there], p_recv.at[d], partner)
    down(c)
    dense(1)
    for d in (2, 1, 3, 0):
        there = lax.rem(y + d, 4)
        take(pr.at[0], p_recv.at[d])
        qs[there] = (pb[there * 2 + c].astype(F32) + pr[there].astype(F32)).astype(BF16)
        if d > 0:
            remote(qs.at[there], yr.at[d - 1], q_recv.at[d - 1], y_peer(d))

    def sum_x(half, f):
        take(xr.at[half, :, f], u_recv.at[half, f])
        total = px[half, 0, f].astype(F32)
        for d in range(3):
            total = total + xr[half, d, f].astype(F32)
        sums_x[...] = total
        for tt in range(2):
            for h in range(2):
                cols = slice(tt * WIDTH + h * 128, tt * WIDTH + (h + 1) * 128)
                for j in range(4):
                    stage[pl.ds(tt * 8 + j * 2 + h, 4, stride=PITCH), :] = sums_x[j * 4 : (j + 1) * 4, cols]
        for k, dz in enumerate(HALVES[half]):
            zs[half * 4 + k, 2 * f : 2 * f + 2] = stage[pl.ds(k * PITCH, 16), :].reshape(2, 8, 128).astype(BF16)
        for k, dz in reversed(tuple(enumerate(HALVES[half]))):
            to = z_peer(NZ - dz)[0]

            def piece(tt):
                remote(zs.at[half * 4 + k, tt], fr.at[z * NTP + t], w_recv, (to, tt))

            for tt in (2 * f, 2 * f + 1):
                if dz:
                    piece(tt)
                else:
                    pl.when(t != tt)(functools.partial(piece, tt))

    for f in range(CHUNKS):
        sum_x(0, f)
    sum_x(1, 0)
    sum_x(1, 1)
    sum_x(1, 2)
    sum_x(1, 3)
    fr[z * NTP + t] = zs[0, t]
    for d in (1, 3, 2):
        take(yr.at[0], q_recv.at[d - 1])
    total = qs[y].astype(F32)
    for d in range(3):
        total = total + yr[d].astype(F32)
    total = total.astype(BF16).astype(F32)
    for h in range(2):
        stage[pl.ds(h, ROWS, stride=2), :] = total[:, h * 128 : (h + 1) * 128]
    ret[...] = stage[pl.ds(0, 256), :].reshape(NEP, 8, 128).astype(BF16)

    for dz in FAR_Z + (0,):
        base = z_peer(dz)[0] - x
        for d in (2, 1, 3, 0):
            if dz or d:
                to = base + lax.rem(x + d, NX)
                remote(ret.at[to], rb.at[ep], b_recv, (to, t))
    rb[ep] = ret[ep]
    loads["mix"]()
    take(fr.at[pl.ds(0, NZ * NTP - 1)], w_recv)
    total = fr[0:NTP].astype(F32)
    for zz in range(1, NZ):
        total = total + fr[zz * NTP : (zz + 1) * NTP].astype(F32)
    stage[pl.ds(0, 64), :] = total.reshape(64, 128)
    take(rb.at[pl.ds(0, NEP - 1)], b_recv)
    back = rb[...].astype(F32).reshape(NEP * 8, 128).astype(BF16)
    for h in range(2):
        cols = slice(h * 128, (h + 1) * 128)
        moe = t_dot(take_mat[2 * h], back) + t_dot(take_mat[2 * h + 1], back)
        dense_out = stage[pl.ds(h, SEQ, stride=2), :]
        result[:, cols] = (
            mixed_s[:, cols].astype(F32) + moe + jax.nn.sigmoid(v_mix[:, cols]) * dense_out
        ).astype(BF16)
    take(count, send)


def write_out(result, new_state, result_out, state_out, sem):
    first = pltpu.make_async_copy(new_state, state_out, sem.at[0])
    second = pltpu.make_async_copy(result, result_out, sem.at[1])
    first.start()
    second.start()
    first.wait()
    second.wait()


def per_device(
    hidden_in, state_in, attn_gain, w_query, w_key, w_value, w_gate, w_beta, w_decay, decay_scale, head_gain, w_output,
    ffn_gain, expert_ids, route_weight, expert_gate, expert_up, expert_down, dense_gate, dense_up, dense_down, dense_mix,
):
    operands = (
        hidden_in, state_in.reshape(SEQ, DK, DK), attn_gain.reshape(NTP, 1, WIDTH), w_query, w_key, w_value, w_gate, w_beta.T,
        w_decay.T, decay_scale.reshape(1, NTP), head_gain.reshape(1, DK), w_output, ffn_gain.reshape(NTP, 1, WIDTH), expert_ids.T,
        route_weight.T, expert_gate[0], expert_up[0], expert_down[0], dense_gate, dense_up, dense_down,
        dense_mix.reshape(1, WIDTH),
    )
    V = pltpu.VMEM
    vmem_of = [
        V((NTP, SEQ, WIDTH), BF16), V((SEQ, DK, DK), F32), V((NTP, 1, WIDTH), F32), V((4, D, DK), BF16), V((NTP, D), BF16),
        V((NTP, D), BF16), V((1, NTP), F32), V((1, DK), F32), V((NTP * DK, WIDTH), BF16), V((NTP, 1, WIDTH), F32),
        V((2, SEQ), I32), V((2, SEQ), F32), V((2, D, FE), BF16), V((NTP, FE, WIDTH), BF16), V((2, D, FD), BF16),
        V((FD, D), BF16), V((1, WIDTH), F32),
    ]
    dma = pltpu.SemaphoreType.DMA
    scratch = vmem_of + [
        V((NTP, SEQ, DK), BF16), V((SEQ, WIDTH), BF16),
        V((2, (NEP + NTP) * 8, SEQ), BF16), V((4, NEP * 8, SEQ), BF16),
        V((NEP, 8, 128), BF16), V((NTP, NEP, 8, 128), BF16), V((16 * PITCH, 128), F32), V((3, 256, 128), F32),
        V((ROWS, 128), F32), V((2, ROWS, FE), F32), V((NTP, ROWS, WIDTH), BF16), V((4, ROWS, WIDTH), BF16), V((4, ROWS, WIDTH), BF16),
        V((3, ROWS, WIDTH), BF16), V((NEP, 8, 128), BF16), V((NEP, 8, 128), BF16),
        V((NTP, 8, 128), BF16), V((NEP, NTP, 8, 128), BF16), V((2, NX * 16, D), F32), V((2, NX * 16, 128), F32),
        V((2, NX, CHUNKS, 16, WIDE), BF16), V((2, NX - 1, CHUNKS, 16, WIDE), BF16), V((16, WIDE), F32),
        V((NZ, NTP, 8, 128), BF16), V((NZ * NTP, 8, 128), BF16), V((SENT, 8, 128), BF16),
        dma((17,)), dma, dma((2,)), dma, dma((5,)), dma((5,)), dma((2,)), dma((3,)), dma((2,)), dma((4,)), dma((3,)),
        dma, dma((2, CHUNKS)), dma,
        pltpu.SemaphoreType.REGULAR((3,)),
    ]
    kept = (V((SEQ, WIDTH), BF16), V((SEQ, DK, DK), F32))
    result, new_state = pl.pallas_call(
        kernel,
        out_shape=kept,
        in_specs=[pl.BlockSpec(memory_space=pltpu.HBM)] * len(operands),
        out_specs=tuple(pl.BlockSpec(memory_space=pltpu.VMEM) for _ in kept),
        scratch_shapes=scratch,
        compiler_params=pltpu.CompilerParams(
            collective_id=0, has_side_effects=True, vmem_limit_bytes=64000000
        ),
    )(*operands)
    result, new_state = pl.pallas_call(
        write_out,
        out_shape=tuple(jax.ShapeDtypeStruct(k.shape, k.dtype) for k in kept),
        in_specs=[pl.BlockSpec(memory_space=pltpu.VMEM)] * 2,
        out_specs=tuple(pl.BlockSpec(memory_space=pltpu.HBM) for _ in kept),
        scratch_shapes=[dma((2,))],
        compiler_params=pltpu.CompilerParams(vmem_limit_bytes=8 * 1024 * 1024),
    )(result, new_state)
    return result, new_state.reshape(state_in.shape)


def solution(mesh):
    return jax.shard_map(
        per_device,
        mesh=mesh,
        in_specs=(
            P("ep", "tp"), P("ep", "tp", None, None), P(), P(None, "tp"), P(None, "tp"), P(None, "tp"), P(None, "tp"),
            P(), P(), P(), P(), P(None, "tp"), P(), P("ep", None), P("ep", None), P("ep", None, "tp"),
            P("ep", None, "tp"), P("ep", "tp", None), P(None, "ep"), P(None, "ep"), P("ep", None), P("tp"),
        ),
        out_specs=(P("ep", "tp"), P("ep", "tp", None, None)),
        check_vma=False,
    )
```

```python
import functools

import jax
import jax.numpy as jnp
from jax import lax
from jax.experimental import pallas as pl
from jax.experimental.pallas import tpu as pltpu
from jax.sharding import PartitionSpec as P

EPS = 1e-06
MESH = pl.DeviceIdType.MESH
F32, BF16, I32 = jnp.float32, jnp.bfloat16, jnp.int32

NX, NZ, NTP, NEP = 4, 8, 8, 32
SEQ, D, WIDTH, DK, CAP = 32, 2048, 256, 128, 4
ROWS = NEP * CAP
FE, FD = 384, 128
PITCH = 72
CHUNKS = 4
WIDE = D // CHUNKS
SENT = 7 * 8 + 7 * 4 + 63 + 31 + 24 * 8 + 3 * 32 + 4 * 32 + 12 * 16 + 4 * 32 + 3 * 32 + 63 + 31
FAR_TP = FAR_Z = (4, 3, 5, 2, 6, 1, 7)
NEAR_TP = (1, 7, 2, 6)
ROUND_OF = (0, 1, 2, 3, 4, 3, 2, 1)
HALVES = ((0, 1, 7, 2), (6, 3, 5, 4))


def silu(v):
    return v * jax.nn.sigmoid(v)


def dot(a, b):
    return jnp.dot(a, b, preferred_element_type=F32)


def dot_t(a, b):
    return lax.dot_general(a, b, (((1,), (1,)), ((), ())), preferred_element_type=F32)


def iota(shape, dim):
    return lax.broadcasted_iota(I32, shape, dim)


def kernel(
    hidden, state, attn_gain, wq, wk, wv, wg, w_beta, w_decay, decay_scale, head_gain, w_out, ffn_gain, ids, route,
    eg, eu, ed, dg, du, dd, mix,
    result, new_state,
    hid_all, v_state, v_again, v_w, v_wb, v_wd, v_dscale, v_hgain, v_wo, v_fgain, v_ids, v_route,
    v_e, v_ed, v_d, v_dd, v_mix,
    heads_all, mixed_s, send_mat, take_mat,
    disp, xa, stage, stage_e, square_e, acc_e, pb, pr, qs, yr, ret, rb,
    own_tok, dx, xn_d, square_d, px, xr, sums_x, zs, fr, count,
    l_sem, send, a_recv, h_recv, t_recv, d_recv, x_recv, y_recv, c_recv, p_recv, q_recv, b_recv, u_recv, w_recv, met,
):
    ep = lax.axis_index("ep")
    t = lax.axis_index("tp")
    z, x = lax.div(ep, NX), lax.rem(ep, NX)
    y, c = lax.div(t, 2), lax.rem(t, 2)

    def tp_peer(d):
        return ep, lax.rem(t + d, NTP)

    def ep_peer(d):
        return lax.rem(ep + d, NEP), t

    def z_peer(d):
        return lax.rem(z + d, NZ) * NX + x, t

    def x_peer(d):
        return z * NX + lax.rem(x + d, NX), t

    def y_peer(d):
        return ep, lax.rem(y + d, 4) * 2 + c

    partner = (ep, y * 2 + 1 - c)

    def remote(src, dst, recv, peer):
        pltpu.make_async_remote_copy(
            src_ref=src, dst_ref=dst, send_sem=send, recv_sem=recv, device_id=peer, device_id_type=MESH
        ).start()

    def take(view, sem):
        pltpu.make_async_copy(view, view, sem).wait()

    barrier = pltpu.get_barrier_semaphore()
    near = [tp_peer(d) for d in range(1, NTP)] + [z_peer(1), z_peer(NZ - 1), x_peer(1), x_peer(NX - 1)]
    for peer in near:
        pl.semaphore_signal(barrier, inc=1, device_id=peer, device_id_type=MESH)

    def tell(number, peers):
        for peer in peers:
            pl.semaphore_signal(met.at[number], inc=1, device_id=peer, device_id_type=MESH)

    loads = {}
    pairs = (
        ("hid", (hidden,), hid_all.at[t]), ("again", (attn_gain,), v_again), ("w", (wq, wk, wv, wg), v_w),
        ("wb", (w_beta,), v_wb), ("wd", (w_decay,), v_wd), ("dscale", (decay_scale,), v_dscale),
        ("hgain", (head_gain,), v_hgain), ("ids", (ids,), v_ids), ("route", (route,), v_route),
        ("state", (state,), v_state), ("wo", (w_out,), v_wo), ("fgain", (ffn_gain,), v_fgain), ("mix", (mix,), v_mix),
        ("d", (dg, du), v_d), ("dd", (dd,), v_dd), ("e", (eg, eu), v_e), ("ed", tuple(ed.at[:, pl.ds(b * WIDTH, WIDTH)] for b in range(NTP)), v_ed),
    )
    for number, (name, sources, dst) in enumerate(pairs):
        loads[name] = functools.partial(take, dst, l_sem.at[number])
        for place, src in enumerate(sources):
            part = dst.at[place] if len(sources) > 1 else dst
            pltpu.make_async_copy(src, part, l_sem.at[number]).start()

    loads["hid"]()
    pl.semaphore_wait(barrier, len(near))

    for d in FAR_TP:
        remote(hid_all.at[t], hid_all.at[t], a_recv.at[0 if d in NEAR_TP else 1], tp_peer(d))
    tell(0, (z_peer(1), z_peer(NZ - 1), x_peer(1), x_peer(NX - 1)))
    loads["ids"]()
    loads["route"]()
    first, second = v_ids[0:1, :], v_ids[1:2, :]
    expert = iota((NEP, SEQ), 0)
    is_first, is_second = first == expert, second == expert
    chosen = jnp.where(is_first | is_second, 1.0, 0.0)
    earlier = jnp.where(iota((SEQ, SEQ), 0) < iota((SEQ, SEQ), 1), 1.0, 0.0).astype(BF16)
    before = dot(chosen.astype(BF16), earlier)
    place = (chosen * (before + 1.0)).astype(BF16)
    row = iota((NEP * 8, NEP), 0)
    spread = jnp.where(row // 8 == iota((NEP * 8, NEP), 1), 1.0, 0.0).astype(BF16)
    hit = dot(spread, place) == ((row % 8) // 2 + 1).astype(F32)
    weight = jnp.where(is_first, v_route[0:1, :], 0.0) + jnp.where(is_second, v_route[1:2, :], 0.0)
    coarse = weight.astype(BF16)
    fine = (weight - coarse.astype(F32)).astype(BF16)
    coarse, fine = dot(spread, coarse), dot(spread, fine)
    for h in range(2):
        here = hit & (row % 2 == h)
        send_mat[h, : NEP * 8] = jnp.where(here, 1.0, 0.0).astype(BF16)
        for i, part in enumerate((coarse, fine)):
            rows = slice((2 * h + i) * SEQ, (2 * h + i + 1) * SEQ)
            take_mat[rows] = jnp.where(here, part, 0.0).T.astype(BF16)
    t_row, t_col = iota((NTP * 8, SEQ), 0), iota((NTP * 8, SEQ), 1)
    for h in range(2):
        send_mat[h, NEP * 8 :] = jnp.where((t_row // 2 == t_col) & (t_row % 2 == h), 1.0, 0.0).astype(BF16)

    pl.semaphore_wait(met.at[0], 4)
    tell(1, (z_peer(2), z_peer(NZ - 2)))
    for name in ("again", "w", "wb", "wd"):
        loads[name]()

    def project(slots):
        sums = None
        for b in slots:
            cols = pl.ds(pl.multiple_of(b * WIDTH, WIDTH), WIDTH)
            wide = hid_all[b].astype(F32)
            part = (wide * v_again[b]).astype(BF16)
            outs = [wide * wide] + [dot(part, v_w[i, cols, :]) for i in range(4)]
            outs += [dot_t(part, v_wb[:, cols]), dot_t(part, v_wd[:, cols])]
            sums = outs if sums is None else [total + out for total, out in zip(sums, outs)]
        return sums

    take(hid_all.at[pl.ds(0, 4)], a_recv.at[0])
    sums = project([t] + [lax.rem(t + NTP - d, NTP) for d in NEAR_TP])
    take(hid_all.at[pl.ds(0, 3)], a_recv.at[1])
    late = project([lax.rem(t + NTP - d, NTP) for d in (3, 5, 4)])
    sums = [total + part for total, part in zip(sums, late)]
    pl.semaphore_wait(met.at[1], 2)
    tell(2, (x_peer(1), x_peer(2), x_peer(3), z_peer(NZ // 2)))
    for name in ("dscale", "hgain"):
        loads[name]()
    scale = lax.rsqrt(jnp.sum(sums[0], axis=-1, keepdims=True) * (1.0 / D) + EPS)
    queries, keys, values, gates, beta_all, decay_all = (total * scale for total in sums[1:])
    queries = queries * lax.rsqrt(jnp.sum(queries * queries, axis=-1, keepdims=True) + EPS) * DK ** (-0.5)
    keys = keys * lax.rsqrt(jnp.sum(keys * keys, axis=-1, keepdims=True) + EPS)
    mine = iota((SEQ, NTP), 1) == t
    beta = jax.nn.sigmoid(jnp.sum(jnp.where(mine, beta_all, 0.0), axis=-1, keepdims=True))
    logit = jnp.sum(jnp.where(mine, decay_all, 0.0), axis=-1, keepdims=True)
    d_scale = jnp.sum(jnp.where(iota((1, NTP), 1) == t, v_dscale[...], 0.0), axis=-1, keepdims=True)
    soft = jnp.maximum(logit, 0.0) + jnp.log(1.0 + jnp.exp(-jnp.abs(logit)))
    decay = jnp.exp(-d_scale * soft)

    loads["state"]()
    qb, kb = queries.astype(BF16), keys.astype(BF16)
    diag = iota((16, 1024), 1) // DK == iota((16, 1024), 0) % 8
    by_query, by_key = [], []
    for i in range(SEQ // 8):
        both = jnp.concatenate([qb[8 * i : 8 * i + 8].astype(F32), kb[8 * i : 8 * i + 8].astype(F32)], axis=0)
        lhs = jnp.where(diag, jnp.concatenate([both] * 8, axis=1), 0.0).astype(BF16)
        rhs = v_state[8 * i : 8 * i + 8].reshape(1024, DK).astype(BF16)
        out = dot(lhs, rhs)
        by_query.append(out[:8])
        by_key.append(out[8:])
    s_q = jnp.concatenate(by_query, axis=0)
    s_k = jnp.concatenate(by_key, axis=0)
    match = beta * jnp.sum(queries * keys, axis=-1, keepdims=True)
    read = decay * (s_q - match * s_k) + match * values
    read = read * lax.rsqrt(jnp.mean(read * read, axis=-1, keepdims=True) + EPS) * v_hgain[...]
    heads_all[t] = (read * silu(gates)).astype(BF16)
    for d in FAR_TP:
        remote(heads_all.at[t], heads_all.at[t], h_recv, tp_peer(d))
    update = beta * (values - decay * s_k)
    keys_t = jnp.concatenate([keys, jnp.zeros((DK - SEQ, DK), F32)], axis=0).T
    decay_rows = jnp.broadcast_to(decay, (SEQ, DK))
    for s in range(SEQ):
        new_state[s] = decay_rows[s : s + 1] * v_state[s] + keys_t[:, s : s + 1] * update[s : s + 1]

    pl.semaphore_wait(met.at[2], 4)
    loads["wo"]()
    take(heads_all.at[pl.ds(0, 7)], h_recv)
    wide = hid_all[t].astype(F32)
    for b in range(NTP):
        wide = wide + dot(heads_all[b], v_wo[b * DK : (b + 1) * DK, :])
    mixed = wide.astype(BF16)
    mixed_s[...] = mixed
    low, high = mixed[:, :128], mixed[:, 128:]

    moved = (dot(send_mat[0], low) + dot(send_mat[1], high)).reshape(NEP + NTP, 8, 128).astype(BF16)
    disp[...] = moved[:NEP]
    own_tok[...] = moved[NEP:]
    def dispatch(dz):
        base = z_peer(dz)[0] - x
        for d in (2, 1, 3, 0):
            if dz or d:
                to = base + lax.rem(x + d, NX)
                remote(disp.at[to], xa.at[t, ep], d_recv.at[ROUND_OF[dz]], (to, t))

    def tokens(dz):
        for d in FAR_TP + (0,):
            if dz or d:
                to = lax.rem(t + d, NTP)
                remote(own_tok.at[to], dx.at[ep, t], t_recv.at[ROUND_OF[dz]], (z_peer(dz)[0], to))

    for dz in FAR_Z + (0,):
        dispatch(dz)
    for dz in FAR_Z + (0,):
        tokens(dz)
    xa[t, ep] = disp[ep]
    dx[ep, t] = own_tok[t]
    for distance in range(NZ // 2 + 1):
        group = [dz for dz in range(NZ) if ROUND_OF[dz] == distance]
        blocks = [lax.rem(z + NZ - dz, NZ) for dz in group]
        take(disp.at[pl.ds(0, NX * len(group) if distance else NX - 1)], d_recv.at[distance])
        for from_z in blocks:
            block = xa.at[t, pl.ds(from_z * NX, NX)]
            for d in (2, 1, 3):
                remote(block, block, y_recv.at[d - 1], y_peer(d))
            remote(block, block, c_recv.at[0], partner)
        take(fr.at[pl.ds(0, NTP * len(group) if distance else NTP - 1)], t_recv.at[distance])
        for dz, from_z in zip(group, blocks):
            block = dx.at[from_z * NX + x]
            for d in (2, 1, 3):
                remote(block, block, x_recv.at[int(dz in HALVES[1])], x_peer(d))
    loads["fgain"]()
    for name in ("d", "dd"):
        loads[name]()

    def load_rows(half, d):
        xx = lax.rem(x + NX - d, NX)
        for k, dz in enumerate(HALVES[half]):
            block = dx[lax.rem(z + NZ - dz, NZ) * NX + xx]
            stage[pl.ds((d * 4 + k) * PITCH, 64), :] = block.astype(F32).reshape(64, 128)
        for j in range(4):
            row = d * 16 + j * 4
            square = 0.0
            for b in range(16):
                part = stage[pl.ds(d * 4 * PITCH + (b // 2) * 8 + j * 2 + b % 2, 4, stride=PITCH), :]
                square = square + part * part
                gain = v_fgain[b // 2, :, (b % 2) * 128 : (b % 2 + 1) * 128]
                xn_d[half, row : row + 4, b * 128 : (b + 1) * 128] = part * gain
            square_d[half, row : row + 4] = square

    def dense(half):
        take(dx.at[pl.ds(0, 12)], x_recv.at[half])
        for d in (1, 3, 2):
            load_rows(half, d)
        rows = xn_d[half].astype(BF16)
        scale = lax.rsqrt(jnp.sum(square_d[half], axis=-1, keepdims=True) * (1.0 / D) + EPS)
        hidden_d = (silu(dot(rows, v_d[0]) * scale) * (dot(rows, v_d[1]) * scale)).astype(BF16)
        for f in range(CHUNKS):
            out = dot(hidden_d, v_dd[:, f * WIDE : (f + 1) * WIDE]).astype(BF16)
            for d in range(NX):
                px[half, d, f] = out[d * 16 : (d + 1) * 16]
        for f in range(CHUNKS):
            for d in (2, 1, 3):
                back = NX - d
                remote(px.at[half, d, f], xr.at[half, back - 1, f], u_recv.at[half, f], x_peer(back))

    load_rows(0, 0)
    load_rows(1, 0)
    for name in ("e", "ed"):
        loads[name]()

    def expert_slices(slots, start):
        square, outs = 0.0, [0.0, 0.0]
        for number, b in enumerate(slots):
            base = pl.multiple_of(b * WIDTH, WIDTH)
            stage_e[number, pl.ds(0, 256), :] = xa[b].astype(F32).reshape(256, 128)
            parts = [stage_e[number, pl.ds(h, ROWS, stride=2), :] for h in range(2)]
            square = square + parts[0] * parts[0] + parts[1] * parts[1]
            gain = v_fgain[b]
            rows = jnp.concatenate([parts[h] * gain[:, h * 128 : (h + 1) * 128] for h in range(2)], axis=1).astype(BF16)
            outs = [outs[i] + dot(rows, v_e[i, pl.ds(base, WIDTH), :]) for i in range(2)]
        square_e[...] = square if start else square_e[...] + square
        for i in range(2):
            acc_e[i] = outs[i] if start else acc_e[i] + outs[i]

    expert_slices([t], True)
    take(xa.at[0], c_recv.at[0])
    expert_slices([y * 2 + 1 - c], False)
    for d in (1, 3, 2):
        take(xa.at[0], y_recv.at[d - 1])
        block = xa.at[lax.rem(y + 4 - d, 4) * 2 + c]
        remote(block, block, c_recv.at[1], partner)
    expert_slices([lax.rem(y + 4 - d, 4) * 2 + c for d in (1, 3, 2)], False)
    dense(0)
    take(xa.at[pl.ds(0, 3)], c_recv.at[1])
    expert_slices([lax.rem(y + 4 - d, 4) * 2 + 1 - c for d in (1, 3, 2)], False)
    scale = lax.rsqrt(jnp.sum(square_e[...], axis=-1, keepdims=True) * (1.0 / D) + EPS)
    inner = (silu(acc_e[0] * scale) * (acc_e[1] * scale)).astype(BF16)

    def down(core):
        for d in (2, 1, 3, 0):
            b = lax.rem(y + d, 4) * 2 + core
            pb[b] = dot(inner, v_ed[b]).astype(BF16)

    down(1 - c)
    for d in (2, 1, 3, 0):
        there = lax.rem(y + d, 4)
        remote(pb.at[there * 2 + 1 - c], pr.at[there], p_recv.at[d], partner)
    down(c)
    dense(1)
    for d in (2, 1, 3, 0):
        there = lax.rem(y + d, 4)
        take(pr.at[0], p_recv.at[d])
        qs[there] = (pb[there * 2 + c].astype(F32) + pr[there].astype(F32)).astype(BF16)
        if d > 0:
            remote(qs.at[there], yr.at[d - 1], q_recv, y_peer(d))

    def sum_x(half, f):
        take(xr.at[half, :, f], u_recv.at[half, f])
        total = px[half, 0, f].astype(F32)
        for d in range(3):
            total = total + xr[half, d, f].astype(F32)
        sums_x[...] = total
        for tt in range(2):
            for h in range(2):
                cols = slice(tt * WIDTH + h * 128, tt * WIDTH + (h + 1) * 128)
                for j in range(4):
                    stage[pl.ds(tt * 8 + j * 2 + h, 4, stride=PITCH), :] = sums_x[j * 4 : (j + 1) * 4, cols]
        for k, dz in enumerate(HALVES[half]):
            zs[half * 4 + k, 2 * f : 2 * f + 2] = stage[pl.ds(k * PITCH, 16), :].reshape(2, 8, 128).astype(BF16)
        for k, dz in reversed(tuple(enumerate(HALVES[half]))):
            to = z_peer(NZ - dz)[0]

            def piece(tt):
                remote(zs.at[half * 4 + k, tt], fr.at[z * NTP + t], w_recv, (to, tt))

            for tt in (2 * f, 2 * f + 1):
                if dz:
                    piece(tt)
                else:
                    pl.when(t != tt)(functools.partial(piece, tt))

    for f in range(CHUNKS):
        sum_x(0, f)
    sum_x(1, 0)
    sum_x(1, 1)
    sum_x(1, 2)
    sum_x(1, 3)
    fr[z * NTP + t] = zs[0, t]
    take(yr, q_recv)
    total = qs[y].astype(F32)
    for d in range(3):
        total = total + yr[d].astype(F32)
    total = total.astype(BF16).astype(F32)
    for h in range(2):
        stage[pl.ds(h, ROWS, stride=2), :] = total[:, h * 128 : (h + 1) * 128]
    ret[...] = stage[pl.ds(0, 256), :].reshape(NEP, 8, 128).astype(BF16)

    for dz in FAR_Z + (0,):
        base = z_peer(dz)[0] - x
        for d in (2, 1, 3, 0):
            if dz or d:
                to = base + lax.rem(x + d, NX)
                remote(ret.at[to], rb.at[ep], b_recv, (to, t))
    rb[ep] = ret[ep]
    loads["mix"]()
    take(fr.at[pl.ds(0, NZ * NTP - 1)], w_recv)
    total = fr[0:NTP].astype(F32)
    for zz in range(1, NZ):
        total = total + fr[zz * NTP : (zz + 1) * NTP].astype(F32)
    stage[pl.ds(0, 64), :] = total.reshape(64, 128)
    take(rb.at[pl.ds(0, NEP - 1)], b_recv)
    back = rb[...].astype(F32).reshape(NEP * 8, 128).astype(BF16)
    taken = dot(take_mat[...], back)
    for h in range(2):
        cols = slice(h * 128, (h + 1) * 128)
        moe = taken[2 * h * SEQ : (2 * h + 1) * SEQ] + taken[(2 * h + 1) * SEQ : (2 * h + 2) * SEQ]
        dense_out = stage[pl.ds(h, SEQ, stride=2), :]
        result[:, cols] = (
            mixed_s[:, cols].astype(F32) + moe + jax.nn.sigmoid(v_mix[:, cols]) * dense_out
        ).astype(BF16)
    take(count, send)


def write_out(result, new_state, result_out, state_out, sem):
    first = pltpu.make_async_copy(new_state, state_out, sem.at[0])
    second = pltpu.make_async_copy(result, result_out, sem.at[1])
    first.start()
    second.start()
    first.wait()
    second.wait()


def per_device(
    hidden_in, state_in, attn_gain, w_query, w_key, w_value, w_gate, w_beta, w_decay, decay_scale, head_gain, w_output,
    ffn_gain, expert_ids, route_weight, expert_gate, expert_up, expert_down, dense_gate, dense_up, dense_down, dense_mix,
):
    operands = (
        hidden_in, state_in.reshape(SEQ, DK, DK), attn_gain.reshape(NTP, 1, WIDTH), w_query, w_key, w_value, w_gate, w_beta.T,
        w_decay.T, decay_scale.reshape(1, NTP), head_gain.reshape(1, DK), w_output, ffn_gain.reshape(NTP, 1, WIDTH), expert_ids.T,
        route_weight.T, expert_gate[0], expert_up[0], expert_down[0], dense_gate, dense_up, dense_down,
        dense_mix.reshape(1, WIDTH),
    )
    V = pltpu.VMEM
    vmem_of = [
        V((NTP, SEQ, WIDTH), BF16), V((SEQ, DK, DK), F32), V((NTP, 1, WIDTH), F32), V((4, D, DK), BF16), V((NTP, D), BF16),
        V((NTP, D), BF16), V((1, NTP), F32), V((1, DK), F32), V((NTP * DK, WIDTH), BF16), V((NTP, 1, WIDTH), F32),
        V((2, SEQ), I32), V((2, SEQ), F32), V((2, D, FE), BF16), V((NTP, FE, WIDTH), BF16), V((2, D, FD), BF16),
        V((FD, D), BF16), V((1, WIDTH), F32),
    ]
    dma = pltpu.SemaphoreType.DMA
    scratch = vmem_of + [
        V((NTP, SEQ, DK), BF16), V((SEQ, WIDTH), BF16),
        V((2, (NEP + NTP) * 8, SEQ), BF16), V((4 * SEQ, NEP * 8), BF16),
        V((NEP, 8, 128), BF16), V((NTP, NEP, 8, 128), BF16), V((18 * PITCH, 128), F32), V((3, 264, 128), F32),
        V((ROWS, 128), F32), V((2, ROWS, FE), F32), V((NTP, ROWS, WIDTH), BF16), V((4, ROWS, WIDTH), BF16), V((4, ROWS, WIDTH), BF16),
        V((3, ROWS, WIDTH), BF16), V((NEP, 8, 128), BF16), V((NEP, 8, 128), BF16),
        V((NTP, 8, 128), BF16), V((NEP, NTP, 8, 128), BF16), V((2, NX * 16, D), F32), V((2, NX * 16, 128), F32),
        V((2, NX, CHUNKS, 16, WIDE), BF16), V((2, NX - 1, CHUNKS, 16, WIDE), BF16), V((16, WIDE), F32),
        V((NZ, NTP, 8, 128), BF16), V((NZ * NTP, 8, 128), BF16), V((SENT, 8, 128), BF16),
        dma((17,)), dma, dma((2,)), dma, dma((5,)), dma((5,)), dma((2,)), dma((3,)), dma((2,)), dma((4,)), dma,
        dma, dma((2, CHUNKS)), dma,
        pltpu.SemaphoreType.REGULAR((3,)),
    ]
    kept = (V((SEQ, WIDTH), BF16), V((SEQ, DK, DK), F32))
    result, new_state = pl.pallas_call(
        kernel,
        out_shape=kept,
        in_specs=[pl.BlockSpec(memory_space=pltpu.HBM)] * len(operands),
        out_specs=tuple(pl.BlockSpec(memory_space=pltpu.VMEM) for _ in kept),
        scratch_shapes=scratch,
        compiler_params=pltpu.CompilerParams(
            collective_id=0, has_side_effects=True, vmem_limit_bytes=64000000
        ),
    )(*operands)
    result, new_state = pl.pallas_call(
        write_out,
        out_shape=tuple(jax.ShapeDtypeStruct(k.shape, k.dtype) for k in kept),
        in_specs=[pl.BlockSpec(memory_space=pltpu.VMEM)] * 2,
        out_specs=tuple(pl.BlockSpec(memory_space=pltpu.HBM) for _ in kept),
        scratch_shapes=[dma((2,))],
        compiler_params=pltpu.CompilerParams(vmem_limit_bytes=8 * 1024 * 1024),
    )(result, new_state)
    return result, new_state.reshape(state_in.shape)


def solution(mesh):
    return jax.shard_map(
        per_device,
        mesh=mesh,
        in_specs=(
            P("ep", "tp"), P("ep", "tp", None, None), P(), P(None, "tp"), P(None, "tp"), P(None, "tp"), P(None, "tp"),
            P(), P(), P(), P(), P(None, "tp"), P(), P("ep", None), P("ep", None), P("ep", None, "tp"),
            P("ep", None, "tp"), P("ep", "tp", None), P(None, "ep"), P(None, "ep"), P("ep", None), P("tp"),
        ),
        out_specs=(P("ep", "tp"), P("ep", "tp", None, None)),
        check_vma=False,
    )
```

```python
import functools

import jax
import jax.numpy as jnp
from jax import lax
from jax.experimental import pallas as pl
from jax.experimental.pallas import tpu as pltpu
from jax.sharding import PartitionSpec as P

EPS = 1e-06
MESH = pl.DeviceIdType.MESH
F32, BF16, I32 = jnp.float32, jnp.bfloat16, jnp.int32

NX, NZ, NTP, NEP = 4, 8, 8, 32
SEQ, D, WIDTH, DK, CAP = 32, 2048, 256, 128, 4
ROWS = NEP * CAP
FE, FD = 384, 128
PITCH = 72
CHUNKS = 4
WIDE = D // CHUNKS
SENT = 7 * 8 + 7 * 4 + 63 + 31 + 24 * 8 + 3 * 32 + 4 * 32 + 12 * 16 + 4 * 32 + 3 * 32 + 63 + 31
FAR_TP = FAR_Z = (4, 3, 5, 2, 6, 1, 7)
NEAR_TP = (1, 7, 2, 6)
ROUND_OF = (0, 1, 2, 3, 4, 3, 2, 1)
HALVES = ((0, 1, 7, 2), (6, 3, 5, 4))


def silu(v):
    return v * jax.nn.sigmoid(v)


def dot(a, b):
    return jnp.dot(a, b, preferred_element_type=F32)


def dot_t(a, b):
    return lax.dot_general(a, b, (((1,), (1,)), ((), ())), preferred_element_type=F32)


def iota(shape, dim):
    return lax.broadcasted_iota(I32, shape, dim)


def kernel(
    hidden, state, attn_gain, wq, wk, wv, wg, w_beta, w_decay, decay_scale, head_gain, w_out, ffn_gain, ids, route,
    eg, eu, ed, dg, du, dd, mix,
    result, new_state,
    hid_all, v_state, v_again, v_w, v_wb, v_wd, v_dscale, v_hgain, v_wo, v_fgain, v_ids, v_route,
    v_e, v_ed, v_d, v_dd, v_mix,
    heads_all, mixed_s, send_mat, take_mat,
    disp, xa, stage, stage_e, square_e, acc_e, pb, pr, qs, yr, ret, rb,
    own_tok, dx, xn_d, square_d, px, xr, sums_x, zs, fr, count,
    l_sem, send, a_recv, h_recv, t_recv, d_recv, x_recv, y_recv, c_recv, p_recv, q_recv, b_recv, u_recv, w_recv, met,
):
    ep = lax.axis_index("ep")
    t = lax.axis_index("tp")
    z, x = lax.div(ep, NX), lax.rem(ep, NX)
    y, c = lax.div(t, 2), lax.rem(t, 2)

    def tp_peer(d):
        return ep, lax.rem(t + d, NTP)

    def ep_peer(d):
        return lax.rem(ep + d, NEP), t

    def z_peer(d):
        return lax.rem(z + d, NZ) * NX + x, t

    def x_peer(d):
        return z * NX + lax.rem(x + d, NX), t

    def y_peer(d):
        return ep, lax.rem(y + d, 4) * 2 + c

    partner = (ep, y * 2 + 1 - c)

    def remote(src, dst, recv, peer):
        pltpu.make_async_remote_copy(
            src_ref=src, dst_ref=dst, send_sem=send, recv_sem=recv, device_id=peer, device_id_type=MESH
        ).start()

    def take(view, sem):
        pltpu.make_async_copy(view, view, sem).wait()

    barrier = pltpu.get_barrier_semaphore()
    near = [tp_peer(d) for d in range(1, NTP)] + [z_peer(1), z_peer(NZ - 1), x_peer(1), x_peer(NX - 1)]
    for peer in near:
        pl.semaphore_signal(barrier, inc=1, device_id=peer, device_id_type=MESH)

    def tell(number, peers):
        for peer in peers:
            pl.semaphore_signal(met.at[number], inc=1, device_id=peer, device_id_type=MESH)

    loads = {}
    pairs = (
        ("hid", (hidden,), hid_all.at[t]), ("again", (attn_gain,), v_again), ("w", (wq, wk, wv, wg), v_w),
        ("wb", (w_beta,), v_wb), ("wd", (w_decay,), v_wd), ("dscale", (decay_scale,), v_dscale),
        ("hgain", (head_gain,), v_hgain), ("ids", (ids,), v_ids), ("route", (route,), v_route),
        ("state", (state,), v_state), ("wo", (w_out,), v_wo), ("fgain", (ffn_gain,), v_fgain), ("mix", (mix,), v_mix),
        ("d", (dg, du), v_d), ("dd", (dd,), v_dd), ("e", (eg, eu), v_e), ("ed", tuple(ed.at[:, pl.ds(b * WIDTH, WIDTH)] for b in range(NTP)), v_ed),
    )
    for number, (name, sources, dst) in enumerate(pairs):
        loads[name] = functools.partial(take, dst, l_sem.at[number])
        for place, src in enumerate(sources):
            part = dst.at[place] if len(sources) > 1 else dst
            pltpu.make_async_copy(src, part, l_sem.at[number]).start()

    loads["hid"]()
    pl.semaphore_wait(barrier, len(near))

    for d in FAR_TP:
        remote(hid_all.at[t], hid_all.at[t], a_recv.at[0 if d in NEAR_TP else 1], tp_peer(d))
    tell(0, (z_peer(1), z_peer(NZ - 1), x_peer(1), x_peer(NX - 1)))
    loads["ids"]()
    loads["route"]()
    first, second = v_ids[0:1, :], v_ids[1:2, :]
    expert = iota((NEP, SEQ), 0)
    is_first, is_second = first == expert, second == expert
    chosen = jnp.where(is_first | is_second, 1.0, 0.0)
    earlier = jnp.where(iota((SEQ, SEQ), 0) < iota((SEQ, SEQ), 1), 1.0, 0.0).astype(BF16)
    before = dot(chosen.astype(BF16), earlier)
    place = (chosen * (before + 1.0)).astype(BF16)
    row = iota((NEP * 8, NEP), 0)
    spread = jnp.where(row // 8 == iota((NEP * 8, NEP), 1), 1.0, 0.0).astype(BF16)
    hit = dot(spread, place) == ((row % 8) // 2 + 1).astype(F32)
    weight = jnp.where(is_first, v_route[0:1, :], 0.0) + jnp.where(is_second, v_route[1:2, :], 0.0)
    coarse = weight.astype(BF16)
    fine = (weight - coarse.astype(F32)).astype(BF16)
    coarse, fine = dot(spread, coarse), dot(spread, fine)
    for h in range(2):
        here = hit & (row % 2 == h)
        send_mat[h, : NEP * 8] = jnp.where(here, 1.0, 0.0).astype(BF16)
        for i, part in enumerate((coarse, fine)):
            rows = slice((2 * h + i) * SEQ, (2 * h + i + 1) * SEQ)
            take_mat[rows] = jnp.where(here, part, 0.0).T.astype(BF16)
    t_row, t_col = iota((NTP * 8, SEQ), 0), iota((NTP * 8, SEQ), 1)
    for h in range(2):
        send_mat[h, NEP * 8 :] = jnp.where((t_row // 2 == t_col) & (t_row % 2 == h), 1.0, 0.0).astype(BF16)

    pl.semaphore_wait(met.at[0], 4)
    tell(1, (z_peer(2), z_peer(NZ - 2)))
    for name in ("again", "w", "wb", "wd"):
        loads[name]()

    def project(slots):
        sums = None
        for b in slots:
            cols = pl.ds(pl.multiple_of(b * WIDTH, WIDTH), WIDTH)
            wide = hid_all[b].astype(F32)
            part = (wide * v_again[b]).astype(BF16)
            outs = [wide * wide] + [dot(part, v_w[i, cols, :]) for i in range(4)]
            outs += [dot_t(part, v_wb[:, cols]), dot_t(part, v_wd[:, cols])]
            sums = outs if sums is None else [total + out for total, out in zip(sums, outs)]
        return sums

    take(hid_all.at[pl.ds(0, 4)], a_recv.at[0])
    sums = project([t] + [lax.rem(t + NTP - d, NTP) for d in NEAR_TP])
    take(hid_all.at[pl.ds(0, 3)], a_recv.at[1])
    late = project([lax.rem(t + NTP - d, NTP) for d in (3, 5, 4)])
    sums = [total + part for total, part in zip(sums, late)]
    pl.semaphore_wait(met.at[1], 2)
    tell(2, (x_peer(1), x_peer(2), x_peer(3), z_peer(NZ // 2)))
    for name in ("dscale", "hgain"):
        loads[name]()
    scale = lax.rsqrt(jnp.sum(sums[0], axis=-1, keepdims=True) * (1.0 / D) + EPS)
    queries, keys, values, gates, beta_all, decay_all = (total * scale for total in sums[1:])
    queries = queries * lax.rsqrt(jnp.sum(queries * queries, axis=-1, keepdims=True) + EPS) * DK ** (-0.5)
    keys = keys * lax.rsqrt(jnp.sum(keys * keys, axis=-1, keepdims=True) + EPS)
    mine = iota((SEQ, NTP), 1) == t
    beta = jax.nn.sigmoid(jnp.sum(jnp.where(mine, beta_all, 0.0), axis=-1, keepdims=True))
    logit = jnp.sum(jnp.where(mine, decay_all, 0.0), axis=-1, keepdims=True)
    d_scale = jnp.sum(jnp.where(iota((1, NTP), 1) == t, v_dscale[...], 0.0), axis=-1, keepdims=True)
    soft = jnp.maximum(logit, 0.0) + jnp.log(1.0 + jnp.exp(-jnp.abs(logit)))
    decay = jnp.exp(-d_scale * soft)

    loads["state"]()
    qb, kb = queries.astype(BF16), keys.astype(BF16)
    diag = iota((16, 1024), 1) // DK == iota((16, 1024), 0) % 8
    by_query, by_key = [], []
    for i in range(SEQ // 8):
        both = jnp.concatenate([qb[8 * i : 8 * i + 8].astype(F32), kb[8 * i : 8 * i + 8].astype(F32)], axis=0)
        lhs = jnp.where(diag, jnp.concatenate([both] * 8, axis=1), 0.0).astype(BF16)
        rhs = v_state[8 * i : 8 * i + 8].reshape(1024, DK).astype(BF16)
        out = dot(lhs, rhs)
        by_query.append(out[:8])
        by_key.append(out[8:])
    s_q = jnp.concatenate(by_query, axis=0)
    s_k = jnp.concatenate(by_key, axis=0)
    match = beta * jnp.sum(queries * keys, axis=-1, keepdims=True)
    read = decay * (s_q - match * s_k) + match * values
    read = read * lax.rsqrt(jnp.mean(read * read, axis=-1, keepdims=True) + EPS) * v_hgain[...]
    heads_all[t] = (read * silu(gates)).astype(BF16)
    for d in FAR_TP:
        remote(heads_all.at[t], heads_all.at[t], h_recv.at[0 if d in NEAR_TP else 1], tp_peer(d))
    update = beta * (values - decay * s_k)
    keys_t = jnp.concatenate([keys, jnp.zeros((DK - SEQ, DK), F32)], axis=0).T
    decay_rows = jnp.broadcast_to(decay, (SEQ, DK))
    for s in range(SEQ):
        new_state[s] = decay_rows[s : s + 1] * v_state[s] + keys_t[:, s : s + 1] * update[s : s + 1]

    pl.semaphore_wait(met.at[2], 4)
    loads["wo"]()

    def project_out(slots):
        total = 0.0
        for b in slots:
            total = total + dot(heads_all[b], v_wo[pl.ds(pl.multiple_of(b * DK, DK), DK), :])
        return total

    take(heads_all.at[pl.ds(0, 4)], h_recv.at[0])
    wide = hid_all[t].astype(F32) + project_out([t] + [lax.rem(t + NTP - d, NTP) for d in NEAR_TP])
    take(heads_all.at[pl.ds(0, 3)], h_recv.at[1])
    wide = wide + project_out([lax.rem(t + NTP - d, NTP) for d in (3, 5, 4)])
    mixed = wide.astype(BF16)
    mixed_s[...] = mixed
    low, high = mixed[:, :128], mixed[:, 128:]

    moved = (dot(send_mat[0], low) + dot(send_mat[1], high)).reshape(NEP + NTP, 8, 128).astype(BF16)
    disp[...] = moved[:NEP]
    own_tok[...] = moved[NEP:]
    def dispatch(dz):
        base = z_peer(dz)[0] - x
        for d in (2, 1, 3, 0):
            if dz or d:
                to = base + lax.rem(x + d, NX)
                remote(disp.at[to], xa.at[t, ep], d_recv.at[ROUND_OF[dz]], (to, t))

    def tokens(dz):
        for d in FAR_TP + (0,):
            if dz or d:
                to = lax.rem(t + d, NTP)
                remote(own_tok.at[to], dx.at[ep, t], t_recv.at[ROUND_OF[dz]], (z_peer(dz)[0], to))

    for dz in FAR_Z + (0,):
        dispatch(dz)
    for dz in FAR_Z + (0,):
        tokens(dz)
    xa[t, ep] = disp[ep]
    dx[ep, t] = own_tok[t]
    for distance in range(NZ // 2 + 1):
        group = [dz for dz in range(NZ) if ROUND_OF[dz] == distance]
        blocks = [lax.rem(z + NZ - dz, NZ) for dz in group]
        take(disp.at[pl.ds(0, NX * len(group) if distance else NX - 1)], d_recv.at[distance])
        for from_z in blocks:
            block = xa.at[t, pl.ds(from_z * NX, NX)]
            for d in (2, 1, 3):
                remote(block, block, y_recv.at[d - 1], y_peer(d))
            remote(block, block, c_recv.at[0], partner)
        take(fr.at[pl.ds(0, NTP * len(group) if distance else NTP - 1)], t_recv.at[distance])
        for dz, from_z in zip(group, blocks):
            block = dx.at[from_z * NX + x]
            for d in (2, 1, 3):
                remote(block, block, x_recv.at[int(dz in HALVES[1])], x_peer(d))
    loads["fgain"]()
    for name in ("d", "dd"):
        loads[name]()

    def load_rows(half, d):
        xx = lax.rem(x + NX - d, NX)
        for k, dz in enumerate(HALVES[half]):
            block = dx[lax.rem(z + NZ - dz, NZ) * NX + xx]
            stage[pl.ds((d * 4 + k) * PITCH, 64), :] = block.astype(F32).reshape(64, 128)
        for j in range(4):
            row = d * 16 + j * 4
            square = 0.0
            for b in range(16):
                part = stage[pl.ds(d * 4 * PITCH + (b // 2) * 8 + j * 2 + b % 2, 4, stride=PITCH), :]
                square = square + part * part
                gain = v_fgain[b // 2, :, (b % 2) * 128 : (b % 2 + 1) * 128]
                xn_d[half, row : row + 4, b * 128 : (b + 1) * 128] = part * gain
            square_d[half, row : row + 4] = square

    def dense(half):
        take(dx.at[pl.ds(0, 12)], x_recv.at[half])
        for d in (1, 3, 2):
            load_rows(half, d)
        rows = xn_d[half].astype(BF16)
        scale = lax.rsqrt(jnp.sum(square_d[half], axis=-1, keepdims=True) * (1.0 / D) + EPS)
        hidden_d = (silu(dot(rows, v_d[0]) * scale) * (dot(rows, v_d[1]) * scale)).astype(BF16)
        for f in range(CHUNKS):
            out = dot(hidden_d, v_dd[:, f * WIDE : (f + 1) * WIDE]).astype(BF16)
            for d in range(NX):
                px[half, d, f] = out[d * 16 : (d + 1) * 16]
        for f in range(CHUNKS):
            for d in (2, 1, 3):
                back = NX - d
                remote(px.at[half, d, f], xr.at[half, back - 1, f], u_recv.at[half, f], x_peer(back))

    load_rows(0, 0)
    load_rows(1, 0)
    for name in ("e", "ed"):
        loads[name]()

    def expert_slices(slots, start):
        square, outs = 0.0, [0.0, 0.0]
        for number, b in enumerate(slots):
            base = pl.multiple_of(b * WIDTH, WIDTH)
            stage_e[number, pl.ds(0, 256), :] = xa[b].astype(F32).reshape(256, 128)
            parts = [stage_e[number, pl.ds(h, ROWS, stride=2), :] for h in range(2)]
            square = square + parts[0] * parts[0] + parts[1] * parts[1]
            gain = v_fgain[b]
            rows = jnp.concatenate([parts[h] * gain[:, h * 128 : (h + 1) * 128] for h in range(2)], axis=1).astype(BF16)
            outs = [outs[i] + dot(rows, v_e[i, pl.ds(base, WIDTH), :]) for i in range(2)]
        square_e[...] = square if start else square_e[...] + square
        for i in range(2):
            acc_e[i] = outs[i] if start else acc_e[i] + outs[i]

    expert_slices([t], True)
    take(xa.at[0], c_recv.at[0])
    expert_slices([y * 2 + 1 - c], False)
    for d in (1, 3, 2):
        take(xa.at[0], y_recv.at[d - 1])
        block = xa.at[lax.rem(y + 4 - d, 4) * 2 + c]
        remote(block, block, c_recv.at[1], partner)
    expert_slices([lax.rem(y + 4 - d, 4) * 2 + c for d in (1, 3, 2)], False)
    dense(0)
    take(xa.at[pl.ds(0, 3)], c_recv.at[1])
    expert_slices([lax.rem(y + 4 - d, 4) * 2 + 1 - c for d in (1, 3, 2)], False)
    scale = lax.rsqrt(jnp.sum(square_e[...], axis=-1, keepdims=True) * (1.0 / D) + EPS)
    inner = (silu(acc_e[0] * scale) * (acc_e[1] * scale)).astype(BF16)

    def down(core):
        for d in (2, 1, 3, 0):
            b = lax.rem(y + d, 4) * 2 + core
            pb[b] = dot(inner, v_ed[b]).astype(BF16)

    down(1 - c)
    for d in (2, 1, 3, 0):
        there = lax.rem(y + d, 4)
        remote(pb.at[there * 2 + 1 - c], pr.at[there], p_recv.at[d], partner)
    down(c)
    dense(1)
    for d in (2, 1, 3, 0):
        there = lax.rem(y + d, 4)
        take(pr.at[0], p_recv.at[d])
        qs[there] = (pb[there * 2 + c].astype(F32) + pr[there].astype(F32)).astype(BF16)
        if d > 0:
            remote(qs.at[there], yr.at[d - 1], q_recv, y_peer(d))

    def sum_x(half, f):
        take(xr.at[half, :, f], u_recv.at[half, f])
        total = px[half, 0, f].astype(F32)
        for d in range(3):
            total = total + xr[half, d, f].astype(F32)
        sums_x[...] = total
        for tt in range(2):
            for h in range(2):
                cols = slice(tt * WIDTH + h * 128, tt * WIDTH + (h + 1) * 128)
                for j in range(4):
                    stage[pl.ds(tt * 8 + j * 2 + h, 4, stride=PITCH), :] = sums_x[j * 4 : (j + 1) * 4, cols]
        for k, dz in enumerate(HALVES[half]):
            zs[half * 4 + k, 2 * f : 2 * f + 2] = stage[pl.ds(k * PITCH, 16), :].reshape(2, 8, 128).astype(BF16)
        for k, dz in reversed(tuple(enumerate(HALVES[half]))):
            to = z_peer(NZ - dz)[0]

            def piece(tt):
                remote(zs.at[half * 4 + k, tt], fr.at[z * NTP + t], w_recv, (to, tt))

            for tt in (2 * f, 2 * f + 1):
                if dz:
                    piece(tt)
                else:
                    pl.when(t != tt)(functools.partial(piece, tt))

    for f in range(CHUNKS):
        sum_x(0, f)
    sum_x(1, 0)
    sum_x(1, 1)
    sum_x(1, 2)
    sum_x(1, 3)
    fr[z * NTP + t] = zs[0, t]
    take(yr, q_recv)
    total = qs[y].astype(F32)
    for d in range(3):
        total = total + yr[d].astype(F32)
    total = total.astype(BF16).astype(F32)
    for h in range(2):
        stage[pl.ds(h, ROWS, stride=2), :] = total[:, h * 128 : (h + 1) * 128]
    ret[...] = stage[pl.ds(0, 256), :].reshape(NEP, 8, 128).astype(BF16)

    for dz in FAR_Z + (0,):
        base = z_peer(dz)[0] - x
        for d in (2, 1, 3, 0):
            if dz or d:
                to = base + lax.rem(x + d, NX)
                remote(ret.at[to], rb.at[ep], b_recv, (to, t))
    rb[ep] = ret[ep]
    loads["mix"]()
    take(fr.at[pl.ds(0, NZ * NTP - 1)], w_recv)
    total = fr[0:NTP].astype(F32)
    for zz in range(1, NZ):
        total = total + fr[zz * NTP : (zz + 1) * NTP].astype(F32)
    stage[pl.ds(0, 64), :] = total.reshape(64, 128)
    take(rb.at[pl.ds(0, NEP - 1)], b_recv)
    back = rb[...].astype(F32).reshape(NEP * 8, 128).astype(BF16)
    taken = dot(take_mat[...], back)
    for h in range(2):
        cols = slice(h * 128, (h + 1) * 128)
        moe = taken[2 * h * SEQ : (2 * h + 1) * SEQ] + taken[(2 * h + 1) * SEQ : (2 * h + 2) * SEQ]
        dense_out = stage[pl.ds(h, SEQ, stride=2), :]
        result[:, cols] = (
            mixed_s[:, cols].astype(F32) + moe + jax.nn.sigmoid(v_mix[:, cols]) * dense_out
        ).astype(BF16)
    take(count, send)


def write_out(result, new_state, result_out, state_out, sem):
    first = pltpu.make_async_copy(new_state, state_out, sem.at[0])
    second = pltpu.make_async_copy(result, result_out, sem.at[1])
    first.start()
    second.start()
    first.wait()
    second.wait()


def per_device(
    hidden_in, state_in, attn_gain, w_query, w_key, w_value, w_gate, w_beta, w_decay, decay_scale, head_gain, w_output,
    ffn_gain, expert_ids, route_weight, expert_gate, expert_up, expert_down, dense_gate, dense_up, dense_down, dense_mix,
):
    operands = (
        hidden_in, state_in.reshape(SEQ, DK, DK), attn_gain.reshape(NTP, 1, WIDTH), w_query, w_key, w_value, w_gate, w_beta.T,
        w_decay.T, decay_scale.reshape(1, NTP), head_gain.reshape(1, DK), w_output, ffn_gain.reshape(NTP, 1, WIDTH), expert_ids.T,
        route_weight.T, expert_gate[0], expert_up[0], expert_down[0], dense_gate, dense_up, dense_down,
        dense_mix.reshape(1, WIDTH),
    )
    V = pltpu.VMEM
    vmem_of = [
        V((NTP, SEQ, WIDTH), BF16), V((SEQ, DK, DK), F32), V((NTP, 1, WIDTH), F32), V((4, D, DK), BF16), V((NTP, D), BF16),
        V((NTP, D), BF16), V((1, NTP), F32), V((1, DK), F32), V((NTP * DK, WIDTH), BF16), V((NTP, 1, WIDTH), F32),
        V((2, SEQ), I32), V((2, SEQ), F32), V((2, D, FE), BF16), V((NTP, FE, WIDTH), BF16), V((2, D, FD), BF16),
        V((FD, D), BF16), V((1, WIDTH), F32),
    ]
    dma = pltpu.SemaphoreType.DMA
    scratch = vmem_of + [
        V((NTP, SEQ, DK), BF16), V((SEQ, WIDTH), BF16),
        V((2, (NEP + NTP) * 8, SEQ), BF16), V((4 * SEQ, NEP * 8), BF16),
        V((NEP, 8, 128), BF16), V((NTP, NEP, 8, 128), BF16), V((18 * PITCH, 128), F32), V((3, 264, 128), F32),
        V((ROWS, 128), F32), V((2, ROWS, FE), F32), V((NTP, ROWS, WIDTH), BF16), V((4, ROWS, WIDTH), BF16), V((4, ROWS, WIDTH), BF16),
        V((3, ROWS, WIDTH), BF16), V((NEP, 8, 128), BF16), V((NEP, 8, 128), BF16),
        V((NTP, 8, 128), BF16), V((NEP, NTP, 8, 128), BF16), V((2, NX * 16, D), F32), V((2, NX * 16, 128), F32),
        V((2, NX, CHUNKS, 16, WIDE), BF16), V((2, NX - 1, CHUNKS, 16, WIDE), BF16), V((16, WIDE), F32),
        V((NZ, NTP, 8, 128), BF16), V((NZ * NTP, 8, 128), BF16), V((SENT, 8, 128), BF16),
        dma((17,)), dma, dma((2,)), dma((2,)), dma((5,)), dma((5,)), dma((2,)), dma((3,)), dma((2,)), dma((4,)), dma,
        dma, dma((2, CHUNKS)), dma,
        pltpu.SemaphoreType.REGULAR((3,)),
    ]
    kept = (V((SEQ, WIDTH), BF16), V((SEQ, DK, DK), F32))
    result, new_state = pl.pallas_call(
        kernel,
        out_shape=kept,
        in_specs=[pl.BlockSpec(memory_space=pltpu.HBM)] * len(operands),
        out_specs=tuple(pl.BlockSpec(memory_space=pltpu.VMEM) for _ in kept),
        scratch_shapes=scratch,
        compiler_params=pltpu.CompilerParams(
            collective_id=0, has_side_effects=True, vmem_limit_bytes=64000000
        ),
    )(*operands)
    result, new_state = pl.pallas_call(
        write_out,
        out_shape=tuple(jax.ShapeDtypeStruct(k.shape, k.dtype) for k in kept),
        in_specs=[pl.BlockSpec(memory_space=pltpu.VMEM)] * 2,
        out_specs=tuple(pl.BlockSpec(memory_space=pltpu.HBM) for _ in kept),
        scratch_shapes=[dma((2,))],
        compiler_params=pltpu.CompilerParams(vmem_limit_bytes=8 * 1024 * 1024),
    )(result, new_state)
    return result, new_state.reshape(state_in.shape)


def solution(mesh):
    return jax.shard_map(
        per_device,
        mesh=mesh,
        in_specs=(
            P("ep", "tp"), P("ep", "tp", None, None), P(), P(None, "tp"), P(None, "tp"), P(None, "tp"), P(None, "tp"),
            P(), P(), P(), P(), P(None, "tp"), P(), P("ep", None), P("ep", None), P("ep", None, "tp"),
            P("ep", None, "tp"), P("ep", "tp", None), P(None, "ep"), P(None, "ep"), P("ep", None), P("tp"),
        ),
        out_specs=(P("ep", "tp"), P("ep", "tp", None, None)),
        check_vma=False,
    )
```
